32 devices in a mesh: sp: 8 (over z, x), tp: 4 (over y, core).
Axes of the slice: x: 2, y: 2, z: 4, core: 2. Of those that a mesh axis runs over, the one named last changes fastest.
Arguments:
- rows_in: bfloat16 [1024, 2048], P(('sp', 'tp')), may hold values from -8 to 8
- in_gain: float32 [2048], replicated, may hold values from 0.1 to 1.9
- query_down: bfloat16 [2048, 256], replicated, may hold values from -0.125 to 0.125
- query_gain: float32 [256], replicated, may hold values from 0.1 to 1.9
- kv_down: bfloat16 [2048, 128], replicated, may hold values from -0.125 to 0.125
- kv_gain: float32 [128], replicated, may hold values from 0.1 to 1.9
- rope_down: bfloat16 [2048, 64], replicated, may hold values from -0.125 to 0.125
- query_nope_up: bfloat16 [256, 512], P(None, 'tp'), may hold values from -0.375 to 0.375
- query_rope_up: bfloat16 [256, 256], P(None, 'tp'), may hold values from -0.375 to 0.375
- key_up: bfloat16 [128, 512], P(None, 'tp'), may hold values from -2.9811459 to 2.9811459
- value_up: bfloat16 [128, 512], P(None, 'tp'), may hold values from -0.5 to 0.5
- rec_query: bfloat16 [2048, 256], P(None, 'tp'), may hold values from -0.125 to 0.125
- rec_key: bfloat16 [2048, 256], P(None, 'tp'), may hold values from -0.125 to 0.125
- rec_value: bfloat16 [2048, 512], P(None, 'tp'), may hold values from -0.125 to 0.125
- gate_weight: bfloat16 [2048, 4, 4], P(None, None, 'tp'), may hold values from -0.125 to 0.125
- forget_level: float32 [1024, 2, 4], P('sp', None, 'tp'), may hold values from 0 to 14
- head_gain: float32 [512], P('tp'), may hold values from 0.1 to 1.9
- init_state: float32 [2, 4, 64, 128], P(None, 'tp'), may hold values from -96 to 96
- init_norm: float32 [2, 4, 64], P(None, 'tp'), may hold values from -96 to 96
- out_attn: bfloat16 [512, 2048], P('tp'), may hold values from -0.25 to 0.25
- out_rec: bfloat16 [512, 2048], P('tp'), may hold values from -0.25 to 0.25
Outputs:
- mixed_out: bfloat16 [1024, 2048], P(('sp', 'tp'))
The draws below stay inside these ranges and needn't reach their ends.
All inputs are finite; a program needn't handle non-finite values.
Results may differ from the reference program's by a relative error of at most 0.023.
Values may be sent and summed in bfloat16 or wider, within the bound.
No kernel may reach another device: no remote copies, remote signals or barrier semaphores. Data moves between devices by JAX's collectives and lax.ppermute only.
A program may use at most 64 MiB of HBM per device.

```python
import math
import jax
import jax.numpy as jnp
from jax import lax

D = 2048
HA = 4
RECURRENT_HEADS = 4
QL = 256
KVL = 128
NOPE = 128
ROPE = 64
VH = 128
MK = 64
MV = 128
MBLOCK = 128
SEQUENCE_TOKENS = 1024
HAG = 1
HMG = 1
N_TP = 4


def draw_rows_in(key, part):
    key_noise = jax.random.fold_in(key, 11)
    key_means = jax.random.fold_in(key, 12)
    regions = 64
    region_of = jnp.arange(SEQUENCE_TOKENS) * regions // SEQUENCE_TOKENS
    noise = jax.random.normal(key_noise, (SEQUENCE_TOKENS, D), jnp.float32)
    centres = 0.7 * jax.random.normal(key_means, (regions, D), jnp.float32)
    values = jnp.clip(noise + centres[region_of], -8.0, 8.0)
    return values.astype(jnp.bfloat16)


def draw_key_up(key, part):
    key_base = jax.random.fold_in(key, 31)
    base = jnp.clip(jax.random.normal(key_base, (KVL, HA, NOPE), jnp.float32), -4.0, 4.0) * KVL ** (-0.5)
    return base.reshape(KVL, HA * NOPE).astype(jnp.bfloat16)


def draw_forget_level(key, part):
    key_slow = jax.random.fold_in(key, 21)
    key_shift = jax.random.fold_in(key, 22)
    key_spike = jax.random.fold_in(key, 23)
    slow_heads = jax.random.bernoulli(key_slow, 0.5, (2, RECURRENT_HEADS))
    floor_level_value = jnp.where(slow_heads, jnp.log(4.0 * SEQUENCE_TOKENS), jnp.log(80.0)).astype(jnp.float32)
    blocks = 256
    block_lookup = jnp.arange(SEQUENCE_TOKENS) * blocks // SEQUENCE_TOKENS
    offset_steps = jax.random.uniform(key_shift, (blocks, 2, RECURRENT_HEADS), jnp.float32, -0.7, 0.7)
    spike_position = jax.random.randint(key_spike, (2, 2, RECURRENT_HEADS), 0, SEQUENCE_TOKENS)
    spike_match = jnp.any(jnp.arange(SEQUENCE_TOKENS)[:, None, None, None] == spike_position[None], axis=1)
    level_value = jnp.where(spike_match, 0.8, floor_level_value[None] + offset_steps[block_lookup])
    return level_value.astype(jnp.float32)


def block_levels(key, dims, split, low, top_value):
    level = 1.0
    for dim, parts in split:
        draws = jax.random.uniform(jax.random.fold_in(jax.random.fold_in(key, 6), dim), (parts,), jnp.float32, low / len(split), top_value / len(split))
        level = level * jnp.repeat(jnp.exp(draws), dims[dim] // parts).reshape((-1,) + (1,) * (len(dims) - 1 - dim))
    return level


def gaussian(key, extent, spread, most, split=(), kind=jnp.bfloat16):
    level = block_levels(key, extent, split, -0.22, 0.18) if split else 1.0
    drawn = jax.random.normal(key, extent, jnp.float32) * spread * level
    return jnp.minimum(jnp.maximum(drawn, -most), most).astype(kind)


def setup_inputs(seed: int = 0) -> dict:
    splits = jax.random.split(jax.random.key(seed), 22)
    rows_in = draw_rows_in(jax.random.fold_in(splits[21], 71), 0)
    in_gain = jnp.clip(1.0 + 0.18 * jax.random.normal(splits[1], (D,), jnp.float32), 0.1, 1.9)
    query_down = gaussian(splits[2], (D, QL), D ** -0.5, 0.125)
    query_gain = jnp.clip(1.0 + 0.18 * jax.random.normal(splits[3], (QL,), jnp.float32), 0.1, 1.9)
    kv_down = gaussian(splits[4], (D, KVL), D ** -0.5, 0.125)
    kv_gain = jnp.clip(1.0 + 0.18 * jax.random.normal(splits[5], (KVL,), jnp.float32), 0.1, 1.9)
    rope_down = gaussian(splits[6], (D, ROPE), D ** -0.5, 0.125)
    query_nope_up = gaussian(splits[7], (QL, HA * NOPE), QL ** -0.5, 0.375, ((1, 4),))
    query_rope_up = gaussian(splits[8], (QL, HA * ROPE), QL ** -0.5, 0.375, ((1, 4),))
    key_up = draw_key_up(jax.random.fold_in(splits[21], 71), 0)
    value_up = gaussian(splits[10], (KVL, HA * VH), KVL ** -0.5, 0.5, ((1, 4),))
    rec_query = gaussian(splits[11], (D, RECURRENT_HEADS * MK), D ** -0.5, 0.125, ((1, 4),))
    rec_key = gaussian(splits[12], (D, RECURRENT_HEADS * MK), D ** -0.5, 0.125, ((1, 4),))
    rec_value = gaussian(splits[13], (D, RECURRENT_HEADS * MV), D ** -0.5, 0.125, ((1, 4),))
    gate_weight = gaussian(splits[14], (D, 4, RECURRENT_HEADS), D ** -0.5, 0.125, ((2, 4),))
    forget_level = draw_forget_level(jax.random.fold_in(splits[21], 71), 0)
    head_gain = jnp.clip(1.0 + 0.18 * jax.random.normal(splits[16], (RECURRENT_HEADS * MV,), jnp.float32), 0.1, 1.9)
    init_state = gaussian(splits[17], (2, RECURRENT_HEADS, MK, MV), (0.5 * SEQUENCE_TOKENS ** 0.5), 96.0, ((1, 4),), jnp.float32)
    init_norm = gaussian(splits[18], (2, RECURRENT_HEADS, MK), (0.5 * SEQUENCE_TOKENS ** 0.5), 96.0, ((1, 4),), jnp.float32)
    out_attn = gaussian(splits[19], (HA * VH, D), (HA * VH) ** -0.5, 0.25, ((0, 4),))
    out_rec = gaussian(splits[20], (RECURRENT_HEADS * MV, D), (RECURRENT_HEADS * MV) ** -0.5, 0.25, ((0, 4),))
    return dict(rows_in=rows_in, in_gain=in_gain, query_down=query_down, query_gain=query_gain, kv_down=kv_down, kv_gain=kv_gain, rope_down=rope_down, query_nope_up=query_nope_up, query_rope_up=query_rope_up, key_up=key_up, value_up=value_up, rec_query=rec_query, rec_key=rec_key, rec_value=rec_value, gate_weight=gate_weight, forget_level=forget_level, head_gain=head_gain, init_state=init_state, init_norm=init_norm, out_attn=out_attn, out_rec=out_rec)


EPS = 1e-06
NEG = -1e+30

def rms_rows(values, gains):
    return values * lax.rsqrt(lax.optimization_barrier(jnp.mean(values * values, axis=-1, keepdims=True)) + EPS) * gains.astype(jnp.float32)

def rotate(values, positions):
    half_len = values.shape[-1] // 2
    frequency = 10000.0 ** (-jnp.arange(half_len, dtype=jnp.float32) / half_len)
    angles = positions.astype(jnp.float32)[:, None] * frequency[None, :]
    angles = jnp.concatenate([angles, angles], axis=-1)[:, None, :]
    turned = jnp.concatenate([-values[..., half_len:], values[..., :half_len]], axis=-1)
    return values * jnp.cos(angles) + turned * jnp.sin(angles)

def recurrence(query, keys_in, value_in, log_in, log_keep, c_start, n_start, m_start, floor_value):
    head_count, seq_len = log_in.shape
    block_count = seq_len // MBLOCK
    lower_mask = jnp.tril(jnp.ones((MBLOCK, MBLOCK), bool))
    highest = lax.Precision.HIGHEST

    def to_blocks(array):
        return jnp.moveaxis(array.reshape((head_count, block_count, MBLOCK) + array.shape[2:]), 1, 0)

    def one_step(carried, inputs):
        c_state, n_state, m_state = carried
        q_block, k_block, v_block, in_block, keep_block = inputs
        log_cum = jnp.cumsum(keep_block, axis=-1)
        log_decay = jnp.where(lower_mask, log_cum[:, :, None] - log_cum[:, None, :] + in_block[:, None, :], NEG)
        carry_log = log_cum + m_state[:, None]
        row_max = jnp.maximum(lax.optimization_barrier(jnp.max(log_decay, axis=-1)), carry_log)
        gated = jnp.einsum('htd,hsd->hts', q_block, k_block, precision=highest) * jnp.exp(log_decay - row_max[..., None])
        carry_weight = jnp.exp(carry_log - row_max)
        numerator = jnp.einsum('hts,hse->hte', gated, v_block, precision=highest) + carry_weight[..., None] * jnp.einsum('htd,hde->hte', q_block, c_state, precision=highest)
        denominator = lax.optimization_barrier(jnp.sum(gated, axis=-1)) + carry_weight * jnp.einsum('htd,hd->ht', q_block, n_state, precision=highest)
        result = numerator / jnp.maximum(jnp.abs(denominator), floor_value * jnp.exp(-row_max))[..., None]
        cum_end = log_cum[:, -1]
        weight_log = cum_end[:, None] - log_cum + in_block
        new_max = jnp.maximum(cum_end + m_state, lax.optimization_barrier(jnp.max(weight_log, axis=-1)))
        decay_all = jnp.exp(cum_end + m_state - new_max)
        in_weights = jnp.exp(weight_log - new_max[:, None])
        c_state = decay_all[:, None, None] * c_state + jnp.einsum('hsd,hse->hde', k_block * in_weights[..., None], v_block, precision=highest)
        n_state = decay_all[:, None] * n_state + jnp.einsum('hs,hsd->hd', in_weights, k_block, precision=highest)
        return ((c_state, n_state, new_max), result)
    inputs = tuple((to_blocks(array) for array in (query, keys_in, value_in, log_in, log_keep)))
    _, outputs = lax.scan(one_step, (c_start, n_start, m_start), inputs)
    return jnp.moveaxis(outputs, 0, 1).reshape(head_count, seq_len, -1)

def heads_first(product, head_width):
    rounded = lax.optimization_barrier(product.astype(jnp.bfloat16))
    return rounded.astype(jnp.float32).reshape(product.shape[0], -1, head_width).transpose(1, 0, 2)

def reference(rows_in, in_gain, query_down, query_gain, kv_down, kv_gain, rope_down, query_nope_up, query_rope_up, key_up, value_up, rec_query, rec_key, rec_value, gate_weight, forget_level, head_gain, init_state, init_norm, out_attn, out_rec):
    f32 = jnp.float32
    bf16 = jnp.bfloat16
    positions = jnp.arange(SEQUENCE_TOKENS, dtype=jnp.int32)
    normed = rms_rows(rows_in.astype(f32), in_gain).astype(bf16)
    q_latent = rms_rows(jnp.dot(normed, query_down, preferred_element_type=f32), query_gain).astype(bf16)
    kv_latent = rms_rows(jnp.dot(normed, kv_down, preferred_element_type=f32), kv_gain).astype(bf16)
    key_rope = rotate(jnp.dot(normed, rope_down, preferred_element_type=f32)[:, None, :], positions)[:, 0, :].astype(bf16)
    query_nope = jnp.dot(q_latent, query_nope_up, preferred_element_type=f32).astype(bf16).reshape(SEQUENCE_TOKENS, HA, NOPE)
    query_rope = rotate(jnp.dot(q_latent, query_rope_up, preferred_element_type=f32).reshape(SEQUENCE_TOKENS, HA, ROPE), positions).astype(bf16)
    query_abs = jnp.einsum('thn,khn->thk', query_nope.astype(f32), key_up.astype(f32).reshape(KVL, HA, NOPE)).astype(bf16)
    queries = jnp.concatenate([query_abs, query_rope], axis=-1)
    key_rows = jnp.concatenate([kv_latent, key_rope], axis=-1)
    score_scale = (NOPE + ROPE) ** (-0.5)
    query_block = math.gcd(SEQUENCE_TOKENS, 128)

    def attend_block(block_q):
        rows_q = block_q.reshape(query_block * HA, KVL + ROPE)
        scores = jnp.dot(rows_q, key_rows.T, preferred_element_type=f32) * score_scale
        row_top = lax.optimization_barrier(jnp.max(scores, axis=-1, keepdims=True))
        expo_all = jnp.exp(scores - row_top)
        totals = lax.optimization_barrier(jnp.sum(expo_all, axis=-1, keepdims=True))
        latent = (jnp.dot(expo_all.astype(bf16), kv_latent, preferred_element_type=f32) / totals).astype(bf16)
        return latent.reshape(query_block, HA, KVL)
    attended = lax.map(attend_block, queries.reshape(SEQUENCE_TOKENS // query_block, query_block, HA, KVL + ROPE)).reshape(SEQUENCE_TOKENS, HA, KVL)
    attention_out = jnp.einsum('thk,khv->thv', attended.astype(f32), value_up.astype(f32).reshape(KVL, HA, VH)).astype(bf16).reshape(SEQUENCE_TOKENS, HA * VH)
    rec_q = heads_first(jnp.dot(normed, rec_query, preferred_element_type=f32), MK)
    rec_k = heads_first(jnp.dot(normed, rec_key, preferred_element_type=f32), MK) * MK ** (-0.5)
    rec_v = heads_first(jnp.dot(normed, rec_value, preferred_element_type=f32), MV)
    gate_pre = jnp.einsum('td,dgh->tgh', normed.astype(f32), gate_weight.astype(f32))
    input_fwd = gate_pre[:, 0].T
    keep_fwd = jax.nn.log_sigmoid(gate_pre[:, 1] + forget_level[:, 0]).T
    input_bwd = gate_pre[:, 2].T
    keep_bwd = jax.nn.log_sigmoid(gate_pre[:, 3] + forget_level[:, 1]).T
    zero_heads = jnp.zeros((RECURRENT_HEADS,), f32)
    floor_value = float(SEQUENCE_TOKENS) ** 0.5
    forward_h = recurrence(rec_q, rec_k, rec_v, input_fwd, keep_fwd, init_state[0], init_norm[0], zero_heads, floor_value)
    backward_h = recurrence(rec_q[:, ::-1], rec_k[:, ::-1], rec_v[:, ::-1], input_bwd[:, ::-1], keep_bwd[:, ::-1], init_state[1], init_norm[1], zero_heads, floor_value)[:, ::-1]
    summed = (forward_h + backward_h).transpose(1, 0, 2)
    recurrent_out = rms_rows(summed, head_gain.reshape(RECURRENT_HEADS, MV)).astype(bf16).reshape(SEQUENCE_TOKENS, RECURRENT_HEADS * MV)
    mixed_out = jnp.zeros((SEQUENCE_TOKENS, D), f32)
    for group in range(N_TP):
        att_cols = attention_out[:, group * HAG * VH:(group + 1) * HAG * VH]
        rec_cols = recurrent_out[:, group * HMG * MV:(group + 1) * HMG * MV]
        partial_value = jnp.dot(att_cols, out_attn[group * HAG * VH:(group + 1) * HAG * VH], preferred_element_type=f32)
        partial_value = partial_value + jnp.dot(rec_cols, out_rec[group * HMG * MV:(group + 1) * HMG * MV], preferred_element_type=f32)
        mixed_out = mixed_out + partial_value.astype(bf16).astype(f32)
    return mixed_out.astype(bf16)
```

```python
import functools

import jax
import jax.numpy as jnp
import numpy as np
from jax import lax
from jax.experimental import pallas as pl
from jax.experimental.pallas import tpu as pltpu
from jax.sharding import PartitionSpec as P

EPS = 1e-06
NEG = -(2.0**100)
AUX = 16
F32 = jnp.float32
BF16 = jnp.bfloat16
NT = (((1,), (1,)), ((), ()))


def radices_of(peers):
    first = 2 if peers % 2 == 0 else 1
    rest = peers // first
    radices = [first]
    while rest > 1:
        step = 4 if rest % 4 == 0 else next(p for p in range(2, rest + 1) if rest % p == 0)
        radices.append(step)
        rest //= step
    if len(radices) == 1:
        radices.append(1)
    return radices


def digit_shift(peers, stride, radix, k):
    pairs = []
    for i in range(peers):
        digit = (i // stride) % radix
        pairs.append((i, i + ((digit + k) % radix - digit) * stride))
    return pairs


def dot(a, b):
    return jnp.dot(a, b, preferred_element_type=F32)


def dot_nt(a, b):
    return lax.dot_general(a, b, NT, preferred_element_type=F32)


def dot_split(a, b):
    high = a.astype(BF16)
    low = (a - high.astype(F32)).astype(BF16)
    return dot(high, b) + dot(low, b)


def rms(values, gain):
    return values * lax.rsqrt(jnp.mean(values * values, axis=-1, keepdims=True) + EPS) * gain


def iota2(rows, cols, dim):
    return lax.broadcasted_iota(jnp.int32, (rows, cols), dim)


def turned_rows(weight_t):
    half = weight_t.shape[0] // 2
    return jnp.concatenate([weight_t, -weight_t[half:], weight_t[:half]], axis=0)


def angle_table(ids_ref, cos_base, sin_base, cos_row, sin_row):
    block = ids_ref[1]
    cb, sb = cos_base[pl.ds(block, 1), :], sin_base[pl.ds(block, 1), :]
    cr, sr = cos_row[...], sin_row[...]
    cos, sin = cb * cr - sb * sr, sb * cr + cb * sr
    half = cr.shape[1] // 2
    return jnp.where(iota2(cr.shape[0], cr.shape[1], 1) < half, cos, sin)


def rotated(product, table):
    mixed = product * table
    return mixed + pltpu.roll(mixed, product.shape[1] // 2, 1)


def aux_rows(n_row, peak_row, keep_row):
    high = keep_row.astype(BF16).astype(F32)
    mid = (keep_row - high).astype(BF16).astype(F32)
    low = keep_row - high - mid
    pad = jnp.zeros((AUX - 5, n_row.shape[1]), F32)
    return jnp.concatenate([n_row, peak_row, high, mid, low, pad], axis=0)


def read_state(block):
    c_rows = block.shape[0] - AUX
    block = block.astype(F32)
    aux = block[c_rows:]
    return block[:c_rows], aux[0:1], aux[1:2], aux[2:3] + aux[3:4] + aux[4:5]


def masked(state, use):
    c_part, n_part, peak, keep = state
    return c_part, n_part, jnp.where(use, peak, NEG), jnp.where(use, keep, 0.0)


def chain(states):
    logs = []
    after = None
    for _, _, peak, keep in reversed(states):
        logs.append(peak if after is None else peak + after)
        after = keep if after is None else keep + after
    logs = logs[::-1]
    top = functools.reduce(jnp.maximum, logs)
    return logs, top, after


def weighted(states, logs, top):
    c_sum = n_sum = None
    for (c_part, n_part, _, _), log in zip(states, logs):
        weight = jnp.exp(log - top)
        c_sum = weight * c_part if c_sum is None else c_sum + weight * c_part
        n_sum = weight * n_part if n_sum is None else n_sum + weight * n_part
    return c_sum, n_sum


def joined(states):
    logs, top, keep = chain(states)
    top = top.astype(BF16).astype(F32)
    c_sum, n_sum = weighted(states, logs, top)
    return jnp.concatenate([c_sum, aux_rows(n_sum, top, keep)], axis=0)


def log_sigmoid(x):
    return jnp.minimum(x, 0.0) - jnp.log(1.0 + jnp.exp(-jnp.abs(x)))


def head_kernel(
    ids,
    *refs,
    pieces,
    key_width,
):
    piece_refs = refs[: 2 * pieces]
    (
        in_gain,
        kv_down,
        kv_gain,
        rope_t,
        key_t,
        rec_value,
        gate_t,
        level,
        cos_base,
        sin_base,
        cos_row,
        sin_row,
        message,
        normed_out,
        keys_out,
        values_out,
        rows_out,
        table_out,
        rows,
    ) = refs[2 * pieces :]
    mine = ids[0]
    pair, core = mine // 2, mine % 2
    step = piece_refs[0].shape[0]
    seq = rows.shape[0]
    for k in range(pieces):
        source = lax.rem(pair - k + pieces, pieces) * 2
        rows[pl.ds(pl.multiple_of((source + core) * step, step), step), :] = piece_refs[2 * k][...]
        rows[pl.ds(pl.multiple_of((source + 1 - core) * step, step), step), :] = piece_refs[
            2 * k + 1
        ][...]
    normed = rms(rows[...].astype(F32), in_gain[...]).astype(BF16)
    normed_out[...] = normed
    table = angle_table(ids, cos_base, sin_base, cos_row, sin_row)
    table_out[...] = table
    gates = dot_nt(gate_t[...], normed)
    lat = rms(dot(normed, kv_down[...]), kv_gain[...]).astype(BF16)
    rope = rotated(dot_nt(normed, turned_rows(rope_t[...])), table)
    half = seq // 2
    lanes = iota2(half, rope.shape[1], 1)
    packed = jnp.where(lanes < rope_t.shape[0], rope[:half], rope[half:])
    message[0:seq, :] = lat
    message[seq : seq + half, :] = packed.astype(BF16)

    key_rows = jnp.concatenate([key_t[...], jnp.zeros_like(key_t)], axis=0)
    keys = (dot_nt(normed, key_rows).astype(BF16).astype(F32)) * key_width ** (-0.5)
    keys_out[...] = keys.astype(BF16)
    values = dot(normed, rec_value[...]).astype(BF16)
    values_out[...] = values

    in_f, in_b = gates[0:1], gates[2:3]
    keep_f = log_sigmoid(gates[1:2] + level[0:1])
    keep_b = log_sigmoid(gates[3:4] + level[1:2])
    row_id, col_id = iota2(seq, seq, 0), iota2(seq, seq, 1)
    upper = jnp.where(row_id <= col_id, 1.0, 0.0)
    lower = jnp.where(row_id >= col_id, 1.0, 0.0)
    keeps = jnp.concatenate([keep_f, keep_b, jnp.zeros((6, seq), F32)], axis=0)
    cums = lax.dot_general(
        keeps,
        jnp.concatenate([upper, lower], axis=1),
        (((1,), (0,)), ((), ())),
        precision=lax.Precision.HIGHEST,
        preferred_element_type=F32,
    )
    cum_f, cum_b = cums[0:1, :seq], cums[1:2, seq:]
    all_f, all_b = cum_f[:, seq - 1 : seq], cum_b[:, 0:1]
    rows_out[...] = jnp.concatenate(
        [cum_f, in_f - cum_f, cum_b, in_b - cum_b, jnp.zeros((4, seq), F32)], axis=0
    )
    keys_t = jnp.transpose(keys)[:key_width]
    base = seq + half
    weights = []
    for index, (cum, log_in, total) in enumerate(((cum_f, in_f, all_f), (cum_b, in_b, all_b))):
        logs = total - cum + log_in
        peak = jnp.max(logs, axis=1, keepdims=True).astype(BF16).astype(F32)
        weight = jnp.exp(logs - peak)
        weights.append((weight, peak, total))
    w_f, w_b = weights[0][0], weights[1][0]
    c_both = dot_split(jnp.concatenate([keys_t * w_f, keys_t * w_b], axis=0), values)
    n_both = dot_split(
        jnp.concatenate([w_f, w_b, jnp.zeros((6, seq), F32)], axis=0), keys.astype(BF16)
    )
    for index in range(2):
        _, peak, total = weights[index]
        c_part = c_both[index * key_width : (index + 1) * key_width]
        n_row = n_both[index : index + 1]
        zero = jnp.zeros_like(n_row)
        block = jnp.concatenate([c_part, aux_rows(n_row, zero + peak, zero + total)], axis=0)
        at = base + index * (key_width + AUX)
        message[at : at + key_width + AUX, :] = block.astype(BF16)


def local_kernel(
    normed_ref,
    keys_ref,
    values_ref,
    rows_ref,
    table_ref,
    query_down,
    query_gain,
    nope_up,
    rope_up_t,
    key_up,
    rec_query_t,
    queries_out,
    rec_q_out,
    local_out,
):
    normed = normed_ref[...]
    seq = normed.shape[0]
    query_rows = jnp.concatenate([rec_query_t[...], jnp.zeros_like(rec_query_t)], axis=0)
    rec_q = dot_nt(normed, query_rows).astype(BF16)
    rec_q_out[...] = rec_q
    q_lat = rms(dot(normed, query_down[...]), query_gain[...]).astype(BF16)
    nope = dot(q_lat, nope_up[...]).astype(BF16)
    rope = rotated(dot_nt(q_lat, turned_rows(rope_up_t[...])), table_ref[...])
    lat = dot_nt(nope, key_up[...]).astype(BF16)
    width = rope_up_t.shape[0]
    lanes = iota2(seq, rope.shape[1], 1)
    queries_out[0] = jnp.concatenate([lat, jnp.where(lanes < width, rope, 0.0).astype(BF16)], axis=1)
    queries_out[1] = jnp.concatenate(
        [lat, jnp.where(lanes >= width, rope, 0.0).astype(BF16)], axis=1
    )
    values = values_ref[...]
    wide = jnp.concatenate([values, jnp.ones_like(values)], axis=1)
    products = dot_nt(rec_q, keys_ref[...])
    row_id, col_id = iota2(seq, seq, 0), iota2(seq, seq, 1)
    rows = rows_ref[...]
    for index in range(2):
        cum = jnp.transpose(jnp.broadcast_to(rows[2 * index : 2 * index + 1], (seq, seq)))
        seen = row_id >= col_id if index == 0 else row_id <= col_id
        logs = jnp.where(seen, cum + rows[2 * index + 1 : 2 * index + 2], NEG)
        peak = jnp.max(logs, axis=1, keepdims=True)
        gated = products * jnp.exp(logs - peak)
        sums = dot_split(gated, wide)
        local_out[index, :, 0 : 2 * seq] = sums
        local_out[index, :, 2 * seq : 3 * seq] = jnp.broadcast_to(peak, (seq, seq))
        local_out[index, :, 3 * seq :] = cum


def level_states(ids, slot, radix, fetch):
    digit = ids[slot]
    forward, backward = [], []
    for k in range(radix - 1, 0, -1):
        forward.append(masked(fetch(k, 0), digit >= k))
    for k in range(1, radix):
        backward.append(masked(fetch(k, 1), digit < k))
    return forward, backward


def merge_kernel(ids, *refs, slot, radix, state_rows, last, next_radix):
    prefix_in = refs[0]
    own = refs[1]
    received = (own,) + refs[2 : 1 + radix]
    outs = refs[1 + radix :]
    prefix_out, messages = outs[0], outs[1:]
    kv_rows = own.shape[0] - 2 * state_rows

    def fetch(k, direction):
        at = kv_rows + direction * state_rows
        return read_state(received[k][at : at + state_rows, :])

    forward, backward = level_states(ids, slot, radix, fetch)
    inner_f = read_state(prefix_in[0])
    inner_b = read_state(prefix_in[1])
    prefix_out[0] = joined(forward + [inner_f])
    prefix_out[1] = joined(backward + [inner_b])
    digit = ids[slot]
    late_f = [masked(fetch(k, 0), digit < k) for k in range(radix - 1, 0, -1)]
    late_b = [masked(fetch(k, 1), digit >= k) for k in range(1, radix)]
    total_f = joined(forward + [fetch(0, 0)] + late_f).astype(BF16)
    total_b = joined(backward + [fetch(0, 1)] + late_b).astype(BF16)
    part = kv_rows // 3
    for number, message in enumerate(messages):
        for section in range(3):
            for k in range(radix):
                to = (section * radix + k) * part
                message[to : to + part, :] = received[k][section * part : (section + 1) * part, :]
        at = radix * kv_rows
        if last:
            ahead = ids[slot + 1] + number + 1 < next_radix
            message[at : at + state_rows, :] = jnp.where(ahead, total_f, total_b)
        else:
            message[at : at + state_rows, :] = total_f
            message[at + state_rows : at + 2 * state_rows, :] = total_b


def mix_kernel(
    ids,
    *refs,
    slot,
    radix,
    state_rows,
    pieces,
    floor_value,
    score_scale,
):
    received = refs[:radix]
    (
        prefix,
        queries,
        rec_q_ref,
        local,
        value_up,
        head_gain,
        init_state,
        init_norm,
        out_attn,
        out_rec,
        send_out,
        keep_out,
        heads,
    ) = refs[radix:]
    kv_rows = received[0].shape[0] - state_rows
    part = kv_rows // 3
    seq = rec_q_ref.shape[0]

    scores = []
    for message in received:
        rope = message[2 * part : 3 * part, :]
        for section in range(2):
            lat = message[section * part : (section + 1) * part, :]
            scores.append(
                dot_nt(queries[section], jnp.concatenate([lat, rope], axis=1)) * score_scale
            )
    top = functools.reduce(jnp.maximum, [jnp.max(s, axis=1, keepdims=True) for s in scores])
    mass = accum = None
    for index, part_scores in enumerate(scores):
        expo = jnp.exp(part_scores - top)
        section = index % 2
        lat = received[index // 2][section * part : (section + 1) * part, :]
        gain = dot(expo.astype(BF16), lat)
        total = jnp.sum(expo, axis=1, keepdims=True)
        accum = gain if accum is None else accum + gain
        mass = total if mass is None else mass + total
    attended = (accum / mass).astype(BF16)
    heads[:, 0 : value_up.shape[1]] = dot(attended, value_up[...]).astype(BF16)

    def fetch(k, direction):
        return read_state(received[k][kv_rows : kv_rows + state_rows, :])

    sides = level_states(ids, slot, radix, fetch)
    rec_q = rec_q_ref[...]
    summed = None
    for index in range(2):
        inner = read_state(prefix[index])
        zero = jnp.zeros_like(inner[1])
        first = (init_state[index], init_norm[index : index + 1], zero, zero)
        states = [first] + sides[index] + [inner]
        logs, start_top, _ = chain(states)
        c_start, n_start = weighted(states, logs, start_top)
        pad = jnp.zeros((rec_q.shape[1] - c_start.shape[0], c_start.shape[1]), F32)
        from_start = lax.dot_general(
            rec_q.astype(F32),
            jnp.concatenate([c_start, pad], axis=0),
            (((1,), (0,)), ((), ())),
            precision=lax.Precision.HIGHEST,
            preferred_element_type=F32,
        )
        norm_start = jnp.sum(rec_q.astype(F32) * n_start, axis=1, keepdims=True)
        numer = local[index, :, 0:seq]
        denom = local[index, :, seq : 2 * seq]
        peak = local[index, :, 2 * seq : 3 * seq]
        carry = local[index, :, 3 * seq :] + start_top
        row_max = jnp.maximum(peak, carry)
        here, there = jnp.exp(peak - row_max), jnp.exp(carry - row_max)
        numer = here * numer + there * from_start
        denom = here * denom + there * norm_start
        result = numer / jnp.maximum(jnp.abs(denom), floor_value * jnp.exp(-row_max))
        summed = result if summed is None else summed + result
    heads[:, value_up.shape[1] :] = rms(summed, head_gain[...]).astype(BF16)

    mine = ids[0]
    pair, core = mine // 2, mine % 2
    step = seq // (2 * pieces)
    split = value_up.shape[1]
    for side, out in ((1 - core, None), (core, keep_out)):
        rows = []
        for k in range(pieces):
            owner = lax.rem(pair + k, pieces) * 2 + side
            rows.append(heads[pl.ds(pl.multiple_of(owner * step, step), step), :])
        rows = jnp.concatenate(rows, axis=0)
        if out is None:
            send_out[...] = (
                dot(rows[:, :split], out_attn[...]) + dot(rows[:, split:], out_rec[...])
            ).astype(BF16)
        else:
            out[...] = rows


def project_kernel(rows, out_attn, out_rec, out):
    split = out_attn.shape[0]
    out[...] = (dot(rows[:, :split], out_attn[...]) + dot(rows[:, split:], out_rec[...])).astype(
        BF16
    )


def call(kernel, outs, inputs, name, scratch=(), ids=True, limit=16 << 20):
    vmem = pl.BlockSpec(memory_space=pltpu.VMEM)
    in_specs = [vmem] * len(inputs)
    if ids:
        in_specs[0] = pl.BlockSpec(memory_space=pltpu.SMEM)
    return pl.pallas_call(
        kernel,
        out_shape=[jax.ShapeDtypeStruct(shape, dtype) for shape, dtype in outs],
        in_specs=in_specs,
        out_specs=[vmem] * len(outs),
        scratch_shapes=scratch,
        name=name,
        compiler_params=pltpu.CompilerParams(vmem_limit_bytes=limit),
    )(*inputs)


def shards(
    rows_in,
    in_gain,
    query_down,
    query_gain,
    kv_down,
    kv_gain,
    rope_down,
    query_nope_up,
    query_rope_up,
    key_up,
    value_up,
    rec_query,
    rec_key,
    rec_value,
    gate_weight,
    forget_level,
    head_gain,
    init_state,
    init_norm,
    out_attn,
    out_rec,
):
    peers, lanes = lax.axis_size("sp"), lax.axis_size("tp")
    block, mine = lax.axis_index("sp"), lax.axis_index("tp")
    seq = forget_level.shape[0]
    width = rows_in.shape[1]
    nope, rope = key_up.shape[1], rope_down.shape[1]
    key_width, value_width = init_state.shape[2], init_state.shape[3]
    pieces = lanes // 2
    radices = radices_of(peers)
    strides = [int(np.prod(radices[:i])) for i in range(len(radices))]
    divide = np.array([1, 1] + strides, np.int32)
    modulo = np.array([lanes, peers] + radices, np.int32)
    first = np.arange(len(divide)) == 0
    ids = (jnp.where(first, mine, block).astype(jnp.int32) // divide) % modulo

    partner = [(i, i ^ 1) for i in range(lanes)]
    ring = [[(i, (i + 2 * k) % lanes) for i in range(lanes)] for k in range(pieces)]

    gathered = [rows_in] + [lax.ppermute(rows_in, "tp", ring[k]) for k in range(1, pieces)]
    row_pieces = []
    for piece in gathered:
        row_pieces += [piece, lax.ppermute(piece, "tp", partner)]

    freq = 10000.0 ** (-np.arange(rope // 2, dtype=np.float64) / (rope // 2))
    freq = np.tile(freq, 4)[None, :]
    base = np.arange(peers, dtype=np.float64)[:, None] * seq * freq
    within = np.arange(seq, dtype=np.float64)[:, None] * freq
    tables = [np.cos(base), np.sin(base), np.cos(within), np.sin(within)]
    tables = [jnp.asarray(table.astype(np.float32)) for table in tables]

    state_rows = key_width + AUX
    kv_rows = seq + seq // 2
    message, normed, keys, values, gate_rows, table = call(
        functools.partial(head_kernel, pieces=pieces, key_width=key_width),
        [
            ((kv_rows + 2 * state_rows, value_width), BF16),
            ((seq, width), BF16),
            ((seq, 2 * key_width), BF16),
            ((seq, value_width), BF16),
            ((8, seq), F32),
            ((seq, 2 * rope), F32),
        ],
        [ids]
        + row_pieces
        + [
            in_gain[None, :],
            kv_down,
            kv_gain[None, :],
            rope_down.T,
            rec_key.T,
            rec_value,
            gate_weight[:, :, 0].T,
            forget_level[:, :, 0].T,
        ]
        + tables,
        "head",
        scratch=[pltpu.VMEM((seq, width), BF16)],
    )
    queries, rec_q, local = call(
        local_kernel,
        [
            ((2, seq, 2 * value_width), BF16),
            ((seq, 2 * key_width), BF16),
            ((2, seq, 4 * seq), F32),
        ],
        [
            normed,
            keys,
            values,
            gate_rows,
            table,
            query_down,
            query_gain[None, :],
            query_nope_up,
            query_rope_up.T,
            key_up,
            rec_query.T,
        ],
        "local",
        ids=False,
    )

    blank = np.zeros((2, state_rows, value_width), np.float32)
    blank[:, key_width + 1] = NEG
    prefix = jnp.asarray(blank)
    for level, radix in enumerate(radices[:-1]):
        received = [
            lax.ppermute(message, "sp", digit_shift(peers, strides[level], radix, k))
            for k in range(1, radix)
        ]
        last = level == len(radices) - 2
        kv_rows *= radix
        count = radices[-1] - 1 if last else 1
        out_rows = kv_rows + (1 if last else 2) * state_rows
        prefix, *messages = call(
            functools.partial(
                merge_kernel,
                slot=2 + level,
                radix=radix,
                state_rows=state_rows,
                last=last,
                next_radix=radices[level + 1],
            ),
            [((2, state_rows, value_width), F32)]
            + [((out_rows, value_width), BF16)] * max(count, 1),
            [ids, prefix, message] + received,
            "merge",
            limit=(16 << 20) if peers <= 16 else (40 << 20),
        )
        message = messages[0]
    level, radix = len(radices) - 1, radices[-1]
    received = [
        lax.ppermute(messages[k - 1], "sp", digit_shift(peers, strides[level], radix, k))
        for k in range(1, radix)
    ]
    send, kept = call(
        functools.partial(
            mix_kernel,
            slot=2 + level,
            radix=radix,
            state_rows=state_rows,
            pieces=pieces,
            floor_value=float(seq * peers) ** 0.5,
            score_scale=(nope + rope) ** (-0.5),
        ),
        [((seq // 2, width), BF16), ((seq // 2, nope + value_width), BF16)],
        [ids, message]
        + received
        + [
            prefix,
            queries,
            rec_q,
            local,
            value_up,
            head_gain[None, :],
            init_state[:, 0],
            jnp.pad(init_norm[:, 0], ((0, 0), (0, value_width - key_width))),
            out_attn,
            out_rec,
        ],
        "mix",
        scratch=[pltpu.VMEM((seq, value_up.shape[1] + value_width), BF16)],
        limit=(16 << 20) if peers <= 16 else (56 << 20),
    )
    other = lax.ppermute(send, "tp", partner)
    (ours,) = call(
        project_kernel,
        [((seq // 2, width), BF16)],
        [kept, out_attn, out_rec],
        "project",
        ids=False,
    )
    both = ours.astype(F32) + other.astype(F32)
    step = seq // lanes
    total = both[:step]
    for k in range(1, pieces):
        piece = both[k * step : (k + 1) * step].astype(BF16)
        total = total + lax.ppermute(piece, "tp", ring[k]).astype(F32)
    return total.astype(BF16)


def solution(mesh):
    in_specs = (
        P(("sp", "tp"), None),
        P(),
        P(),
        P(),
        P(),
        P(),
        P(),
        P(None, "tp"),
        P(None, "tp"),
        P(None, "tp"),
        P(None, "tp"),
        P(None, "tp"),
        P(None, "tp"),
        P(None, "tp"),
        P(None, None, "tp"),
        P("sp", None, "tp"),
        P("tp"),
        P(None, "tp", None, None),
        P(None, "tp", None),
        P("tp", None),
        P("tp", None),
    )
    out_specs = P(("sp", "tp"), None)
    return jax.shard_map(shards, mesh=mesh, in_specs=in_specs, out_specs=out_specs, check_vma=False)
```

```python
import functools

import jax
import jax.numpy as jnp
import numpy as np
from jax import lax
from jax.experimental import pallas as pl
from jax.experimental.pallas import tpu as pltpu
from jax.sharding import PartitionSpec as P

EPS = 1e-06
NEG = -(2.0**100)
AUX = 16
F32 = jnp.float32
BF16 = jnp.bfloat16
NT = (((1,), (1,)), ((), ()))


def radices_of(peers):
    first = 2 if peers % 2 == 0 else 1
    rest = peers // first
    radices = [first]
    while rest > 1:
        step = 4 if rest % 4 == 0 else next(p for p in range(2, rest + 1) if rest % p == 0)
        radices.append(step)
        rest //= step
    if len(radices) == 1:
        radices.append(1)
    return radices


def digit_shift(peers, stride, radix, k):
    pairs = []
    for i in range(peers):
        digit = (i // stride) % radix
        pairs.append((i, i + ((digit + k) % radix - digit) * stride))
    return pairs


def dot(a, b):
    return jnp.dot(a, b, preferred_element_type=F32)


def dot_nt(a, b):
    return lax.dot_general(a, b, NT, preferred_element_type=F32)


def dot_split(a, b):
    high = a.astype(BF16)
    low = (a - high.astype(F32)).astype(BF16)
    return dot(high, b) + dot(low, b)


def rms(values, gain):
    return values * lax.rsqrt(jnp.mean(values * values, axis=-1, keepdims=True) + EPS) * gain


def iota2(rows, cols, dim):
    return lax.broadcasted_iota(jnp.int32, (rows, cols), dim)


def turned_rows(weight_t):
    half = weight_t.shape[0] // 2
    return jnp.concatenate([weight_t, -weight_t[half:], weight_t[:half]], axis=0)


def angle_table(ids_ref, cos_base, sin_base, cos_row, sin_row):
    block = ids_ref[1]
    cb, sb = cos_base[pl.ds(block, 1), :], sin_base[pl.ds(block, 1), :]
    cr, sr = cos_row[...], sin_row[...]
    cos, sin = cb * cr - sb * sr, sb * cr + cb * sr
    half = cr.shape[1] // 2
    return jnp.where(iota2(cr.shape[0], cr.shape[1], 1) < half, cos, sin)


def rotated(product, table):
    mixed = product * table
    return mixed + pltpu.roll(mixed, product.shape[1] // 2, 1)


def aux_rows(n_row, peak_row, keep_row):
    high = keep_row.astype(BF16).astype(F32)
    mid = (keep_row - high).astype(BF16).astype(F32)
    low = keep_row - high - mid
    pad = jnp.zeros((AUX - 5, n_row.shape[1]), F32)
    return jnp.concatenate([n_row, peak_row, high, mid, low, pad], axis=0)


def read_state(block):
    c_rows = block.shape[0] - AUX
    block = block.astype(F32)
    aux = block[c_rows:]
    return block[:c_rows], aux[0:1], aux[1:2], aux[2:3] + aux[3:4] + aux[4:5]


def masked(state, use):
    c_part, n_part, peak, keep = state
    return c_part, n_part, jnp.where(use, peak, NEG), jnp.where(use, keep, 0.0)


def chain(states):
    logs = []
    after = None
    for _, _, peak, keep in reversed(states):
        logs.append(peak if after is None else peak + after)
        after = keep if after is None else keep + after
    logs = logs[::-1]
    top = functools.reduce(jnp.maximum, logs)
    return logs, top, after


def weighted(states, logs, top):
    c_sum = n_sum = None
    for (c_part, n_part, _, _), log in zip(states, logs):
        weight = jnp.exp(log - top)
        c_sum = weight * c_part if c_sum is None else c_sum + weight * c_part
        n_sum = weight * n_part if n_sum is None else n_sum + weight * n_part
    return c_sum, n_sum


def joined(states):
    logs, top, keep = chain(states)
    top = top.astype(BF16).astype(F32)
    c_sum, n_sum = weighted(states, logs, top)
    return jnp.concatenate([c_sum, aux_rows(n_sum, top, keep)], axis=0)


def log_sigmoid(x):
    return jnp.minimum(x, 0.0) - jnp.log(1.0 + jnp.exp(-jnp.abs(x)))


def head_kernel(
    ids,
    *refs,
    pieces,
    key_width,
):
    piece_refs = refs[: 2 * pieces]
    (
        in_gain,
        kv_down,
        kv_gain,
        rope_t,
        key_t,
        rec_value,
        gate_t,
        level,
        cos_base,
        sin_base,
        cos_row,
        sin_row,
        message,
        normed_out,
        keys_out,
        values_out,
        rows_out,
        table_out,
        rows,
    ) = refs[2 * pieces :]
    mine = ids[0]
    pair, core = mine // 2, mine % 2
    step = piece_refs[0].shape[0]
    seq = rows.shape[0]
    for k in range(pieces):
        source = lax.rem(pair - k + pieces, pieces) * 2
        rows[pl.ds(pl.multiple_of((source + core) * step, step), step), :] = piece_refs[2 * k][...]
        rows[pl.ds(pl.multiple_of((source + 1 - core) * step, step), step), :] = piece_refs[
            2 * k + 1
        ][...]
    normed = rms(rows[...].astype(F32), in_gain[...]).astype(BF16)
    normed_out[...] = normed
    table = angle_table(ids, cos_base, sin_base, cos_row, sin_row)
    table_out[...] = table
    gates = dot_nt(gate_t[...], normed)
    lat = rms(dot(normed, kv_down[...]), kv_gain[...]).astype(BF16)
    rope = rotated(dot_nt(normed, turned_rows(rope_t[...])), table)
    half = seq // 2
    quarter = half // 2
    lat = jnp.where(core == 0, lat[:half], lat[half:])
    rope = jnp.where(core == 0, rope[:half], rope[half:])
    lanes = iota2(quarter, rope.shape[1], 1)
    packed = jnp.where(lanes < rope_t.shape[0], rope[:quarter], rope[quarter:])
    message[0:half, :] = lat
    message[half : half + quarter, :] = packed.astype(BF16)

    key_rows = jnp.concatenate([key_t[...], jnp.zeros_like(key_t)], axis=0)
    keys = (dot_nt(normed, key_rows).astype(BF16).astype(F32)) * key_width ** (-0.5)
    keys_out[...] = keys.astype(BF16)
    values = dot(normed, rec_value[...]).astype(BF16)
    values_out[...] = values

    in_f, in_b = gates[0:1], gates[2:3]
    keep_f = log_sigmoid(gates[1:2] + level[0:1])
    keep_b = log_sigmoid(gates[3:4] + level[1:2])
    row_id, col_id = iota2(seq, seq, 0), iota2(seq, seq, 1)
    upper = jnp.where(row_id <= col_id, 1.0, 0.0)
    lower = jnp.where(row_id >= col_id, 1.0, 0.0)
    keeps = jnp.concatenate([keep_f, keep_b, jnp.zeros((6, seq), F32)], axis=0)
    cums = lax.dot_general(
        keeps,
        jnp.concatenate([upper, lower], axis=1),
        (((1,), (0,)), ((), ())),
        precision=lax.Precision.HIGHEST,
        preferred_element_type=F32,
    )
    cum_f, cum_b = cums[0:1, :seq], cums[1:2, seq:]
    all_f, all_b = cum_f[:, seq - 1 : seq], cum_b[:, 0:1]
    rows_out[...] = jnp.concatenate(
        [cum_f, in_f - cum_f, cum_b, in_b - cum_b, jnp.zeros((4, seq), F32)], axis=0
    )
    keys_t = jnp.transpose(keys)[:key_width]
    base = half + quarter
    weights = []
    for index, (cum, log_in, total) in enumerate(((cum_f, in_f, all_f), (cum_b, in_b, all_b))):
        logs = total - cum + log_in
        peak = jnp.max(logs, axis=1, keepdims=True).astype(BF16).astype(F32)
        weight = jnp.exp(logs - peak)
        weights.append((weight, peak, total))
    w_f, w_b = weights[0][0], weights[1][0]
    c_both = dot_split(jnp.concatenate([keys_t * w_f, keys_t * w_b], axis=0), values)
    n_both = dot_split(
        jnp.concatenate([w_f, w_b, jnp.zeros((6, seq), F32)], axis=0), keys.astype(BF16)
    )
    for index in range(2):
        _, peak, total = weights[index]
        c_part = c_both[index * key_width : (index + 1) * key_width]
        n_row = n_both[index : index + 1]
        zero = jnp.zeros_like(n_row)
        block = jnp.concatenate([c_part, aux_rows(n_row, zero + peak, zero + total)], axis=0)
        at = base + index * (key_width + AUX)
        message[at : at + key_width + AUX, :] = block.astype(BF16)


def local_kernel(
    normed_ref,
    keys_ref,
    values_ref,
    rows_ref,
    table_ref,
    query_down,
    query_gain,
    nope_up,
    rope_up_t,
    key_up,
    rec_query_t,
    queries_out,
    rec_q_out,
    local_out,
):
    normed = normed_ref[...]
    seq = normed.shape[0]
    query_rows = jnp.concatenate([rec_query_t[...], jnp.zeros_like(rec_query_t)], axis=0)
    rec_q = dot_nt(normed, query_rows).astype(BF16)
    rec_q_out[...] = rec_q
    q_lat = rms(dot(normed, query_down[...]), query_gain[...]).astype(BF16)
    nope = dot(q_lat, nope_up[...]).astype(BF16)
    rope = rotated(dot_nt(q_lat, turned_rows(rope_up_t[...])), table_ref[...])
    lat = dot_nt(nope, key_up[...]).astype(BF16)
    width = rope_up_t.shape[0]
    lanes = iota2(seq, rope.shape[1], 1)
    queries_out[0] = jnp.concatenate([lat, jnp.where(lanes < width, rope, 0.0).astype(BF16)], axis=1)
    queries_out[1] = jnp.concatenate(
        [lat, jnp.where(lanes >= width, rope, 0.0).astype(BF16)], axis=1
    )
    values = values_ref[...]
    wide = jnp.concatenate([values, jnp.ones_like(values)], axis=1)
    products = dot_nt(rec_q, keys_ref[...])
    row_id, col_id = iota2(seq, seq, 0), iota2(seq, seq, 1)
    rows = rows_ref[...]
    for index in range(2):
        cum = jnp.transpose(jnp.broadcast_to(rows[2 * index : 2 * index + 1], (seq, seq)))
        seen = row_id >= col_id if index == 0 else row_id <= col_id
        logs = jnp.where(seen, cum + rows[2 * index + 1 : 2 * index + 2], NEG)
        peak = jnp.max(logs, axis=1, keepdims=True)
        gated = products * jnp.exp(logs - peak)
        sums = dot_split(gated, wide)
        local_out[index, :, 0 : 2 * seq] = sums
        local_out[index, :, 2 * seq : 3 * seq] = jnp.broadcast_to(peak, (seq, seq))
        local_out[index, :, 3 * seq :] = cum


def level_states(ids, slot, radix, fetch):
    digit = ids[slot]
    forward, backward = [], []
    for k in range(radix - 1, 0, -1):
        forward.append(masked(fetch(k, 0), digit >= k))
    for k in range(1, radix):
        backward.append(masked(fetch(k, 1), digit < k))
    return forward, backward


def merge_kernel(ids, *refs, slot, radix, state_rows, last, next_radix):
    prefix_in = refs[0]
    own = refs[1]
    received = (own,) + refs[2 : 1 + radix]
    outs = refs[1 + radix :]
    prefix_out, messages = outs[0], outs[1:]
    kv_rows = own.shape[0] - 2 * state_rows

    def fetch(k, direction):
        at = kv_rows + direction * state_rows
        return read_state(received[k][at : at + state_rows, :])

    forward, backward = level_states(ids, slot, radix, fetch)
    inner_f = read_state(prefix_in[0])
    inner_b = read_state(prefix_in[1])
    prefix_out[0] = joined(forward + [inner_f])
    prefix_out[1] = joined(backward + [inner_b])
    digit = ids[slot]
    late_f = [masked(fetch(k, 0), digit < k) for k in range(radix - 1, 0, -1)]
    late_b = [masked(fetch(k, 1), digit >= k) for k in range(1, radix)]
    total_f = joined(forward + [fetch(0, 0)] + late_f).astype(BF16)
    total_b = joined(backward + [fetch(0, 1)] + late_b).astype(BF16)
    part = kv_rows // 3
    for number, message in enumerate(messages):
        for section in range(3):
            for k in range(radix):
                to = (section * radix + k) * part
                message[to : to + part, :] = received[k][section * part : (section + 1) * part, :]
        at = radix * kv_rows
        if last:
            ahead = ids[slot + 1] + number + 1 < next_radix
            message[at : at + state_rows, :] = jnp.where(ahead, total_f, total_b)
        else:
            message[at : at + state_rows, :] = total_f
            message[at + state_rows : at + 2 * state_rows, :] = total_b


def load_kernel(*refs):
    count = (len(refs) - 1) // 2
    sems = refs[-1]
    copies = [
        pltpu.make_async_copy(refs[i], refs[count + i], sems.at[i]) for i in range(count)
    ]
    for copy in copies:
        copy.start()
    for copy in copies:
        copy.wait()


def pack_kernel(*refs):
    received, out = refs[1:-1], refs[-1]
    rows = out.shape[0] // len(received)
    for k, message in enumerate(received):
        out[k * rows : (k + 1) * rows, :] = message[0:rows, :]


def recur_kernel(
    ids,
    *refs,
    slot,
    radix,
    state_rows,
    floor_value,
):
    received = refs[:radix]
    prefix, rec_q_ref, local, head_gain, init_state, init_norm, out = refs[radix:]
    kv_rows = received[0].shape[0] - state_rows
    seq = rec_q_ref.shape[0]

    def fetch(k, direction):
        return read_state(received[k][kv_rows : kv_rows + state_rows, :])

    sides = level_states(ids, slot, radix, fetch)
    rec_q = rec_q_ref[...]
    summed = None
    for index in range(2):
        inner = read_state(prefix[index])
        zero = jnp.zeros_like(inner[1])
        first = (init_state[index], init_norm[index : index + 1], zero, zero)
        states = [first] + sides[index] + [inner]
        logs, start_top, _ = chain(states)
        c_start, n_start = weighted(states, logs, start_top)
        pad = jnp.zeros((rec_q.shape[1] - c_start.shape[0], c_start.shape[1]), F32)
        from_start = lax.dot_general(
            rec_q.astype(F32),
            jnp.concatenate([c_start, pad], axis=0),
            (((1,), (0,)), ((), ())),
            precision=lax.Precision.HIGHEST,
            preferred_element_type=F32,
        )
        norm_start = jnp.sum(rec_q.astype(F32) * n_start, axis=1, keepdims=True)
        numer = local[index, :, 0:seq]
        denom = local[index, :, seq : 2 * seq]
        peak = local[index, :, 2 * seq : 3 * seq]
        carry = local[index, :, 3 * seq :] + start_top
        row_max = jnp.maximum(peak, carry)
        here, there = jnp.exp(peak - row_max), jnp.exp(carry - row_max)
        numer = here * numer + there * from_start
        denom = here * denom + there * norm_start
        result = numer / jnp.maximum(jnp.abs(denom), floor_value * jnp.exp(-row_max))
        summed = result if summed is None else summed + result
    out[...] = rms(summed, head_gain[...]).astype(BF16)


def mix_kernel(
    ids,
    own_keys,
    other_keys,
    queries,
    recurrent,
    value_up,
    out_attn,
    out_rec,
    send_out,
    keep_out,
    heads,
    *,
    groups,
    pieces,
    score_scale,
):
    seq = recurrent.shape[0]
    rows = own_keys.shape[0] // groups
    part = rows // 3
    scores, lats = [], []
    for keys in (own_keys, other_keys):
        for group in range(groups):
            at = group * rows
            rope = keys[at + 2 * part : at + 3 * part, :]
            for section in range(2):
                lat = keys[at + section * part : at + (section + 1) * part, :]
                lats.append(lat)
                scores.append(
                    dot_nt(queries[section], jnp.concatenate([lat, rope], axis=1)) * score_scale
                )
    top = functools.reduce(jnp.maximum, [jnp.max(s, axis=1, keepdims=True) for s in scores])
    mass = accum = None
    for part_scores, lat in zip(scores, lats):
        expo = jnp.exp(part_scores - top)
        gain = dot(expo.astype(BF16), lat)
        total = jnp.sum(expo, axis=1, keepdims=True)
        accum = gain if accum is None else accum + gain
        mass = total if mass is None else mass + total
    attended = (accum / mass).astype(BF16)
    split = value_up.shape[1]
    heads[:, 0:split] = dot(attended, value_up[...]).astype(BF16)
    heads[:, split:] = recurrent[...]

    mine = ids[0]
    pair, core = mine // 2, mine % 2
    step = seq // (2 * pieces)
    for side, out in ((1 - core, None), (core, keep_out)):
        rows = []
        for k in range(pieces):
            owner = lax.rem(pair + k, pieces) * 2 + side
            rows.append(heads[pl.ds(pl.multiple_of(owner * step, step), step), :])
        rows = jnp.concatenate(rows, axis=0)
        if out is None:
            send_out[...] = (
                dot(rows[:, :split], out_attn[...]) + dot(rows[:, split:], out_rec[...])
            ).astype(BF16)
        else:
            out[...] = rows


def project_kernel(rows, out_attn, out_rec, out):
    split = out_attn.shape[0]
    out[...] = (dot(rows[:, :split], out_attn[...]) + dot(rows[:, split:], out_rec[...])).astype(
        BF16
    )


def call(kernel, outs, inputs, name, scratch=(), ids=True, limit=16 << 20, cost=None):
    vmem = pl.BlockSpec(memory_space=pltpu.VMEM)
    in_specs = [vmem] * len(inputs)
    if ids:
        in_specs[0] = pl.BlockSpec(memory_space=pltpu.SMEM)
    return pl.pallas_call(
        kernel,
        out_shape=[jax.ShapeDtypeStruct(shape, dtype) for shape, dtype in outs],
        in_specs=in_specs,
        out_specs=[vmem] * len(outs),
        scratch_shapes=scratch,
        name=name,
        cost_estimate=cost,
        compiler_params=pltpu.CompilerParams(vmem_limit_bytes=limit),
    )(*inputs)


def shards(
    rows_in,
    in_gain,
    query_down,
    query_gain,
    kv_down,
    kv_gain,
    rope_down,
    query_nope_up,
    query_rope_up,
    key_up,
    value_up,
    rec_query,
    rec_key,
    rec_value,
    gate_weight,
    forget_level,
    head_gain,
    init_state,
    init_norm,
    out_attn,
    out_rec,
):
    peers, lanes = lax.axis_size("sp"), lax.axis_size("tp")
    block, mine = lax.axis_index("sp"), lax.axis_index("tp")
    seq = forget_level.shape[0]
    width = rows_in.shape[1]
    nope, rope = key_up.shape[1], rope_down.shape[1]
    key_width, value_width = init_state.shape[2], init_state.shape[3]
    pieces = lanes // 2
    radices = radices_of(peers)
    strides = [int(np.prod(radices[:i])) for i in range(len(radices))]
    divide = np.array([1, 1] + strides, np.int32)
    modulo = np.array([lanes, peers] + radices, np.int32)
    first = np.arange(len(divide)) == 0
    ids = (jnp.where(first, mine, block).astype(jnp.int32) // divide) % modulo

    partner = [(i, i ^ 1) for i in range(lanes)]
    ring = [[(i, (i + 2 * k) % lanes) for i in range(lanes)] for k in range(pieces)]

    gathered = [rows_in] + [lax.ppermute(rows_in, "tp", ring[k]) for k in range(1, pieces)]
    row_pieces = []
    for piece in gathered:
        row_pieces += [piece, lax.ppermute(piece, "tp", partner)]

    freq = 10000.0 ** (-np.arange(rope // 2, dtype=np.float64) / (rope // 2))
    freq = np.tile(freq, 4)[None, :]
    base = np.arange(peers, dtype=np.float64)[:, None] * seq * freq
    within = np.arange(seq, dtype=np.float64)[:, None] * freq
    tables = [np.cos(base), np.sin(base), np.cos(within), np.sin(within)]
    tables = [jnp.asarray(table.astype(np.float32)) for table in tables]

    held = [
        in_gain[None, :],
        kv_down,
        kv_gain[None, :],
        rope_down.T,
        rec_key.T,
        rec_value,
        gate_weight[:, :, 0].T,
        forget_level[:, :, 0].T,
        *tables,
        query_down,
        query_gain[None, :],
        query_nope_up,
        query_rope_up.T,
        key_up,
        rec_query.T,
        value_up,
        head_gain[None, :],
        init_state[:, 0],
        out_attn,
        out_rec,
    ]
    held = list(
        pl.pallas_call(
            load_kernel,
            out_shape=[pltpu.VMEM(array.shape, array.dtype) for array in held],
            in_specs=[pl.BlockSpec(memory_space=pltpu.HBM)] * len(held),
            out_specs=[pl.BlockSpec(memory_space=pltpu.VMEM)] * len(held),
            scratch_shapes=[pltpu.SemaphoreType.DMA((len(held),))],
            name="load",
            cost_estimate=pl.CostEstimate(flops=10**8, bytes_accessed=1 << 22, transcendentals=0),
            compiler_params=pltpu.CompilerParams(vmem_limit_bytes=16 << 20),
        )(*[pltpu.with_memory_space_constraint(array, pltpu.HBM) for array in held])
    )
    head_args, local_args = held[:12], held[12:18]
    value_up, head_gain, init_state, out_attn, out_rec = held[18:]

    state_rows = key_width + AUX
    kv_rows = seq // 2 + seq // 4
    message, normed, keys, values, gate_rows, table = call(
        functools.partial(head_kernel, pieces=pieces, key_width=key_width),
        [
            ((kv_rows + 2 * state_rows, value_width), BF16),
            ((seq, width), BF16),
            ((seq, 2 * key_width), BF16),
            ((seq, value_width), BF16),
            ((8, seq), F32),
            ((seq, 2 * rope), F32),
        ],
        [ids]
        + row_pieces
        + head_args,
        "head",
        scratch=[pltpu.VMEM((seq, width), BF16)],
    )
    queries, rec_q, local = call(
        local_kernel,
        [
            ((2, seq, 2 * value_width), BF16),
            ((seq, 2 * key_width), BF16),
            ((2, seq, 4 * seq), F32),
        ],
        [
            normed,
            keys,
            values,
            gate_rows,
            table,
            *local_args,
        ],
        "local",
        ids=False,
    )

    blank = np.zeros((2, state_rows, value_width), np.float32)
    blank[:, key_width + 1] = NEG
    prefix = jnp.asarray(blank)
    wide = (16 << 20) if peers <= 16 else (40 << 20)
    for level, radix in enumerate(radices[:-1]):
        received = [
            lax.ppermute(message, "sp", digit_shift(peers, strides[level], radix, k))
            for k in range(1, radix)
        ]
        last = level == len(radices) - 2
        kv_rows *= radix
        count = radices[-1] - 1 if last else 1
        out_rows = kv_rows + (1 if last else 2) * state_rows
        prefix, *messages = call(
            functools.partial(
                merge_kernel,
                slot=2 + level,
                radix=radix,
                state_rows=state_rows,
                last=last,
                next_radix=radices[level + 1],
            ),
            [((2, state_rows, value_width), F32)]
            + [((out_rows, value_width), BF16)] * max(count, 1),
            [ids, prefix, message] + received,
            "merge",
            limit=wide,
        )
        message = messages[0]
    level, radix = len(radices) - 1, radices[-1]
    received = [
        lax.ppermute(messages[k - 1], "sp", digit_shift(peers, strides[level], radix, k))
        for k in range(1, radix)
    ]
    (packed,) = call(
        pack_kernel,
        [((radix * kv_rows, value_width), BF16)],
        [rec_q, message] + received,
        "pack",
        ids=False,
        limit=wide,
    )
    swapped = lax.ppermute(packed, "tp", partner)
    (recurrent,) = call(
        functools.partial(
            recur_kernel,
            slot=2 + level,
            radix=radix,
            state_rows=state_rows,
            floor_value=float(seq * peers) ** 0.5,
        ),
        [((seq, value_width), BF16)],
        [ids, message]
        + received
        + [
            prefix,
            rec_q,
            local,
            head_gain,
            init_state,
            jnp.pad(init_norm[:, 0], ((0, 0), (0, value_width - key_width))),
        ],
        "recur",
        limit=wide,
        cost=pl.CostEstimate(flops=10**8, bytes_accessed=1 << 20, transcendentals=0),
    )
    send, kept = call(
        functools.partial(
            mix_kernel,
            groups=radix,
            pieces=pieces,
            score_scale=(nope + rope) ** (-0.5),
        ),
        [((seq // 2, width), BF16), ((seq // 2, nope + value_width), BF16)],
        [ids, packed, swapped, queries, recurrent, value_up, out_attn, out_rec],
        "mix",
        scratch=[pltpu.VMEM((seq, value_up.shape[1] + value_width), BF16)],
        limit=wide if peers <= 16 else 56 << 20,
    )
    other = lax.ppermute(send, "tp", partner)
    (ours,) = call(
        project_kernel,
        [((seq // 2, width), BF16)],
        [kept, out_attn, out_rec],
        "project",
        ids=False,
    )
    both = ours.astype(F32) + other.astype(F32)
    step = seq // lanes
    total = both[:step]
    for k in range(1, pieces):
        piece = both[k * step : (k + 1) * step].astype(BF16)
        total = total + lax.ppermute(piece, "tp", ring[k]).astype(F32)
    return total.astype(BF16)


def solution(mesh):
    in_specs = (
        P(("sp", "tp"), None),
        P(),
        P(),
        P(),
        P(),
        P(),
        P(),
        P(None, "tp"),
        P(None, "tp"),
        P(None, "tp"),
        P(None, "tp"),
        P(None, "tp"),
        P(None, "tp"),
        P(None, "tp"),
        P(None, None, "tp"),
        P("sp", None, "tp"),
        P("tp"),
        P(None, "tp", None, None),
        P(None, "tp", None),
        P("tp", None),
        P("tp", None),
    )
    out_specs = P(("sp", "tp"), None)
    return jax.shard_map(shards, mesh=mesh, in_specs=in_specs, out_specs=out_specs, check_vma=False)
```

```python
import functools

import jax
import jax.numpy as jnp
import numpy as np
from jax import lax
from jax.experimental import pallas as pl
from jax.experimental.pallas import tpu as pltpu
from jax.sharding import PartitionSpec as P

EPS = 1e-06
NEG = -(2.0**100)
AUX = 8
F32 = jnp.float32
BF16 = jnp.bfloat16
NT = (((1,), (1,)), ((), ()))


def radices_of(peers):
    first = 2 if peers % 2 == 0 else 1
    rest = peers // first
    radices = [first]
    while rest > 1:
        step = 4 if rest % 4 == 0 else next(p for p in range(2, rest + 1) if rest % p == 0)
        radices.append(step)
        rest //= step
    if len(radices) == 1:
        radices.append(1)
    return radices


def peer_digit(digit, radix, k, sending):
    if radix & (radix - 1) == 0:
        return digit ^ k
    return (digit + k if sending else digit - k + radix) % radix


def digit_pairs(peers, stride, radix, k):
    pairs = []
    for i in range(peers):
        digit = (i // stride) % radix
        pairs.append((i, i + (peer_digit(digit, radix, k, True) - digit) * stride))
    return pairs


def dot(a, b):
    return jnp.dot(a, b, preferred_element_type=F32)


def dot_nt(a, b):
    return lax.dot_general(a, b, NT, preferred_element_type=F32)


def dot_split(a, b):
    high = a.astype(BF16)
    low = (a - high.astype(F32)).astype(BF16)
    return dot(high, b) + dot(low, b)


def rms(values, gain):
    return values * lax.rsqrt(jnp.mean(values * values, axis=-1, keepdims=True) + EPS) * gain


def iota2(rows, cols, dim):
    return lax.broadcasted_iota(jnp.int32, (rows, cols), dim)


def turned_rows(weight_t):
    half = weight_t.shape[0] // 2
    return jnp.concatenate([weight_t, -weight_t[half:], weight_t[:half]], axis=0)


def angle_table(ids_ref, cos_base, sin_base, cos_row, sin_row):
    block = ids_ref[1]
    cb, sb = cos_base[pl.ds(block, 1), :], sin_base[pl.ds(block, 1), :]
    cr, sr = cos_row[...], sin_row[...]
    cos, sin = cb * cr - sb * sr, sb * cr + cb * sr
    half = cr.shape[1] // 2
    return jnp.where(iota2(cr.shape[0], cr.shape[1], 1) < half, cos, sin)


def rotated(product, table):
    mixed = product * table
    return mixed + pltpu.roll(mixed, product.shape[1] // 2, 1)


def aux_rows(n_row, peak_row, keep_row):
    high = keep_row.astype(BF16).astype(F32)
    mid = (keep_row - high).astype(BF16).astype(F32)
    low = keep_row - high - mid
    pad = jnp.zeros((AUX - 5, n_row.shape[1]), F32)
    return jnp.concatenate([n_row, peak_row, high, mid, low, pad], axis=0)


def read_state(block):
    c_rows = block.shape[0] - AUX
    block = block.astype(F32)
    aux = block[c_rows:]
    return block[:c_rows], aux[0:1], aux[1:2], aux[2:3] + aux[3:4] + aux[4:5]


def placed(state, place, use=None):
    c_part, n_part, peak, keep = state
    if use is not None:
        peak, keep = jnp.where(use, peak, NEG), jnp.where(use, keep, 0.0)
    return c_part, n_part, peak, keep, place


def chain(states):
    logs = []
    total = functools.reduce(jnp.add, [state[3] for state in states])
    for index, (_, _, peak, _, place) in enumerate(states):
        log = peak
        for other, (_, _, _, keep, at) in enumerate(states):
            if other != index:
                log = log + jnp.where(at > place, keep, 0.0)
        logs.append(log)
    return logs, functools.reduce(jnp.maximum, logs), total


def weighted(states, logs, top):
    c_sum = n_sum = None
    for state, log in zip(states, logs):
        weight = jnp.exp(log - top)
        c_part, n_part = weight * state[0], weight * state[1]
        c_sum = c_part if c_sum is None else c_sum + c_part
        n_sum = n_part if n_sum is None else n_sum + n_part
    return c_sum, n_sum


def joined(states):
    logs, top, keep = chain(states)
    top = top.astype(BF16).astype(F32)
    c_sum, n_sum = weighted(states, logs, top)
    return jnp.concatenate([c_sum, aux_rows(n_sum, top, keep)], axis=0)


def log_sigmoid(x):
    return jnp.minimum(x, 0.0) - jnp.log(1.0 + jnp.exp(-jnp.abs(x)))


def head_kernel(
    ids,
    *refs,
    pieces,
    key_width,
):
    piece_refs = refs[: 2 * pieces]
    (
        in_gain,
        kv_down,
        kv_gain,
        rope_t,
        key_t,
        rec_value,
        gate_t,
        level,
        cos_base,
        sin_base,
        cos_row,
        sin_row,
        message,
        normed_out,
        keys_out,
        values_out,
        rows_out,
        table_out,
        rows,
    ) = refs[2 * pieces :]
    mine = ids[0]
    pair, core = mine // 2, mine % 2
    step = piece_refs[0].shape[0]
    seq = rows.shape[0]
    for k in range(pieces):
        source = lax.rem(pair - k + pieces, pieces) * 2
        rows[pl.ds(pl.multiple_of((source + core) * step, step), step), :] = piece_refs[2 * k][...]
        rows[pl.ds(pl.multiple_of((source + 1 - core) * step, step), step), :] = piece_refs[
            2 * k + 1
        ][...]
    normed = rms(rows[...].astype(F32), in_gain[...]).astype(BF16)
    normed_out[...] = normed
    table = angle_table(ids, cos_base, sin_base, cos_row, sin_row)
    table_out[...] = table
    gates = dot_nt(gate_t[...], normed)
    lat = rms(dot(normed, kv_down[...]), kv_gain[...]).astype(BF16)
    rope = rotated(dot_nt(normed, turned_rows(rope_t[...])), table)
    half = seq // 2
    quarter = half // 2
    lat = jnp.where(core == 0, lat[:half], lat[half:])
    rope = jnp.where(core == 0, rope[:half], rope[half:])
    lanes = iota2(quarter, rope.shape[1], 1)
    packed = jnp.where(lanes < rope_t.shape[0], rope[:quarter], rope[quarter:])
    message[0:half, :] = lat
    message[half : half + quarter, :] = packed.astype(BF16)

    key_rows = jnp.concatenate([key_t[...], jnp.zeros_like(key_t)], axis=0)
    keys = (dot_nt(normed, key_rows).astype(BF16).astype(F32)) * key_width ** (-0.5)
    keys_out[...] = keys.astype(BF16)
    values = dot(normed, rec_value[...]).astype(BF16)
    values_out[...] = values

    in_f, in_b = gates[0:1], gates[2:3]
    keep_f = log_sigmoid(gates[1:2] + level[0:1])
    keep_b = log_sigmoid(gates[3:4] + level[1:2])
    row_id, col_id = iota2(seq, seq, 0), iota2(seq, seq, 1)
    upper = jnp.where(row_id <= col_id, 1.0, 0.0).astype(BF16)
    lower = jnp.where(row_id >= col_id, 1.0, 0.0).astype(BF16)
    keeps = jnp.concatenate([keep_f, keep_b, jnp.zeros((6, seq), F32)], axis=0)
    high = keeps.astype(BF16)
    mid = (keeps - high.astype(F32)).astype(BF16)
    low = (keeps - high.astype(F32) - mid.astype(F32)).astype(BF16)
    thirds = jnp.concatenate([high, mid, low, jnp.zeros_like(low)], axis=0)
    cums = dot(thirds, jnp.concatenate([upper, lower], axis=1))
    cums = cums[0:8] + cums[8:16] + cums[16:24]
    cum_f, cum_b = cums[0:1, :seq], cums[1:2, seq:]
    all_f, all_b = cum_f[:, seq - 1 : seq], cum_b[:, 0:1]
    rows_out[...] = jnp.concatenate(
        [cum_f, in_f - cum_f, cum_b, in_b - cum_b, jnp.zeros((4, seq), F32)], axis=0
    )
    keys_t = jnp.transpose(keys)[:key_width]
    base = half + quarter
    weights = []
    for index, (cum, log_in, total) in enumerate(((cum_f, in_f, all_f), (cum_b, in_b, all_b))):
        logs = total - cum + log_in
        peak = jnp.max(logs, axis=1, keepdims=True).astype(BF16).astype(F32)
        weight = jnp.exp(logs - peak)
        weights.append((weight, peak, total))
    w_f, w_b = weights[0][0], weights[1][0]
    c_both = dot_split(jnp.concatenate([keys_t * w_f, keys_t * w_b], axis=0), values)
    n_both = dot_split(
        jnp.concatenate([w_f, w_b, jnp.zeros((6, seq), F32)], axis=0), keys.astype(BF16)
    )
    for index in range(2):
        _, peak, total = weights[index]
        c_part = c_both[index * key_width : (index + 1) * key_width]
        n_row = n_both[index : index + 1]
        zero = jnp.zeros_like(n_row)
        block = jnp.concatenate([c_part, aux_rows(n_row, zero + peak, zero + total)], axis=0)
        at = base + index * (key_width + AUX)
        message[at : at + key_width + AUX, :] = block.astype(BF16)


def local_kernel(
    normed_ref,
    keys_ref,
    values_ref,
    rows_ref,
    table_ref,
    query_down,
    query_gain,
    nope_up,
    rope_up_t,
    key_up,
    rec_query_t,
    queries_out,
    rec_q_out,
    local_out,
):
    normed = normed_ref[...]
    seq = normed.shape[0]
    query_rows = jnp.concatenate([rec_query_t[...], jnp.zeros_like(rec_query_t)], axis=0)
    rec_q = dot_nt(normed, query_rows).astype(BF16)
    rec_q_out[...] = rec_q
    q_lat = rms(dot(normed, query_down[...]), query_gain[...]).astype(BF16)
    nope = dot(q_lat, nope_up[...]).astype(BF16)
    rope = rotated(dot_nt(q_lat, turned_rows(rope_up_t[...])), table_ref[...])
    lat = dot_nt(nope, key_up[...]).astype(BF16)
    width = rope_up_t.shape[0]
    lanes = iota2(seq, rope.shape[1], 1)
    queries_out[0] = jnp.concatenate([lat, jnp.where(lanes < width, rope, 0.0).astype(BF16)], axis=1)
    queries_out[1] = jnp.concatenate(
        [lat, jnp.where(lanes >= width, rope, 0.0).astype(BF16)], axis=1
    )
    values = values_ref[...]
    wide = jnp.concatenate([values, jnp.ones_like(values)], axis=1)
    products = dot_nt(rec_q, keys_ref[...])
    row_id, col_id = iota2(seq, seq, 0), iota2(seq, seq, 1)
    rows = rows_ref[...]
    for index in range(2):
        cum = jnp.transpose(jnp.broadcast_to(rows[2 * index : 2 * index + 1], (seq, seq)))
        seen = row_id >= col_id if index == 0 else row_id <= col_id
        logs = jnp.where(seen, cum + rows[2 * index + 1 : 2 * index + 2], NEG)
        peak = jnp.max(logs, axis=1, keepdims=True)
        gated = products * jnp.exp(logs - peak)
        sums = dot_split(gated, wide)
        local_out[index, :, 0 : 2 * seq] = sums
        local_out[index, :, 2 * seq : 3 * seq] = jnp.broadcast_to(peak, (seq, seq))
        local_out[index, :, 3 * seq :] = cum


def level_states(ids, slot, radix, fetch):
    digit = ids[slot]
    forward, backward = [], []
    for k in range(1, radix):
        source = peer_digit(digit, radix, k, False)
        forward.append(placed(fetch(k, 0), source, source < digit))
        backward.append(placed(fetch(k, 1), -source, source > digit))
    return forward, backward


def merge_kernel(ids, *refs, slot, radix, state_rows, last, next_radix):
    prefix_in = refs[0]
    own = refs[1]
    received = (own,) + refs[2 : 1 + radix]
    outs = refs[1 + radix :]
    prefix_out, messages = outs[0], outs[1:]
    kv_rows = own.shape[0] - 2 * state_rows

    def fetch(k, direction):
        at = kv_rows + direction * state_rows
        return read_state(received[k][at : at + state_rows, :])

    digit = ids[slot]
    totals = []
    for direction in range(2):
        sign = 1 - 2 * direction
        inner = placed(read_state(prefix_in[direction]), sign * digit)
        before, whole = [inner], [placed(fetch(0, direction), sign * digit)]
        for k in range(1, radix):
            source = peer_digit(digit, radix, k, False)
            state = fetch(k, direction)
            before.append(placed(state, sign * source, sign * source < sign * digit))
            whole.append(placed(state, sign * source))
        prefix_out[direction] = joined(before)
        totals.append(joined(whole).astype(BF16))
    total_f, total_b = totals
    part = kv_rows // 3
    for number, message in enumerate(messages):
        for section in range(3):
            for k in range(radix):
                to = (section * radix + k) * part
                message[to : to + part, :] = received[k][section * part : (section + 1) * part, :]
        at = radix * kv_rows
        if last:
            target = peer_digit(ids[slot + 1], next_radix, number + 1, True)
            ahead = target > ids[slot + 1]
            message[at : at + state_rows, :] = jnp.where(ahead, total_f, total_b)
        else:
            message[at : at + state_rows, :] = total_f
            message[at + state_rows : at + 2 * state_rows, :] = total_b


def load_kernel(*refs):
    count = (len(refs) - 1) // 2
    sems = refs[-1]
    copies = [
        pltpu.make_async_copy(refs[i], refs[count + i], sems.at[i]) for i in range(count)
    ]
    for copy in copies:
        copy.start()
    for copy in copies:
        copy.wait()


def pack_kernel(*refs):
    received, out = refs[1:-1], refs[-1]
    count = len(received)
    part = out.shape[0] // (3 * count)
    for k, message in enumerate(received):
        for section in range(3):
            to = (section * count + k) * part
            out[to : to + part, :] = message[section * part : (section + 1) * part, :]


def recur_kernel(
    ids,
    *refs,
    slot,
    radix,
    state_rows,
    floor_value,
):
    received = refs[:radix]
    prefix, rec_q_ref, local, head_gain, init_state, init_norm, out = refs[radix:]
    kv_rows = received[0].shape[0] - state_rows
    seq = rec_q_ref.shape[0]

    def fetch(k, direction):
        return read_state(received[k][kv_rows : kv_rows + state_rows, :])

    sides = level_states(ids, slot, radix, fetch)
    rec_q = rec_q_ref[...]
    starts = []
    for index in range(2):
        inner = read_state(prefix[index])
        zero = jnp.zeros_like(inner[1])
        key_width = init_norm.shape[1]
        norm = jnp.concatenate(
            [init_norm[index : index + 1], jnp.zeros((1, zero.shape[1] - key_width), F32)], axis=1
        )
        first = placed((init_state[index], norm, zero, zero), -radix)
        states = [first] + sides[index] + [placed(inner, ids[slot] if index == 0 else -ids[slot])]
        logs, start_top, _ = chain(states)
        starts.append(weighted(states, logs, start_top) + (start_top,))
    c_start = jnp.concatenate([starts[0][0], starts[1][0]], axis=1)
    pad = jnp.zeros((rec_q.shape[1] - c_start.shape[0], c_start.shape[1]), F32)
    c_start = jnp.concatenate([c_start, pad], axis=0)
    high = c_start.astype(BF16)
    low = (c_start - high.astype(F32)).astype(BF16)
    products = dot(rec_q, high) + dot(rec_q, low)
    summed = None
    for index in range(2):
        _, n_start, start_top = starts[index]
        from_start = products[:, index * seq : (index + 1) * seq]
        norm_start = jnp.sum(rec_q.astype(F32) * n_start, axis=1, keepdims=True)
        numer = local[index, :, 0:seq]
        denom = local[index, :, seq : 2 * seq]
        peak = local[index, :, 2 * seq : 3 * seq]
        carry = local[index, :, 3 * seq :] + start_top
        row_max = jnp.maximum(peak, carry)
        here, there = jnp.exp(peak - row_max), jnp.exp(carry - row_max)
        numer = here * numer + there * from_start
        denom = here * denom + there * norm_start
        result = numer / jnp.maximum(jnp.abs(denom), floor_value * jnp.exp(-row_max))
        summed = result if summed is None else summed + result
    out[...] = rms(summed, head_gain[...]).astype(BF16)


def mix_kernel(
    ids,
    own_keys,
    other_keys,
    queries,
    recurrent,
    value_up,
    out_attn,
    out_rec,
    send_out,
    keep_out,
    heads,
    *,
    pieces,
    score_scale,
):
    seq = recurrent.shape[0]
    part = own_keys.shape[0] // 3
    scores, lats = [], []
    for keys in (own_keys, other_keys):
        rope = keys[2 * part : 3 * part, :]
        for section in range(2):
            lat = keys[section * part : (section + 1) * part, :]
            lats.append(lat)
            scores.append(
                dot_nt(queries[section], jnp.concatenate([lat, rope], axis=1)) * score_scale
            )
    top = functools.reduce(jnp.maximum, [jnp.max(s, axis=1, keepdims=True) for s in scores])
    mass = accum = None
    for part_scores, lat in zip(scores, lats):
        expo = jnp.exp(part_scores - top)
        gain = dot(expo.astype(BF16), lat)
        total = jnp.sum(expo, axis=1, keepdims=True)
        accum = gain if accum is None else accum + gain
        mass = total if mass is None else mass + total
    attended = (accum / mass).astype(BF16)
    split = value_up.shape[1]
    heads[:, 0:split] = dot(attended, value_up[...]).astype(BF16)
    heads[:, split:] = recurrent[...]

    mine = ids[0]
    pair, core = mine // 2, mine % 2
    step = seq // (2 * pieces)
    for side, out in ((1 - core, None), (core, keep_out)):
        rows = []
        for k in range(pieces):
            owner = lax.rem(pair + k, pieces) * 2 + side
            rows.append(heads[pl.ds(pl.multiple_of(owner * step, step), step), :])
        rows = jnp.concatenate(rows, axis=0)
        if out is None:
            send_out[...] = (
                dot(rows[:, :split], out_attn[...]) + dot(rows[:, split:], out_rec[...])
            ).astype(BF16)
        else:
            out[...] = rows


def project_kernel(rows, out_attn, out_rec, out):
    split = out_attn.shape[0]
    out[...] = (dot(rows[:, :split], out_attn[...]) + dot(rows[:, split:], out_rec[...])).astype(
        BF16
    )


def call(kernel, outs, inputs, name, scratch=(), ids=True, limit=16 << 20, cost=None):
    vmem = pl.BlockSpec(memory_space=pltpu.VMEM)
    in_specs = [vmem] * len(inputs)
    if ids:
        in_specs[0] = pl.BlockSpec(memory_space=pltpu.SMEM)
    return pl.pallas_call(
        kernel,
        out_shape=[jax.ShapeDtypeStruct(shape, dtype) for shape, dtype in outs],
        in_specs=in_specs,
        out_specs=[vmem] * len(outs),
        scratch_shapes=scratch,
        name=name,
        cost_estimate=cost,
        compiler_params=pltpu.CompilerParams(vmem_limit_bytes=limit),
    )(*inputs)


def shards(
    rows_in,
    in_gain,
    query_down,
    query_gain,
    kv_down,
    kv_gain,
    rope_down,
    query_nope_up,
    query_rope_up,
    key_up,
    value_up,
    rec_query,
    rec_key,
    rec_value,
    gate_weight,
    forget_level,
    head_gain,
    init_state,
    init_norm,
    out_attn,
    out_rec,
):
    peers, lanes = lax.axis_size("sp"), lax.axis_size("tp")
    block, mine = lax.axis_index("sp"), lax.axis_index("tp")
    seq = forget_level.shape[0]
    width = rows_in.shape[1]
    nope, rope = key_up.shape[1], rope_down.shape[1]
    key_width, value_width = init_state.shape[2], init_state.shape[3]
    pieces = lanes // 2
    radices = radices_of(peers)
    strides = [int(np.prod(radices[:i])) for i in range(len(radices))]
    divide = np.array([1, 1] + strides, np.int32)
    modulo = np.array([lanes, peers] + radices, np.int32)
    first = np.arange(len(divide)) == 0
    ids = (jnp.where(first, mine, block).astype(jnp.int32) // divide) % modulo

    partner = [(i, i ^ 1) for i in range(lanes)]
    ring = [[(i, (i + 2 * k) % lanes) for i in range(lanes)] for k in range(pieces)]

    gathered = [rows_in] + [lax.ppermute(rows_in, "tp", ring[k]) for k in range(1, pieces)]
    row_pieces = []
    for piece in gathered:
        row_pieces += [piece, lax.ppermute(piece, "tp", partner)]

    freq = 10000.0 ** (-np.arange(rope // 2, dtype=np.float64) / (rope // 2))
    freq = np.tile(freq, 4)[None, :]
    base = np.arange(peers, dtype=np.float64)[:, None] * seq * freq
    within = np.arange(seq, dtype=np.float64)[:, None] * freq
    tables = [np.cos(base), np.sin(base), np.cos(within), np.sin(within)]
    tables = [jnp.asarray(table.astype(np.float32)) for table in tables]

    held = [
        in_gain[None, :],
        kv_down,
        kv_gain[None, :],
        rope_down.T,
        rec_key.T,
        rec_value,
        gate_weight[:, :, 0].T,
        forget_level[:, :, 0].T,
        *tables,
        query_down,
        query_gain[None, :],
        query_nope_up,
        query_rope_up.T,
        key_up,
        rec_query.T,
        value_up,
        head_gain[None, :],
        init_state[:, 0],
        init_norm[:, 0],
        out_attn,
        out_rec,
    ]
    held = list(
        pl.pallas_call(
            load_kernel,
            out_shape=[pltpu.VMEM(array.shape, array.dtype) for array in held],
            in_specs=[pl.BlockSpec(memory_space=pltpu.HBM)] * len(held),
            out_specs=[pl.BlockSpec(memory_space=pltpu.VMEM)] * len(held),
            scratch_shapes=[pltpu.SemaphoreType.DMA((len(held),))],
            name="load",
            cost_estimate=pl.CostEstimate(flops=10**8, bytes_accessed=1 << 22, transcendentals=0),
            compiler_params=pltpu.CompilerParams(vmem_limit_bytes=16 << 20),
        )(*[pltpu.with_memory_space_constraint(array, pltpu.HBM) for array in held])
    )
    head_args, local_args = held[:12], held[12:18]
    value_up, head_gain, init_state, init_norm, out_attn, out_rec = held[18:]

    state_rows = key_width + AUX
    kv_rows = seq // 2 + seq // 4
    message, normed, keys, values, gate_rows, table = call(
        functools.partial(head_kernel, pieces=pieces, key_width=key_width),
        [
            ((kv_rows + 2 * state_rows, value_width), BF16),
            ((seq, width), BF16),
            ((seq, 2 * key_width), BF16),
            ((seq, value_width), BF16),
            ((8, seq), F32),
            ((seq, 2 * rope), F32),
        ],
        [ids]
        + row_pieces
        + head_args,
        "head",
        scratch=[pltpu.VMEM((seq, width), BF16)],
    )
    queries, rec_q, local = call(
        local_kernel,
        [
            ((2, seq, 2 * value_width), BF16),
            ((seq, 2 * key_width), BF16),
            ((2, seq, 4 * seq), F32),
        ],
        [
            normed,
            keys,
            values,
            gate_rows,
            table,
            *local_args,
        ],
        "local",
        ids=False,
    )

    blank = np.zeros((2, state_rows, value_width), np.float32)
    blank[:, key_width + 1] = NEG
    prefix = jnp.asarray(blank)
    wide = (16 << 20) if peers <= 16 else (40 << 20)
    for level, radix in enumerate(radices[:-1]):
        received = [
            lax.ppermute(message, "sp", digit_pairs(peers, strides[level], radix, k))
            for k in range(1, radix)
        ]
        last = level == len(radices) - 2
        kv_rows *= radix
        count = radices[-1] - 1 if last else 1
        out_rows = kv_rows + (1 if last else 2) * state_rows
        prefix, *messages = call(
            functools.partial(
                merge_kernel,
                slot=2 + level,
                radix=radix,
                state_rows=state_rows,
                last=last,
                next_radix=radices[level + 1],
            ),
            [((2, state_rows, value_width), F32)]
            + [((out_rows, value_width), BF16)] * max(count, 1),
            [ids, prefix, message] + received,
            "merge",
            limit=wide,
        )
        message = messages[0]
    level, radix = len(radices) - 1, radices[-1]
    received = [
        lax.ppermute(messages[k - 1], "sp", digit_pairs(peers, strides[level], radix, k))
        for k in range(1, radix)
    ]
    (packed,) = call(
        pack_kernel,
        [((radix * kv_rows, value_width), BF16)],
        [rec_q, message] + received,
        "pack",
        ids=False,
        limit=wide,
    )
    swapped = lax.ppermute(packed, "tp", partner)
    (recurrent,) = call(
        functools.partial(
            recur_kernel,
            slot=2 + level,
            radix=radix,
            state_rows=state_rows,
            floor_value=float(seq * peers) ** 0.5,
        ),
        [((seq, value_width), BF16)],
        [ids, message]
        + received
        + [
            prefix,
            rec_q,
            local,
            head_gain,
            init_state,
            init_norm,
        ],
        "recur",
        limit=wide,
        cost=pl.CostEstimate(flops=10**8, bytes_accessed=1 << 20, transcendentals=0),
    )
    send, kept = call(
        functools.partial(
            mix_kernel,
            pieces=pieces,
            score_scale=(nope + rope) ** (-0.5),
        ),
        [((seq // 2, width), BF16), ((seq // 2, nope + value_width), BF16)],
        [ids, packed, swapped, queries, recurrent, value_up, out_attn, out_rec],
        "mix",
        scratch=[pltpu.VMEM((seq, value_up.shape[1] + value_width), BF16)],
        limit=wide if peers <= 16 else 56 << 20,
    )
    other = lax.ppermute(send, "tp", partner)
    (ours,) = call(
        project_kernel,
        [((seq // 2, width), BF16)],
        [kept, out_attn, out_rec],
        "project",
        ids=False,
    )
    both = ours.astype(F32) + other.astype(F32)
    step = seq // lanes
    total = both[:step]
    for k in range(1, pieces):
        piece = both[k * step : (k + 1) * step].astype(BF16)
        total = total + lax.ppermute(piece, "tp", ring[k]).astype(F32)
    return total.astype(BF16)


def solution(mesh):
    in_specs = (
        P(("sp", "tp"), None),
        P(),
        P(),
        P(),
        P(),
        P(),
        P(),
        P(None, "tp"),
        P(None, "tp"),
        P(None, "tp"),
        P(None, "tp"),
        P(None, "tp"),
        P(None, "tp"),
        P(None, "tp"),
        P(None, None, "tp"),
        P("sp", None, "tp"),
        P("tp"),
        P(None, "tp", None, None),
        P(None, "tp", None),
        P("tp", None),
        P("tp", None),
    )
    out_specs = P(("sp", "tp"), None)
    return jax.shard_map(shards, mesh=mesh, in_specs=in_specs, out_specs=out_specs, check_vma=False)
```

```python
import functools

import jax
import jax.numpy as jnp
import numpy as np
from jax import lax
from jax.experimental import pallas as pl
from jax.experimental.pallas import tpu as pltpu
from jax.sharding import PartitionSpec as P

EPS = 1e-06
NEG = -(2.0**100)
AUX = 8
F32 = jnp.float32
BF16 = jnp.bfloat16
NT = (((1,), (1,)), ((), ()))


def radices_of(peers):
    first = 2 if peers % 2 == 0 else 1
    rest = peers // first
    radices = [first]
    while rest > 1:
        step = 4 if rest % 4 == 0 else next(p for p in range(2, rest + 1) if rest % p == 0)
        radices.append(step)
        rest //= step
    if len(radices) == 1:
        radices.append(1)
    return radices


def peer_digit(digit, radix, k, sending):
    if radix & (radix - 1) == 0:
        return digit ^ k
    return (digit + k if sending else digit - k + radix) % radix


def digit_pairs(peers, stride, radix, k):
    pairs = []
    for i in range(peers):
        digit = (i // stride) % radix
        pairs.append((i, i + (peer_digit(digit, radix, k, True) - digit) * stride))
    return pairs


def dot(a, b):
    return jnp.dot(a, b, preferred_element_type=F32)


def dot_nt(a, b):
    return lax.dot_general(a, b, NT, preferred_element_type=F32)


def dot_split(a, b):
    high = a.astype(BF16)
    low = (a - high.astype(F32)).astype(BF16)
    return dot(high, b) + dot(low, b)


def rms(values, gain):
    return values * lax.rsqrt(jnp.mean(values * values, axis=-1, keepdims=True) + EPS) * gain


def iota2(rows, cols, dim):
    return lax.broadcasted_iota(jnp.int32, (rows, cols), dim)


def turned_rows(weight_t):
    half = weight_t.shape[0] // 2
    return jnp.concatenate([weight_t, -weight_t[half:], weight_t[:half]], axis=0)


def angle_table(ids_ref, cos_base, sin_base, cos_row, sin_row):
    block = ids_ref[1]
    cb, sb = cos_base[pl.ds(block, 1), :], sin_base[pl.ds(block, 1), :]
    cr, sr = cos_row[...], sin_row[...]
    cos, sin = cb * cr - sb * sr, sb * cr + cb * sr
    half = cr.shape[1] // 2
    return jnp.where(iota2(cr.shape[0], cr.shape[1], 1) < half, cos, sin)


def rotated(product, table):
    mixed = product * table
    return mixed + pltpu.roll(mixed, product.shape[1] // 2, 1)


def aux_rows(n_row, peak_row, keep_row):
    high = keep_row.astype(BF16).astype(F32)
    mid = (keep_row - high).astype(BF16).astype(F32)
    low = keep_row - high - mid
    pad = jnp.zeros((AUX - 5, n_row.shape[1]), F32)
    return jnp.concatenate([n_row, peak_row, high, mid, low, pad], axis=0)


def read_state(block):
    c_rows = block.shape[0] - AUX
    block = block.astype(F32)
    aux = block[c_rows:]
    return block[:c_rows], aux[0:1], aux[1:2], aux[2:3] + aux[3:4] + aux[4:5]


def placed(state, place, use=None):
    c_part, n_part, peak, keep = state
    if use is not None:
        peak, keep = jnp.where(use, peak, NEG), jnp.where(use, keep, 0.0)
    return c_part, n_part, peak, keep, place


def chain(states):
    logs = []
    total = functools.reduce(jnp.add, [state[3] for state in states])
    for index, (_, _, peak, _, place) in enumerate(states):
        log = peak
        for other, (_, _, _, keep, at) in enumerate(states):
            if other != index:
                log = log + jnp.where(at > place, keep, 0.0)
        logs.append(log)
    return logs, functools.reduce(jnp.maximum, logs), total


def weighted(states, logs, top):
    c_sum = n_sum = None
    for state, log in zip(states, logs):
        weight = jnp.exp(log - top)
        c_part, n_part = weight * state[0], weight * state[1]
        c_sum = c_part if c_sum is None else c_sum + c_part
        n_sum = n_part if n_sum is None else n_sum + n_part
    return c_sum, n_sum


def joined(states):
    logs, top, keep = chain(states)
    top = top.astype(BF16).astype(F32)
    c_sum, n_sum = weighted(states, logs, top)
    return jnp.concatenate([c_sum, aux_rows(n_sum, top, keep)], axis=0)


def log_sigmoid(x):
    return jnp.minimum(x, 0.0) - jnp.log(1.0 + jnp.exp(-jnp.abs(x)))


def head_kernel(
    ids,
    *refs,
    pieces,
    key_width,
):
    piece_refs = refs[: 2 * pieces]
    (
        in_gain,
        kv_down,
        kv_gain,
        rope_t,
        key_t,
        rec_value,
        gate_t,
        level,
        cos_base,
        sin_base,
        cos_row,
        sin_row,
        message,
        normed_out,
        keys_out,
        values_out,
        rows_out,
        table_out,
        rows,
    ) = refs[2 * pieces :]
    mine = ids[0]
    pair, core = mine // 2, mine % 2
    step = piece_refs[0].shape[0]
    seq = rows.shape[0]
    for k in range(pieces):
        source = lax.rem(pair - k + pieces, pieces) * 2
        rows[pl.ds(pl.multiple_of((source + core) * step, step), step), :] = piece_refs[2 * k][...]
        rows[pl.ds(pl.multiple_of((source + 1 - core) * step, step), step), :] = piece_refs[
            2 * k + 1
        ][...]
    normed = rms(rows[...].astype(F32), in_gain[...]).astype(BF16)
    normed_out[...] = normed
    table = angle_table(ids, cos_base, sin_base, cos_row, sin_row)
    table_out[...] = table
    latent = kv_down.shape[1]
    straight = dot(normed, jnp.concatenate([kv_down[...], rec_value[...]], axis=1))
    turned = turned_rows(rope_t[...])
    gate_rows = gate_t.shape[0]
    fill = jnp.zeros((turned.shape[0] - key_width - gate_rows, turned.shape[1]), BF16)
    crossed = dot_nt(
        normed, jnp.concatenate([turned, key_t[...], gate_t[...], fill], axis=0)
    )
    rope_lanes = turned.shape[0]
    lat = rms(straight[:, :latent], kv_gain[...]).astype(BF16)
    rope = rotated(crossed[:, :rope_lanes], table)
    half = seq // 2
    quarter = half // 2
    lat = jnp.where(core == 0, lat[:half], lat[half:])
    rope = jnp.where(core == 0, rope[:half], rope[half:])
    lanes = iota2(quarter, rope.shape[1], 1)
    packed = jnp.where(lanes < rope_t.shape[0], rope[:quarter], rope[quarter:])
    message[0:half, :] = lat
    message[half : half + quarter, :] = packed.astype(BF16)

    mixed = crossed[:, rope_lanes:]
    keys = mixed.astype(BF16).astype(F32) * key_width ** (-0.5)
    keys = jnp.where(iota2(seq, keys.shape[1], 1) < key_width, keys, 0.0)
    keys_out[...] = keys.astype(BF16)
    values = straight[:, latent:].astype(BF16)
    values_out[...] = values
    mixed_t = jnp.transpose(mixed)
    gates = mixed_t[key_width : key_width + 8]

    in_f, in_b = gates[0:1], gates[2:3]
    keep_f = log_sigmoid(gates[1:2] + level[0:1])
    keep_b = log_sigmoid(gates[3:4] + level[1:2])
    row_id, col_id = iota2(seq, seq, 0), iota2(seq, seq, 1)
    upper = jnp.where(row_id <= col_id, 1.0, 0.0).astype(BF16)
    lower = jnp.where(row_id >= col_id, 1.0, 0.0).astype(BF16)
    keeps = jnp.concatenate([keep_f, keep_b, jnp.zeros((6, seq), F32)], axis=0)
    high = keeps.astype(BF16)
    mid = (keeps - high.astype(F32)).astype(BF16)
    low = (keeps - high.astype(F32) - mid.astype(F32)).astype(BF16)
    thirds = jnp.concatenate([high, mid, low, jnp.zeros_like(low)], axis=0)
    cums = dot(thirds, jnp.concatenate([upper, lower], axis=1))
    cums = cums[0:8] + cums[8:16] + cums[16:24]
    cum_f, cum_b = cums[0:1, :seq], cums[1:2, seq:]
    all_f, all_b = cum_f[:, seq - 1 : seq], cum_b[:, 0:1]
    rows_out[...] = jnp.concatenate(
        [cum_f, in_f - cum_f, cum_b, in_b - cum_b, jnp.zeros((4, seq), F32)], axis=0
    )
    keys_t = mixed_t[:key_width].astype(BF16).astype(F32) * key_width ** (-0.5)
    base = half + quarter
    weights = []
    for cum, log_in, total in ((cum_f, in_f, all_f), (cum_b, in_b, all_b)):
        logs = total - cum + log_in
        peak = jnp.max(logs, axis=1, keepdims=True).astype(BF16).astype(F32)
        weight = jnp.exp(logs - peak)
        weights.append((weight, peak, total))
    w_f, w_b = weights[0][0], weights[1][0]
    c_both = dot_split(jnp.concatenate([keys_t * w_f, keys_t * w_b], axis=0), values)
    n_both = dot_split(
        jnp.concatenate([w_f, w_b, jnp.zeros((6, seq), F32)], axis=0), keys.astype(BF16)
    )
    for index in range(2):
        _, peak, total = weights[index]
        c_part = c_both[index * key_width : (index + 1) * key_width]
        n_row = n_both[index : index + 1]
        zero = jnp.zeros_like(n_row)
        block = jnp.concatenate([c_part, aux_rows(n_row, zero + peak, zero + total)], axis=0)
        at = base + index * (key_width + AUX)
        message[at : at + key_width + AUX, :] = block.astype(BF16)


def thirds_of(x):
    high = x.astype(BF16)
    mid = (x - high.astype(F32)).astype(BF16)
    low = (x - high.astype(F32) - mid.astype(F32)).astype(BF16)
    return [high, mid, low]


def local_kernel(
    ids,
    normed_ref,
    keys_ref,
    values_ref,
    rows_ref,
    table_ref,
    query_down,
    query_gain,
    nope_up,
    rope_up_t,
    key_up,
    rec_query_t,
    init_state,
    init_norm,
    keep_out,
    share_out,
    whole,
    *,
    pieces,
):
    normed = normed_ref[...]
    seq = normed.shape[0]
    query_rows = jnp.concatenate([rec_query_t[...], jnp.zeros_like(rec_query_t)], axis=0)
    rec_q = dot_nt(normed, query_rows).astype(BF16)
    q_lat = rms(dot(normed, query_down[...]), query_gain[...]).astype(BF16)
    nope = dot(q_lat, nope_up[...]).astype(BF16)
    rope = rotated(dot_nt(q_lat, turned_rows(rope_up_t[...])), table_ref[...])
    lat = dot_nt(nope, key_up[...]).astype(BF16)
    width = rope_up_t.shape[0]
    lanes = iota2(seq, rope.shape[1], 1)
    low_rope = jnp.where(lanes < width, rope, 0.0).astype(BF16)
    high_rope = jnp.where(lanes >= width, rope, 0.0).astype(BF16)
    values = values_ref[...]
    wide = jnp.concatenate([values, jnp.ones_like(values)], axis=1)
    products = dot_nt(rec_q, keys_ref[...])
    row_id, col_id = iota2(seq, seq, 0), iota2(seq, seq, 1)
    rows = rows_ref[...]
    numers, denoms, marks = [], [], []
    for index in range(2):
        cum = jnp.transpose(jnp.broadcast_to(rows[2 * index : 2 * index + 1], (seq, seq)))
        seen = row_id >= col_id if index == 0 else row_id <= col_id
        logs = jnp.where(seen, cum + rows[2 * index + 1 : 2 * index + 2], NEG)
        peak = jnp.max(logs, axis=1, keepdims=True)
        gated = products * jnp.exp(logs - peak)
        sums = dot_split(gated, wide)
        numers.append(sums[:, : values.shape[1]].astype(BF16))
        denoms.append(sums[:, values.shape[1] :].astype(BF16))
        marks += thirds_of(jnp.broadcast_to(peak, (seq, seq))) + thirds_of(cum)
    columns = [lat, low_rope, high_rope] + numers + denoms + [rec_q] + marks
    step_cols = lat.shape[1]
    for index, column in enumerate(columns):
        whole[:, index * step_cols : (index + 1) * step_cols] = column
    mine = ids[0]
    pair, core = mine // 2, mine % 2
    step = seq // (2 * pieces)
    for side, out in ((core, keep_out), (1 - core, share_out)):
        for k in range(pieces):
            owner = lax.rem(pair + k, pieces) * 2 + side
            out[k * step : (k + 1) * step, 0 : whole.shape[1]] = whole[
                pl.ds(pl.multiple_of(owner * step, step), step), :
            ]
    lanes = init_state.shape[2]
    norms = init_norm[...]
    norms = jnp.concatenate([norms, jnp.zeros((2, lanes - norms.shape[1]), F32)], axis=1)
    rest = jnp.zeros((init_state.shape[1] - 2, lanes), F32)
    first = jnp.concatenate([norms, rest], axis=0).astype(BF16)
    starts = [init_state[0].astype(BF16), init_state[1].astype(BF16), first]
    for out in (keep_out, share_out):
        for index, block in enumerate(starts):
            at = whole.shape[1] + index * lanes
            out[0 : block.shape[0], at : at + lanes] = block


def fold_kernel(value_up, head_gain, out_attn, out_rec, out):
    rows = value_up.shape[0]
    out[0:rows, :] = dot(value_up[...], out_attn[...]).astype(BF16)
    gain = head_gain[...]
    width = gain.shape[1]
    column = jnp.transpose(jnp.broadcast_to(gain, (width, width)))[:, 0:1]
    out[rows:, :] = (column * out_rec[...].astype(F32)).astype(BF16)


def level_states(ids, slot, radix, fetch):
    digit = ids[slot]
    forward, backward = [], []
    for k in range(1, radix):
        source = peer_digit(digit, radix, k, False)
        forward.append(placed(fetch(k, 0), source, source < digit))
        backward.append(placed(fetch(k, 1), -source, source > digit))
    return forward, backward


def merge_kernel(ids, *refs, slot, radix, state_rows, last, next_radix):
    prefix_in = refs[0]
    own = refs[1]
    received = (own,) + refs[2 : 1 + radix]
    outs = refs[1 + radix :]
    prefix_out, sides_out, messages = outs[0], outs[1], outs[2:]
    kv_rows = own.shape[0] - 2 * state_rows

    def fetch(k, direction):
        at = kv_rows + direction * state_rows
        return read_state(received[k][at : at + state_rows, :])

    digit = ids[slot]
    totals = []
    for direction in range(2):
        sign = 1 - 2 * direction
        inner = placed(read_state(prefix_in[direction]), sign * digit)
        before, whole = [inner], [placed(fetch(0, direction), sign * digit)]
        for k in range(1, radix):
            source = peer_digit(digit, radix, k, False)
            state = fetch(k, direction)
            before.append(placed(state, sign * source, sign * source < sign * digit))
            whole.append(placed(state, sign * source))
        inside = joined(before)
        prefix_out[direction] = inside
        sides_out[direction * state_rows : (direction + 1) * state_rows, :] = inside.astype(BF16)
        totals.append(joined(whole).astype(BF16))
    total_f, total_b = totals
    part = kv_rows // 3
    for number, message in enumerate(messages):
        for section in range(3):
            for k in range(radix):
                to = (section * radix + k) * part
                message[to : to + part, :] = received[k][section * part : (section + 1) * part, :]
        at = radix * kv_rows
        if last:
            target = peer_digit(ids[slot + 1], next_radix, number + 1, True)
            ahead = target > ids[slot + 1]
            message[at : at + state_rows, :] = jnp.where(ahead, total_f, total_b)
        else:
            message[at : at + state_rows, :] = total_f
            message[at + state_rows : at + 2 * state_rows, :] = total_b


def load_kernel(*refs):
    count = (len(refs) - 1) // 2
    sems = refs[-1]
    copies = [
        pltpu.make_async_copy(refs[i], refs[count + i], sems.at[i]) for i in range(count)
    ]
    for copy in copies:
        copy.start()
    for copy in copies:
        copy.wait()


def pack_kernel(*refs, count, state_rows):
    received, out = refs[-1 - count : -1], refs[-1]
    part = (received[0].shape[0] - state_rows) // 3
    for k, message in enumerate(received):
        for section in range(3):
            to = (section * count + k) * part
            out[to : to + part, :] = message[section * part : (section + 1) * part, :]
        if k > 0:
            to = 3 * count * part + (k - 1) * state_rows
            out[to : to + state_rows, :] = message[3 * part : 3 * part + state_rows, :]


def attend(sections, keys, part, score_scale):
    rope = keys[2 * part : 3 * part, :]
    scores, lats = [], []
    for section in range(2):
        lat = keys[section * part : (section + 1) * part, :]
        lats.append(lat)
        scores.append(dot_nt(sections[section], jnp.concatenate([lat, rope], axis=1)) * score_scale)
    top = functools.reduce(jnp.maximum, [jnp.max(s, axis=1, keepdims=True) for s in scores])
    mass = accum = None
    for part_scores, lat in zip(scores, lats):
        expo = jnp.exp(part_scores - top)
        gain = dot(expo.astype(BF16), lat)
        total = jnp.sum(expo, axis=1, keepdims=True)
        accum = gain if accum is None else accum + gain
        mass = total if mass is None else mass + total
    return top, mass, accum


def sections_of(queries, width):
    return [
        queries[:, 0 : 2 * width],
        jnp.concatenate([queries[:, 0:width], queries[:, 2 * width :]], axis=1),
    ]


def finished(ids, block, first_ref, packed, sides, slot, radix, state_rows, floor_value):
    base = packed.shape[0] - (radix - 1) * state_rows
    width = packed.shape[1]

    def column(index):
        return block[:, index * width : (index + 1) * width].astype(F32)

    def triple(index):
        return column(index) + column(index + 1) + column(index + 2)

    def fetch(k, direction):
        at = base + (k - 1) * state_rows
        return read_state(packed[at : at + state_rows, :])

    levels = level_states(ids, slot, radix, fetch)
    rec_q = block[:, 7 * width : 8 * width]
    starts = []
    for index in range(2):
        inner = read_state(sides[index * state_rows : (index + 1) * state_rows, :])
        zero = jnp.zeros_like(inner[1])
        first = (
            first_ref[:, (20 + index) * width : (21 + index) * width].astype(F32),
            first_ref[0:8, 22 * width :].astype(F32)[index : index + 1],
            zero,
            zero,
        )
        states = [placed(first, -radix)] + levels[index]
        states.append(placed(inner, ids[slot] if index == 0 else -ids[slot]))
        logs, start_top, _ = chain(states)
        starts.append(weighted(states, logs, start_top) + (start_top,))
    c_start = jnp.concatenate([starts[0][0], starts[1][0]], axis=1)
    pad = jnp.zeros((rec_q.shape[1] - c_start.shape[0], c_start.shape[1]), F32)
    c_start = jnp.concatenate([c_start, pad], axis=0)
    high = c_start.astype(BF16)
    low = (c_start - high.astype(F32)).astype(BF16)
    products = dot(rec_q, high) + dot(rec_q, low)
    summed = None
    for index in range(2):
        _, n_start, start_top = starts[index]
        from_start = products[:, index * width : (index + 1) * width]
        norm_start = jnp.sum(rec_q.astype(F32) * n_start, axis=1, keepdims=True)
        numer, denom = column(3 + index), column(5 + index)
        peak, carry = triple(8 + 6 * index), triple(11 + 6 * index) + start_top
        row_max = jnp.maximum(peak, carry)
        here, there = jnp.exp(peak - row_max), jnp.exp(carry - row_max)
        numer = here * numer + there * from_start
        denom = here * denom + there * norm_start
        result = numer / jnp.maximum(jnp.abs(denom), floor_value * jnp.exp(-row_max))
        summed = result if summed is None else summed + result
    return rms(summed, 1.0).astype(BF16)


def half_kernel(
    ids,
    packed,
    sides,
    kept,
    shared,
    recurrent_out,
    top_out,
    mass_out,
    accum_out,
    *,
    slot,
    radix,
    state_rows,
    floor_value,
    score_scale,
):
    width = packed.shape[1]
    part = (packed.shape[0] - (radix - 1) * state_rows) // 3
    recurrent_out[...] = finished(
        ids, kept[...], kept, packed, sides, slot, radix, state_rows, floor_value
    )
    queries = jnp.concatenate([kept[:, 0 : 3 * width], shared[:, 0 : 3 * width]], axis=0)
    top, mass, accum = attend(sections_of(queries, width), packed, part, score_scale)
    top_out[...] = jnp.broadcast_to(top, top_out.shape)
    mass_out[...] = jnp.broadcast_to(mass, mass_out.shape)
    accum_out[...] = accum


def mix_kernel(
    ids,
    swapped,
    sides,
    kept,
    shared,
    recurrent,
    top_half,
    mass_half,
    accum_half,
    weights,
    other_weights,
    out,
    *,
    slot,
    radix,
    state_rows,
    floor_value,
    score_scale,
    piece,
    step,
):
    width = swapped.shape[1]
    part = (swapped.shape[0] - (radix - 1) * state_rows) // 3
    at = slice(piece * step, (piece + 1) * step)
    also = slice(kept.shape[0] + piece * step, kept.shape[0] + (piece + 1) * step)
    queries = jnp.concatenate([kept[at, 0 : 3 * width], shared[at, 0 : 3 * width]], axis=0)
    top, mass, accum = attend(sections_of(queries, width), swapped, part, score_scale)

    def both(ref):
        return jnp.concatenate([ref[at, :], ref[also, :]], axis=0)

    other_top = both(top_half)
    peak = jnp.maximum(top, other_top)
    here, there = jnp.exp(top - peak), jnp.exp(other_top - peak)
    accum = here * accum + there * both(accum_half)
    mass = here * mass + there * both(mass_half)
    attended = (accum / mass).astype(BF16)
    other = finished(
        ids, shared[at, :], shared, swapped, sides, slot, radix, state_rows, floor_value
    )
    mine = jnp.concatenate([attended[:step], recurrent[at, :]], axis=1)
    theirs = jnp.concatenate([attended[step:], other], axis=1)
    out[...] = (dot(mine, weights[...]) + dot(theirs, other_weights[...])).astype(out.dtype)


def call(kernel, outs, inputs, scratch=(), ids=True, limit=16 << 20, cost=None):
    vmem = pl.BlockSpec(memory_space=pltpu.VMEM)
    in_specs = [vmem] * len(inputs)
    if ids:
        in_specs[0] = pl.BlockSpec(memory_space=pltpu.SMEM)
    return pl.pallas_call(
        kernel,
        out_shape=[jax.ShapeDtypeStruct(shape, dtype) for shape, dtype in outs],
        in_specs=in_specs,
        out_specs=[vmem] * len(outs),
        scratch_shapes=scratch,
        cost_estimate=cost,
        compiler_params=pltpu.CompilerParams(vmem_limit_bytes=limit),
    )(*inputs)


def shards(
    rows_in,
    in_gain,
    query_down,
    query_gain,
    kv_down,
    kv_gain,
    rope_down,
    query_nope_up,
    query_rope_up,
    key_up,
    value_up,
    rec_query,
    rec_key,
    rec_value,
    gate_weight,
    forget_level,
    head_gain,
    init_state,
    init_norm,
    out_attn,
    out_rec,
):
    peers, lanes = lax.axis_size("sp"), lax.axis_size("tp")
    block, mine = lax.axis_index("sp"), lax.axis_index("tp")
    seq = forget_level.shape[0]
    width = rows_in.shape[1]
    nope, rope = key_up.shape[1], rope_down.shape[1]
    key_width, value_width = init_state.shape[2], init_state.shape[3]
    pieces = lanes // 2
    radices = radices_of(peers)
    strides = [int(np.prod(radices[:i])) for i in range(len(radices))]
    divide = np.array([1, 1] + strides, np.int32)
    modulo = np.array([lanes, peers] + radices, np.int32)
    first = np.arange(len(divide)) == 0
    ids = (jnp.where(first, mine, block).astype(jnp.int32) // divide) % modulo

    partner = [(i, i ^ 1) for i in range(lanes)]
    ring = [[(i, (i + 2 * k) % lanes) for i in range(lanes)] for k in range(pieces)]

    gathered = [rows_in]
    for k in range(1, pieces):
        gathered.append(lax.ppermute(rows_in, "tp", ring[k]))
    row_pieces = []
    for piece in gathered:
        row_pieces += [piece, lax.ppermute(piece, "tp", partner)]

    freq = 10000.0 ** (-np.arange(rope // 2, dtype=np.float64) / (rope // 2))
    freq = np.tile(freq, 4)[None, :]
    base = np.arange(peers, dtype=np.float64)[:, None] * seq * freq
    within = np.arange(seq, dtype=np.float64)[:, None] * freq
    tables = [np.cos(base), np.sin(base), np.cos(within), np.sin(within)]
    tables = [jnp.asarray(table.astype(np.float32)) for table in tables]

    held = [
        in_gain[None, :],
        kv_down,
        kv_gain[None, :],
        rope_down.T,
        rec_key.T,
        rec_value,
        gate_weight[:, :, 0].T,
        forget_level[:, :, 0].T,
        *tables,
        query_down,
        query_gain[None, :],
        query_nope_up,
        query_rope_up.T,
        key_up,
        rec_query.T,
        value_up,
        head_gain[None, :],
        init_state[:, 0],
        init_norm[:, 0],
        out_attn,
        out_rec,
    ]
    held = list(
        pl.pallas_call(
            load_kernel,
            out_shape=[pltpu.VMEM(array.shape, array.dtype) for array in held],
            in_specs=[pl.BlockSpec(memory_space=pltpu.HBM)] * len(held),
            out_specs=[pl.BlockSpec(memory_space=pltpu.VMEM)] * len(held),
            scratch_shapes=[pltpu.SemaphoreType.DMA((len(held),))],
            name="load",
            cost_estimate=pl.CostEstimate(flops=10**8, bytes_accessed=1 << 22, transcendentals=0),
            compiler_params=pltpu.CompilerParams(vmem_limit_bytes=16 << 20),
        )(*[pltpu.with_memory_space_constraint(array, pltpu.HBM) for array in held])
    )
    head_args, local_args = held[:12], held[12:18]
    value_up, head_gain, init_state, init_norm, out_attn, out_rec = held[18:]

    state_rows = key_width + AUX
    kv_rows = seq // 2 + seq // 4
    message, normed, keys, values, gate_rows, table = call(
        functools.partial(head_kernel, pieces=pieces, key_width=key_width),
        [
            ((kv_rows + 2 * state_rows, value_width), BF16),
            ((seq, width), BF16),
            ((seq, 2 * key_width), BF16),
            ((seq, value_width), BF16),
            ((8, seq), F32),
            ((seq, 2 * rope), F32),
        ],
        [ids]
        + row_pieces
        + head_args,
        scratch=[pltpu.VMEM((seq, width), BF16)],
    )
    columns = 20 * value_width
    assert key_width == seq // 2
    kept, share = call(
        functools.partial(local_kernel, pieces=pieces),
        [((seq // 2, columns + 3 * value_width), BF16)] * 2,
        [
            ids,
            normed,
            keys,
            values,
            gate_rows,
            table,
            *local_args,
            init_state,
            init_norm,
        ],
        scratch=[pltpu.VMEM((seq, columns), BF16)],
        cost=pl.CostEstimate(flops=10**8, bytes_accessed=1 << 20, transcendentals=0),
    )
    (weights,) = call(
        fold_kernel,
        [((2 * value_width, width), BF16)],
        [value_up, head_gain, out_attn, out_rec],
        ids=False,
        cost=pl.CostEstimate(flops=10**8, bytes_accessed=1 << 20, transcendentals=0),
    )
    other_weights = lax.ppermute(weights, "tp", partner)
    shared = lax.ppermute(share, "tp", partner)

    blank = np.zeros((2, state_rows, value_width), np.float32)
    blank[:, key_width + 1] = NEG
    prefix = jnp.asarray(blank)
    wide = (16 << 20) if peers <= 16 else (40 << 20)
    for level, radix in enumerate(radices[:-1]):
        received = [
            lax.ppermute(message, "sp", digit_pairs(peers, strides[level], radix, k))
            for k in range(1, radix)
        ]
        last = level == len(radices) - 2
        kv_rows *= radix
        count = radices[-1] - 1 if last else 1
        out_rows = kv_rows + (1 if last else 2) * state_rows
        prefix, sides, *messages = call(
            functools.partial(
                merge_kernel,
                slot=2 + level,
                radix=radix,
                state_rows=state_rows,
                last=last,
                next_radix=radices[level + 1],
            ),
            [((2, state_rows, value_width), F32), ((2 * state_rows, value_width), BF16)]
            + [((out_rows, value_width), BF16)] * max(count, 1),
            [ids, prefix, message] + received,
            limit=wide,
        )
        message = messages[0]
    level, radix = len(radices) - 1, radices[-1]
    received = []
    for k in range(1, radix):
        pairs = digit_pairs(peers, strides[level], radix, k)
        received.append(lax.ppermute(messages[k - 1], "sp", pairs))
    other_sides = lax.ppermute(sides, "tp", partner)
    (packed,) = call(
        functools.partial(pack_kernel, count=radix, state_rows=state_rows),
        [((radix * kv_rows + (radix - 1) * state_rows, value_width), BF16)],
        [other_weights, shared, other_sides, message] + received,
        ids=False,
        limit=wide,
    )
    swapped = lax.ppermute(packed, "tp", partner)
    level_facts = dict(
        slot=2 + level,
        radix=radix,
        state_rows=state_rows,
        floor_value=float(seq * peers) ** 0.5,
        score_scale=(nope + rope) ** (-0.5),
    )
    half = call(
        functools.partial(half_kernel, **level_facts),
        [((seq // 2, value_width), BF16)] + [((seq, value_width), F32)] * 3,
        [ids, packed, sides, kept, shared],
        limit=wide,
        cost=pl.CostEstimate(flops=10**8, bytes_accessed=1 << 20, transcendentals=0),
    )
    step = seq // lanes

    def mixed(piece, dtype):
        return call(
            functools.partial(
                mix_kernel,
                piece=piece,
                step=step,
                **level_facts,
            ),
            [((step, width), dtype)],
            [
                ids,
                swapped,
                other_sides,
                kept,
                shared,
                *half,
                weights,
                other_weights,
            ],
            limit=wide if peers <= 16 else 56 << 20,
            cost=pl.CostEstimate(flops=10**8, bytes_accessed=1 << 20, transcendentals=0),
        )[0]

    arrived = []
    for k in range(1, pieces):
        piece = mixed(k, BF16)
        arrived.append(lax.ppermute(piece, "tp", ring[k]))
    total = mixed(0, F32)
    for piece in arrived:
        total = total + piece.astype(F32)
    return total.astype(BF16)


def solution(mesh):
    in_specs = (
        P(("sp", "tp"), None),
        P(),
        P(),
        P(),
        P(),
        P(),
        P(),
        P(None, "tp"),
        P(None, "tp"),
        P(None, "tp"),
        P(None, "tp"),
        P(None, "tp"),
        P(None, "tp"),
        P(None, "tp"),
        P(None, None, "tp"),
        P("sp", None, "tp"),
        P("tp"),
        P(None, "tp", None, None),
        P(None, "tp", None),
        P("tp", None),
        P("tp", None),
    )
    out_specs = P(("sp", "tp"), None)

    return jax.shard_map(shards, mesh=mesh, in_specs=in_specs, out_specs=out_specs, check_vma=False)
```

```python
import functools

import jax
import jax.numpy as jnp
import numpy as np
from jax import lax
from jax.experimental import pallas as pl
from jax.experimental.pallas import tpu as pltpu
from jax.sharding import PartitionSpec as P

EPS = 1e-06
NEG = -(2.0**100)
AUX = 8
F32 = jnp.float32
BF16 = jnp.bfloat16
NT = (((1,), (1,)), ((), ()))


def radices_of(peers):
    first = 2 if peers % 2 == 0 else 1
    rest = peers // first
    radices = [first]
    while rest > 1:
        step = 4 if rest % 4 == 0 else next(p for p in range(2, rest + 1) if rest % p == 0)
        radices.append(step)
        rest //= step
    if len(radices) == 1:
        radices.append(1)
    return radices


def peer_digit(digit, radix, k, sending):
    if radix & (radix - 1) == 0:
        return digit ^ k
    return (digit + k if sending else digit - k + radix) % radix


def digit_pairs(peers, stride, radix, k):
    pairs = []
    for i in range(peers):
        digit = (i // stride) % radix
        pairs.append((i, i + (peer_digit(digit, radix, k, True) - digit) * stride))
    return pairs


def dot(a, b):
    return jnp.dot(a, b, preferred_element_type=F32)


def dot_nt(a, b):
    return lax.dot_general(a, b, NT, preferred_element_type=F32)


def dot_split(a, b):
    high = a.astype(BF16)
    low = (a - high.astype(F32)).astype(BF16)
    return dot(high, b) + dot(low, b)


def rms(values, gain):
    return values * lax.rsqrt(jnp.mean(values * values, axis=-1, keepdims=True) + EPS) * gain


def iota2(rows, cols, dim):
    return lax.broadcasted_iota(jnp.int32, (rows, cols), dim)


def turned_rows(weight_t):
    half = weight_t.shape[0] // 2
    return jnp.concatenate([weight_t, -weight_t[half:], weight_t[:half]], axis=0)


def angle_table(ids_ref, cos_base, sin_base, cos_row, sin_row):
    block = ids_ref[1]
    cb, sb = cos_base[pl.ds(block, 1), :], sin_base[pl.ds(block, 1), :]
    cr, sr = cos_row[...], sin_row[...]
    cos, sin = cb * cr - sb * sr, sb * cr + cb * sr
    half = cr.shape[1] // 2
    return jnp.where(iota2(cr.shape[0], cr.shape[1], 1) < half, cos, sin)


def rotated(product, table):
    mixed = product * table
    return mixed + pltpu.roll(mixed, product.shape[1] // 2, 1)


def aux_rows(n_row, peak_row, keep_row):
    high = keep_row.astype(BF16).astype(F32)
    mid = (keep_row - high).astype(BF16).astype(F32)
    low = keep_row - high - mid
    pad = jnp.zeros((AUX - 5, n_row.shape[1]), F32)
    return jnp.concatenate([n_row, peak_row, high, mid, low, pad], axis=0)


def read_state(block):
    c_rows = block.shape[0] - AUX
    block = block.astype(F32)
    aux = block[c_rows:]
    return block[:c_rows], aux[0:1], aux[1:2], aux[2:3] + aux[3:4] + aux[4:5]


def placed(state, place, use=None):
    c_part, n_part, peak, keep = state
    if use is not None:
        peak, keep = jnp.where(use, peak, NEG), jnp.where(use, keep, 0.0)
    return c_part, n_part, peak, keep, place


def chain(states):
    logs = []
    total = functools.reduce(jnp.add, [state[3] for state in states])
    for index, (_, _, peak, _, place) in enumerate(states):
        log = peak
        for other, (_, _, _, keep, at) in enumerate(states):
            if other != index:
                log = log + jnp.where(at > place, keep, 0.0)
        logs.append(log)
    return logs, functools.reduce(jnp.maximum, logs), total


def weighted(states, logs, top):
    c_sum = n_sum = None
    for state, log in zip(states, logs):
        weight = jnp.exp(log - top)
        c_part, n_part = weight * state[0], weight * state[1]
        c_sum = c_part if c_sum is None else c_sum + c_part
        n_sum = n_part if n_sum is None else n_sum + n_part
    return c_sum, n_sum


def joined(states):
    logs, top, keep = chain(states)
    top = top.astype(BF16).astype(F32)
    c_sum, n_sum = weighted(states, logs, top)
    return jnp.concatenate([c_sum, aux_rows(n_sum, top, keep)], axis=0)


def log_sigmoid(x):
    return jnp.minimum(x, 0.0) - jnp.log(1.0 + jnp.exp(-jnp.abs(x)))


def head_kernel(
    ids,
    *refs,
    pieces,
    key_width,
):
    piece_refs = refs[: 2 * pieces]
    (
        in_gain,
        kv_down,
        kv_gain,
        rope_t,
        key_t,
        rec_value,
        gate_t,
        level,
        cos_base,
        sin_base,
        cos_row,
        sin_row,
        message,
        normed_out,
        keys_out,
        values_out,
        rows_out,
        table_out,
        rows,
    ) = refs[2 * pieces :]
    mine = ids[0]
    pair, core = mine // 2, mine % 2
    step = piece_refs[0].shape[0]
    seq = rows.shape[0]
    for k in range(pieces):
        source = lax.rem(pair - k + pieces, pieces) * 2
        rows[pl.ds(pl.multiple_of((source + core) * step, step), step), :] = piece_refs[2 * k][...]
        rows[pl.ds(pl.multiple_of((source + 1 - core) * step, step), step), :] = piece_refs[
            2 * k + 1
        ][...]
    normed = rms(rows[...].astype(F32), in_gain[...]).astype(BF16)
    normed_out[...] = normed
    table = angle_table(ids, cos_base, sin_base, cos_row, sin_row)
    table_out[...] = table
    latent = kv_down.shape[1]
    straight = dot(normed, jnp.concatenate([kv_down[...], rec_value[...]], axis=1))
    turned = turned_rows(rope_t[...])
    gate_rows = gate_t.shape[0]
    fill = jnp.zeros((turned.shape[0] - key_width - gate_rows, turned.shape[1]), BF16)
    crossed = dot_nt(
        normed, jnp.concatenate([turned, key_t[...], gate_t[...], fill], axis=0)
    )
    rope_lanes = turned.shape[0]
    lat = rms(straight[:, :latent], kv_gain[...]).astype(BF16)
    rope = rotated(crossed[:, :rope_lanes], table)
    half = seq // 2
    quarter = half // 2
    lat = jnp.where(core == 0, lat[:half], lat[half:])
    rope = jnp.where(core == 0, rope[:half], rope[half:])
    lanes = iota2(quarter, rope.shape[1], 1)
    packed = jnp.where(lanes < rope_t.shape[0], rope[:quarter], rope[quarter:])
    message[0:half, :] = lat
    message[half : half + quarter, :] = packed.astype(BF16)

    mixed = crossed[:, rope_lanes:]
    keys = mixed.astype(BF16).astype(F32) * key_width ** (-0.5)
    keys = jnp.where(iota2(seq, keys.shape[1], 1) < key_width, keys, 0.0)
    keys_out[...] = keys.astype(BF16)
    values = straight[:, latent:].astype(BF16)
    values_out[...] = values
    mixed_t = jnp.transpose(mixed)
    gates = mixed_t[key_width : key_width + 8]

    in_f, in_b = gates[0:1], gates[2:3]
    keep_f = log_sigmoid(gates[1:2] + level[0:1])
    keep_b = log_sigmoid(gates[3:4] + level[1:2])
    row_id, col_id = iota2(seq, seq, 0), iota2(seq, seq, 1)
    upper = jnp.where(row_id <= col_id, 1.0, 0.0).astype(BF16)
    lower = jnp.where(row_id >= col_id, 1.0, 0.0).astype(BF16)
    keeps = jnp.concatenate([keep_f, keep_b, jnp.zeros((6, seq), F32)], axis=0)
    high = keeps.astype(BF16)
    mid = (keeps - high.astype(F32)).astype(BF16)
    low = (keeps - high.astype(F32) - mid.astype(F32)).astype(BF16)
    thirds = jnp.concatenate([high, mid, low, jnp.zeros_like(low)], axis=0)
    cums = dot(thirds, jnp.concatenate([upper, lower], axis=1))
    cums = cums[0:8] + cums[8:16] + cums[16:24]
    cum_f, cum_b = cums[0:1, :seq], cums[1:2, seq:]
    all_f, all_b = cum_f[:, seq - 1 : seq], cum_b[:, 0:1]
    rows_out[...] = jnp.concatenate(
        [cum_f, in_f - cum_f, cum_b, in_b - cum_b, jnp.zeros((4, seq), F32)], axis=0
    )
    keys_t = mixed_t[:key_width].astype(BF16).astype(F32) * key_width ** (-0.5)
    base = half + quarter
    weights = []
    for cum, log_in, total in ((cum_f, in_f, all_f), (cum_b, in_b, all_b)):
        logs = total - cum + log_in
        peak = jnp.max(logs, axis=1, keepdims=True).astype(BF16).astype(F32)
        weight = jnp.exp(logs - peak)
        weights.append((weight, peak, total))
    w_f, w_b = weights[0][0], weights[1][0]
    c_both = dot_split(jnp.concatenate([keys_t * w_f, keys_t * w_b], axis=0), values)
    n_both = dot_split(
        jnp.concatenate([w_f, w_b, jnp.zeros((6, seq), F32)], axis=0), keys.astype(BF16)
    )
    for index in range(2):
        _, peak, total = weights[index]
        c_part = c_both[index * key_width : (index + 1) * key_width]
        n_row = n_both[index : index + 1]
        zero = jnp.zeros_like(n_row)
        block = jnp.concatenate([c_part, aux_rows(n_row, zero + peak, zero + total)], axis=0)
        at = base + index * (key_width + AUX)
        message[at : at + key_width + AUX, :] = block.astype(BF16)


def thirds_of(x):
    high = x.astype(BF16)
    mid = (x - high.astype(F32)).astype(BF16)
    low = (x - high.astype(F32) - mid.astype(F32)).astype(BF16)
    return [high, mid, low]


def local_kernel(
    ids,
    normed_ref,
    keys_ref,
    values_ref,
    rows_ref,
    table_ref,
    query_down,
    query_gain,
    nope_up,
    rope_up_t,
    key_up,
    rec_query_t,
    init_state,
    init_norm,
    keep_out,
    share_out,
    whole,
    *,
    pieces,
):
    normed = normed_ref[...]
    seq = normed.shape[0]
    query_rows = jnp.concatenate([rec_query_t[...], jnp.zeros_like(rec_query_t)], axis=0)
    rec_q = dot_nt(normed, query_rows).astype(BF16)
    q_lat = rms(dot(normed, query_down[...]), query_gain[...]).astype(BF16)
    nope = dot(q_lat, nope_up[...]).astype(BF16)
    rope = rotated(dot_nt(q_lat, turned_rows(rope_up_t[...])), table_ref[...])
    lat = dot_nt(nope, key_up[...]).astype(BF16)
    width = rope_up_t.shape[0]
    lanes = iota2(seq, rope.shape[1], 1)
    low_rope = jnp.where(lanes < width, rope, 0.0).astype(BF16)
    high_rope = jnp.where(lanes >= width, rope, 0.0).astype(BF16)
    values = values_ref[...]
    wide = jnp.concatenate([values, jnp.ones_like(values)], axis=1)
    products = dot_nt(rec_q, keys_ref[...])
    row_id, col_id = iota2(seq, seq, 0), iota2(seq, seq, 1)
    rows = rows_ref[...]
    numers, denoms, marks = [], [], []
    for index in range(2):
        cum = jnp.transpose(jnp.broadcast_to(rows[2 * index : 2 * index + 1], (seq, seq)))
        seen = row_id >= col_id if index == 0 else row_id <= col_id
        logs = jnp.where(seen, cum + rows[2 * index + 1 : 2 * index + 2], NEG)
        peak = jnp.max(logs, axis=1, keepdims=True)
        gated = products * jnp.exp(logs - peak)
        sums = dot_split(gated, wide)
        numers.append(sums[:, : values.shape[1]].astype(BF16))
        denoms.append(sums[:, values.shape[1] :].astype(BF16))
        marks += thirds_of(jnp.broadcast_to(peak, (seq, seq))) + thirds_of(cum)
    columns = [lat, low_rope, high_rope] + numers + denoms + [rec_q] + marks
    step_cols = lat.shape[1]
    for index, column in enumerate(columns):
        whole[:, index * step_cols : (index + 1) * step_cols] = column
    mine = ids[0]
    pair, core = mine // 2, mine % 2
    step = seq // (2 * pieces)
    for side, out in ((core, keep_out), (1 - core, share_out)):
        for k in range(pieces):
            owner = lax.rem(pair + k, pieces) * 2 + side
            out[k * step : (k + 1) * step, 0 : whole.shape[1]] = whole[
                pl.ds(pl.multiple_of(owner * step, step), step), :
            ]
    lanes = init_state.shape[2]
    norms = init_norm[...]
    norms = jnp.concatenate([norms, jnp.zeros((2, lanes - norms.shape[1]), F32)], axis=1)
    rest = jnp.zeros((init_state.shape[1] - 2, lanes), F32)
    first = jnp.concatenate([norms, rest], axis=0).astype(BF16)
    starts = [init_state[0].astype(BF16), init_state[1].astype(BF16), first]
    for out in (keep_out, share_out):
        for index, block in enumerate(starts):
            at = whole.shape[1] + index * lanes
            out[0 : block.shape[0], at : at + lanes] = block


def fold_kernel(value_up, head_gain, out_attn, out_rec, out):
    rows = value_up.shape[0]
    out[0:rows, :] = dot(value_up[...], out_attn[...]).astype(BF16)
    gain = head_gain[...]
    width = gain.shape[1]
    column = jnp.transpose(jnp.broadcast_to(gain, (width, width)))[:, 0:1]
    out[rows:, :] = (column * out_rec[...].astype(F32)).astype(BF16)


def level_states(ids, slot, radix, fetch):
    digit = ids[slot]
    forward, backward = [], []
    for k in range(1, radix):
        source = peer_digit(digit, radix, k, False)
        forward.append(placed(fetch(k, 0), source, source < digit))
        backward.append(placed(fetch(k, 1), -source, source > digit))
    return forward, backward


def merge_kernel(ids, *refs, slot, radix, state_rows, last, next_radix):
    prefix_in = refs[0]
    own = refs[1]
    received = (own,) + refs[2 : 1 + radix]
    outs = refs[1 + radix :]
    state_out, messages = outs[0], outs[1:]
    kv_rows = own.shape[0] - 2 * state_rows

    def fetch(k, direction):
        at = kv_rows + direction * state_rows
        return read_state(received[k][at : at + state_rows, :])

    digit = ids[slot]
    totals = []
    for direction in range(2):
        sign = 1 - 2 * direction
        at = slice(direction * state_rows, (direction + 1) * state_rows)
        inner = placed(read_state(prefix_in[at, :]), sign * digit)
        before, whole = [inner], [placed(fetch(0, direction), sign * digit)]
        for k in range(1, radix):
            source = peer_digit(digit, radix, k, False)
            state = fetch(k, direction)
            before.append(placed(state, sign * source, sign * source < sign * digit))
            whole.append(placed(state, sign * source))
        at = slice(direction * state_rows, (direction + 1) * state_rows)
        state_out[at, :] = joined(before).astype(state_out.dtype)
        totals.append(joined(whole).astype(BF16))
    total_f, total_b = totals
    part = kv_rows // 3
    for number, message in enumerate(messages):
        for section in range(3):
            for k in range(radix):
                to = (section * radix + k) * part
                message[to : to + part, :] = received[k][section * part : (section + 1) * part, :]
        at = radix * kv_rows
        if last:
            target = peer_digit(ids[slot + 1], next_radix, number + 1, True)
            ahead = target > ids[slot + 1]
            message[at : at + state_rows, :] = jnp.where(ahead, total_f, total_b)
        else:
            message[at : at + state_rows, :] = total_f
            message[at + state_rows : at + 2 * state_rows, :] = total_b


def load_kernel(*refs):
    count = (len(refs) - 1) // 2
    sems = refs[-1]
    copies = [
        pltpu.make_async_copy(refs[i], refs[count + i], sems.at[i]) for i in range(count)
    ]
    for copy in copies:
        copy.start()
    for copy in copies:
        copy.wait()


def pack_kernel(*refs, count, state_rows):
    received, out = refs[-1 - count : -1], refs[-1]
    part = (received[0].shape[0] - state_rows) // 3
    for k, message in enumerate(received):
        for section in range(3):
            to = (section * count + k) * part
            out[to : to + part, :] = message[section * part : (section + 1) * part, :]
        if k > 0:
            to = 3 * count * part + (k - 1) * state_rows
            out[to : to + state_rows, :] = message[3 * part : 3 * part + state_rows, :]


def attend(sections, keys, part, score_scale):
    rope = keys[2 * part : 3 * part, :]
    scores, lats = [], []
    for section in range(2):
        lat = keys[section * part : (section + 1) * part, :]
        lats.append(lat)
        scores.append(dot_nt(sections[section], jnp.concatenate([lat, rope], axis=1)) * score_scale)
    top = functools.reduce(jnp.maximum, [jnp.max(s, axis=1, keepdims=True) for s in scores])
    mass = accum = None
    for part_scores, lat in zip(scores, lats):
        expo = jnp.exp(part_scores - top)
        gain = dot(expo.astype(BF16), lat)
        total = jnp.sum(expo, axis=1, keepdims=True)
        accum = gain if accum is None else accum + gain
        mass = total if mass is None else mass + total
    return top, mass, accum


def sections_of(queries, width):
    return [
        queries[:, 0 : 2 * width],
        jnp.concatenate([queries[:, 0:width], queries[:, 2 * width :]], axis=1),
    ]


def finished(ids, block, first_ref, packed, sides, slot, radix, state_rows, floor_value):
    base = packed.shape[0] - (radix - 1) * state_rows
    width = packed.shape[1]

    def column(index):
        return block[:, index * width : (index + 1) * width].astype(F32)

    def triple(index):
        return column(index) + column(index + 1) + column(index + 2)

    def fetch(k, direction):
        at = base + (k - 1) * state_rows
        return read_state(packed[at : at + state_rows, :])

    levels = level_states(ids, slot, radix, fetch)
    rec_q = block[:, 7 * width : 8 * width]
    starts = []
    for index in range(2):
        inner = read_state(sides[index * state_rows : (index + 1) * state_rows, :])
        zero = jnp.zeros_like(inner[1])
        first = (
            first_ref[:, (20 + index) * width : (21 + index) * width].astype(F32),
            first_ref[0:8, 22 * width :].astype(F32)[index : index + 1],
            zero,
            zero,
        )
        states = [placed(first, -radix)] + levels[index]
        states.append(placed(inner, ids[slot] if index == 0 else -ids[slot]))
        logs, start_top, _ = chain(states)
        starts.append(weighted(states, logs, start_top) + (start_top,))
    c_start = jnp.concatenate([starts[0][0], starts[1][0]], axis=1)
    pad = jnp.zeros((rec_q.shape[1] - c_start.shape[0], c_start.shape[1]), F32)
    c_start = jnp.concatenate([c_start, pad], axis=0)
    high = c_start.astype(BF16)
    low = (c_start - high.astype(F32)).astype(BF16)
    products = dot(rec_q, high) + dot(rec_q, low)
    summed = None
    for index in range(2):
        _, n_start, start_top = starts[index]
        from_start = products[:, index * width : (index + 1) * width]
        norm_start = jnp.sum(rec_q.astype(F32) * n_start, axis=1, keepdims=True)
        numer, denom = column(3 + index), column(5 + index)
        peak, carry = triple(8 + 6 * index), triple(11 + 6 * index) + start_top
        row_max = jnp.maximum(peak, carry)
        here, there = jnp.exp(peak - row_max), jnp.exp(carry - row_max)
        numer = here * numer + there * from_start
        denom = here * denom + there * norm_start
        result = numer / jnp.maximum(jnp.abs(denom), floor_value * jnp.exp(-row_max))
        summed = result if summed is None else summed + result
    return rms(summed, 1.0).astype(BF16)


def half_kernel(
    ids,
    packed,
    sides,
    kept,
    shared,
    recurrent_out,
    top_out,
    mass_out,
    accum_out,
    *,
    slot,
    radix,
    state_rows,
    floor_value,
    score_scale,
):
    width = packed.shape[1]
    part = (packed.shape[0] - (radix - 1) * state_rows) // 3
    recurrent_out[...] = finished(
        ids, kept[...], kept, packed, sides, slot, radix, state_rows, floor_value
    )
    queries = jnp.concatenate([kept[:, 0 : 3 * width], shared[:, 0 : 3 * width]], axis=0)
    top, mass, accum = attend(sections_of(queries, width), packed, part, score_scale)
    top_out[...] = jnp.broadcast_to(top, top_out.shape)
    mass_out[...] = jnp.broadcast_to(mass, mass_out.shape)
    accum_out[...] = accum


def mix_kernel(
    ids,
    swapped,
    sides,
    kept,
    shared,
    recurrent,
    top_half,
    mass_half,
    accum_half,
    weights,
    other_weights,
    out,
    *,
    slot,
    radix,
    state_rows,
    floor_value,
    score_scale,
    piece,
    step,
):
    width = swapped.shape[1]
    part = (swapped.shape[0] - (radix - 1) * state_rows) // 3
    at = slice(piece * step, (piece + 1) * step)
    also = slice(kept.shape[0] + piece * step, kept.shape[0] + (piece + 1) * step)
    queries = jnp.concatenate([kept[at, 0 : 3 * width], shared[at, 0 : 3 * width]], axis=0)
    top, mass, accum = attend(sections_of(queries, width), swapped, part, score_scale)

    def both(ref):
        return jnp.concatenate([ref[at, :], ref[also, :]], axis=0)

    other_top = both(top_half)
    peak = jnp.maximum(top, other_top)
    here, there = jnp.exp(top - peak), jnp.exp(other_top - peak)
    accum = here * accum + there * both(accum_half)
    mass = here * mass + there * both(mass_half)
    attended = (accum / mass).astype(BF16)
    other = finished(
        ids, shared[at, :], shared, swapped, sides, slot, radix, state_rows, floor_value
    )
    mine = jnp.concatenate([attended[:step], recurrent[at, :]], axis=1)
    theirs = jnp.concatenate([attended[step:], other], axis=1)
    out[...] = (dot(mine, weights[...]) + dot(theirs, other_weights[...])).astype(out.dtype)


def call(kernel, outs, inputs, scratch=(), ids=True, limit=16 << 20, cost=None):
    vmem = pl.BlockSpec(memory_space=pltpu.VMEM)
    in_specs = [vmem] * len(inputs)
    if ids:
        in_specs[0] = pl.BlockSpec(memory_space=pltpu.SMEM)
    return pl.pallas_call(
        kernel,
        out_shape=[jax.ShapeDtypeStruct(shape, dtype) for shape, dtype in outs],
        in_specs=in_specs,
        out_specs=[vmem] * len(outs),
        scratch_shapes=scratch,
        cost_estimate=cost,
        compiler_params=pltpu.CompilerParams(vmem_limit_bytes=limit),
    )(*inputs)


def shards(
    rows_in,
    in_gain,
    query_down,
    query_gain,
    kv_down,
    kv_gain,
    rope_down,
    query_nope_up,
    query_rope_up,
    key_up,
    value_up,
    rec_query,
    rec_key,
    rec_value,
    gate_weight,
    forget_level,
    head_gain,
    init_state,
    init_norm,
    out_attn,
    out_rec,
):
    peers, lanes = lax.axis_size("sp"), lax.axis_size("tp")
    block, mine = lax.axis_index("sp"), lax.axis_index("tp")
    seq = forget_level.shape[0]
    width = rows_in.shape[1]
    nope, rope = key_up.shape[1], rope_down.shape[1]
    key_width, value_width = init_state.shape[2], init_state.shape[3]
    pieces = lanes // 2
    radices = radices_of(peers)
    strides = [int(np.prod(radices[:i])) for i in range(len(radices))]
    divide = np.array([1, 1] + strides, np.int32)
    modulo = np.array([lanes, peers] + radices, np.int32)
    first = np.arange(len(divide)) == 0
    ids = (jnp.where(first, mine, block).astype(jnp.int32) // divide) % modulo

    partner = [(i, i ^ 1) for i in range(lanes)]
    ring = [[(i, (i + 2 * k) % lanes) for i in range(lanes)] for k in range(pieces)]

    gathered = [rows_in]
    for k in range(1, pieces):
        gathered.append(lax.ppermute(rows_in, "tp", ring[k]))
    row_pieces = []
    for piece in gathered:
        row_pieces += [piece, lax.ppermute(piece, "tp", partner)]

    freq = 10000.0 ** (-np.arange(rope // 2, dtype=np.float64) / (rope // 2))
    freq = np.tile(freq, 4)[None, :]
    base = np.arange(peers, dtype=np.float64)[:, None] * seq * freq
    within = np.arange(seq, dtype=np.float64)[:, None] * freq
    tables = [np.cos(base), np.sin(base), np.cos(within), np.sin(within)]
    tables = [jnp.asarray(table.astype(np.float32)) for table in tables]

    held = [
        in_gain[None, :],
        kv_down,
        kv_gain[None, :],
        rope_down.T,
        rec_key.T,
        rec_value,
        gate_weight[:, :, 0].T,
        forget_level[:, :, 0].T,
        *tables,
        query_down,
        query_gain[None, :],
        query_nope_up,
        query_rope_up.T,
        key_up,
        rec_query.T,
        value_up,
        head_gain[None, :],
        init_state[:, 0],
        init_norm[:, 0],
        out_attn,
        out_rec,
    ]
    held = list(
        pl.pallas_call(
            load_kernel,
            out_shape=[pltpu.VMEM(array.shape, array.dtype) for array in held],
            in_specs=[pl.BlockSpec(memory_space=pltpu.HBM)] * len(held),
            out_specs=[pl.BlockSpec(memory_space=pltpu.VMEM)] * len(held),
            scratch_shapes=[pltpu.SemaphoreType.DMA((len(held),))],
            name="load",
            cost_estimate=pl.CostEstimate(flops=10**8, bytes_accessed=1 << 22, transcendentals=0),
            compiler_params=pltpu.CompilerParams(vmem_limit_bytes=16 << 20),
        )(*[pltpu.with_memory_space_constraint(array, pltpu.HBM) for array in held])
    )
    head_args, local_args = held[:12], held[12:18]
    value_up, head_gain, init_state, init_norm, out_attn, out_rec = held[18:]

    state_rows = key_width + AUX
    kv_rows = seq // 2 + seq // 4
    message, normed, keys, values, gate_rows, table = call(
        functools.partial(head_kernel, pieces=pieces, key_width=key_width),
        [
            ((kv_rows + 2 * state_rows, value_width), BF16),
            ((seq, width), BF16),
            ((seq, 2 * key_width), BF16),
            ((seq, value_width), BF16),
            ((8, seq), F32),
            ((seq, 2 * rope), F32),
        ],
        [ids]
        + row_pieces
        + head_args,
        scratch=[pltpu.VMEM((seq, width), BF16)],
    )
    columns = 20 * value_width
    assert key_width == seq // 2
    kept, share = call(
        functools.partial(local_kernel, pieces=pieces),
        [((seq // 2, columns + 3 * value_width), BF16)] * 2,
        [
            ids,
            normed,
            keys,
            values,
            gate_rows,
            table,
            *local_args,
            init_state,
            init_norm,
        ],
        scratch=[pltpu.VMEM((seq, columns), BF16)],
        cost=pl.CostEstimate(flops=10**8, bytes_accessed=1 << 20, transcendentals=0),
    )
    (weights,) = call(
        fold_kernel,
        [((2 * value_width, width), BF16)],
        [value_up, head_gain, out_attn, out_rec],
        ids=False,
        cost=pl.CostEstimate(flops=10**8, bytes_accessed=1 << 20, transcendentals=0),
    )
    other_weights = lax.ppermute(weights, "tp", partner)
    shared = lax.ppermute(share, "tp", partner)

    blank = np.zeros((2, state_rows, value_width), np.float32)
    blank[:, key_width + 1] = NEG
    sides = jnp.asarray(blank.reshape(2 * state_rows, value_width))
    wide = (16 << 20) if peers <= 16 else (40 << 20)
    for level, radix in enumerate(radices[:-1]):
        received = [
            lax.ppermute(message, "sp", digit_pairs(peers, strides[level], radix, k))
            for k in range(1, radix)
        ]
        last = level == len(radices) - 2
        kv_rows *= radix
        count = radices[-1] - 1 if last else 1
        out_rows = kv_rows + (1 if last else 2) * state_rows
        sides, *messages = call(
            functools.partial(
                merge_kernel,
                slot=2 + level,
                radix=radix,
                state_rows=state_rows,
                last=last,
                next_radix=radices[level + 1],
            ),
            [((2 * state_rows, value_width), BF16 if last else F32)]
            + [((out_rows, value_width), BF16)] * max(count, 1),
            [ids, sides, message] + received,
            limit=wide,
        )
        message = messages[0]
    level, radix = len(radices) - 1, radices[-1]
    received = []
    for k in range(1, radix):
        pairs = digit_pairs(peers, strides[level], radix, k)
        received.append(lax.ppermute(messages[k - 1], "sp", pairs))
    other_sides = lax.ppermute(sides, "tp", partner)
    (packed,) = call(
        functools.partial(pack_kernel, count=radix, state_rows=state_rows),
        [((radix * kv_rows + (radix - 1) * state_rows, value_width), BF16)],
        [other_weights, shared, other_sides, message] + received,
        ids=False,
        limit=wide,
    )
    swapped = lax.ppermute(packed, "tp", partner)
    level_facts = dict(
        slot=2 + level,
        radix=radix,
        state_rows=state_rows,
        floor_value=float(seq * peers) ** 0.5,
        score_scale=(nope + rope) ** (-0.5),
    )
    half = call(
        functools.partial(half_kernel, **level_facts),
        [((seq // 2, value_width), BF16)] + [((seq, value_width), F32)] * 3,
        [ids, packed, sides, kept, shared],
        limit=wide,
        cost=pl.CostEstimate(flops=10**8, bytes_accessed=1 << 20, transcendentals=0),
    )
    step = seq // lanes

    def mixed(piece, dtype):
        return call(
            functools.partial(
                mix_kernel,
                piece=piece,
                step=step,
                **level_facts,
            ),
            [((step, width), dtype)],
            [
                ids,
                swapped,
                other_sides,
                kept,
                shared,
                *half,
                weights,
                other_weights,
            ],
            limit=wide if peers <= 16 else 56 << 20,
            cost=pl.CostEstimate(flops=10**8, bytes_accessed=1 << 20, transcendentals=0),
        )[0]

    arrived = []
    for k in range(1, pieces):
        piece = mixed(k, BF16)
        arrived.append(lax.ppermute(piece, "tp", ring[k]))
    total = mixed(0, F32)
    for piece in arrived:
        total = total + piece.astype(F32)
    return total.astype(BF16)


def solution(mesh):
    in_specs = (
        P(("sp", "tp"), None),
        P(),
        P(),
        P(),
        P(),
        P(),
        P(),
        P(None, "tp"),
        P(None, "tp"),
        P(None, "tp"),
        P(None, "tp"),
        P(None, "tp"),
        P(None, "tp"),
        P(None, "tp"),
        P(None, None, "tp"),
        P("sp", None, "tp"),
        P("tp"),
        P(None, "tp", None, None),
        P(None, "tp", None),
        P("tp", None),
        P("tp", None),
    )
    out_specs = P(("sp", "tp"), None)

    return jax.shard_map(shards, mesh=mesh, in_specs=in_specs, out_specs=out_specs, check_vma=False)
```

```python
import functools

import jax
import jax.numpy as jnp
import numpy as np
from jax import lax
from jax.experimental import pallas as pl
from jax.experimental.pallas import tpu as pltpu
from jax.sharding import PartitionSpec as P

EPS = 1e-06
NEG = -(2.0**100)
AUX = 8
F32 = jnp.float32
BF16 = jnp.bfloat16
NT = (((1,), (1,)), ((), ()))


def radices_of(peers):
    first = 2 if peers % 2 == 0 else 1
    rest = peers // first
    radices = [first]
    while rest > 1:
        step = 4 if rest % 4 == 0 else next(p for p in range(2, rest + 1) if rest % p == 0)
        radices.append(step)
        rest //= step
    if len(radices) == 1:
        radices.append(1)
    return radices


def peer_digit(digit, radix, k, sending):
    if radix & (radix - 1) == 0:
        return digit ^ k
    return (digit + k if sending else digit - k + radix) % radix


def digit_pairs(peers, stride, radix, k):
    pairs = []
    for i in range(peers):
        digit = (i // stride) % radix
        pairs.append((i, i + (peer_digit(digit, radix, k, True) - digit) * stride))
    return pairs


def dot(a, b):
    return jnp.dot(a, b, preferred_element_type=F32)


def dot_nt(a, b):
    return lax.dot_general(a, b, NT, preferred_element_type=F32)


def dot_split(a, b):
    high = a.astype(BF16)
    low = (a - high.astype(F32)).astype(BF16)
    return dot(high, b) + dot(low, b)


def rms(values, gain):
    return values * lax.rsqrt(jnp.mean(values * values, axis=-1, keepdims=True) + EPS) * gain


def iota2(rows, cols, dim):
    return lax.broadcasted_iota(jnp.int32, (rows, cols), dim)


def turned_rows(weight_t):
    half = weight_t.shape[0] // 2
    return jnp.concatenate([weight_t, -weight_t[half:], weight_t[:half]], axis=0)


def angle_table(ids_ref, cos_base, sin_base, cos_row, sin_row):
    block = ids_ref[1]
    cb, sb = cos_base[pl.ds(block, 1), :], sin_base[pl.ds(block, 1), :]
    cr, sr = cos_row[...], sin_row[...]
    cos, sin = cb * cr - sb * sr, sb * cr + cb * sr
    half = cr.shape[1] // 2
    return jnp.where(iota2(cr.shape[0], cr.shape[1], 1) < half, cos, sin)


def rotated(product, table):
    mixed = product * table
    return mixed + pltpu.roll(mixed, product.shape[1] // 2, 1)


def aux_rows(n_row, peak_row, keep_row):
    high = keep_row.astype(BF16).astype(F32)
    mid = (keep_row - high).astype(BF16).astype(F32)
    low = keep_row - high - mid
    pad = jnp.zeros((AUX - 5, n_row.shape[1]), F32)
    return jnp.concatenate([n_row, peak_row, high, mid, low, pad], axis=0)


def read_state(block):
    c_rows = block.shape[0] - AUX
    block = block.astype(F32)
    aux = block[c_rows:]
    return block[:c_rows], aux[0:1], aux[1:2], aux[2:3] + aux[3:4] + aux[4:5]


def placed(state, place, use=None):
    c_part, n_part, peak, keep = state
    if use is not None:
        peak, keep = jnp.where(use, peak, NEG), jnp.where(use, keep, 0.0)
    return c_part, n_part, peak, keep, place


def chain(states):
    logs = []
    total = functools.reduce(jnp.add, [state[3] for state in states])
    for index, (_, _, peak, _, place) in enumerate(states):
        log = peak
        for other, (_, _, _, keep, at) in enumerate(states):
            if other != index:
                log = log + jnp.where(at > place, keep, 0.0)
        logs.append(log)
    return logs, functools.reduce(jnp.maximum, logs), total


def weighted(states, logs, top):
    c_sum = n_sum = None
    for state, log in zip(states, logs):
        weight = jnp.exp(log - top)
        c_part, n_part = weight * state[0], weight * state[1]
        c_sum = c_part if c_sum is None else c_sum + c_part
        n_sum = n_part if n_sum is None else n_sum + n_part
    return c_sum, n_sum


def joined(states):
    logs, top, keep = chain(states)
    top = top.astype(BF16).astype(F32)
    c_sum, n_sum = weighted(states, logs, top)
    return jnp.concatenate([c_sum, aux_rows(n_sum, top, keep)], axis=0)


def log_sigmoid(x):
    return jnp.minimum(x, 0.0) - jnp.log(1.0 + jnp.exp(-jnp.abs(x)))


def norms_kernel(*refs):
    pieces, in_gain, out = refs[:-2], refs[-2], refs[-1]
    step = pieces[0].shape[0]
    for index, piece in enumerate(pieces):
        at = slice(index * step, (index + 1) * step)
        out[at, :] = rms(piece[...].astype(F32), in_gain[...]).astype(BF16)


def head_kernel(
    ids,
    ready,
    late,
    *refs,
    pieces,
    key_width,
):
    (
        in_gain,
        kv_down,
        kv_gain,
        rope_t,
        key_t,
        rec_value,
        gate_t,
        level,
        cos_base,
        sin_base,
        cos_row,
        sin_row,
        message,
        normed_out,
        keys_out,
        values_out,
        rows_out,
        table_out,
    ) = refs
    mine = ids[0]
    pair, core = mine // 2, mine % 2
    step = late.shape[0]
    seq = normed_out.shape[0]
    last = rms(late[...].astype(F32), in_gain[...]).astype(BF16)
    for index in range(2 * pieces):
        source = lax.rem(pair - index // 2 + pieces, pieces) * 2
        source += core if index % 2 == 0 else 1 - core
        if index < 2 * pieces - 1:
            block = ready[index * step : (index + 1) * step, :]
        else:
            block = last
        normed_out[pl.ds(pl.multiple_of(source * step, step), step), :] = block
    normed = normed_out[...]
    table = angle_table(ids, cos_base, sin_base, cos_row, sin_row)
    table_out[...] = table
    latent = kv_down.shape[1]
    straight = dot(normed, jnp.concatenate([kv_down[...], rec_value[...]], axis=1))
    turned = turned_rows(rope_t[...])
    gate_rows = gate_t.shape[0]
    fill = jnp.zeros((turned.shape[0] - key_width - gate_rows, turned.shape[1]), BF16)
    crossed = dot_nt(
        normed, jnp.concatenate([turned, key_t[...], gate_t[...], fill], axis=0)
    )
    rope_lanes = turned.shape[0]
    lat = rms(straight[:, :latent], kv_gain[...]).astype(BF16)
    rope = rotated(crossed[:, :rope_lanes], table)
    half = seq // 2
    quarter = half // 2
    lat = jnp.where(core == 0, lat[:half], lat[half:])
    rope = jnp.where(core == 0, rope[:half], rope[half:])
    lanes = iota2(quarter, rope.shape[1], 1)
    packed = jnp.where(lanes < rope_t.shape[0], rope[:quarter], rope[quarter:])
    message[0:half, :] = lat
    message[half : half + quarter, :] = packed.astype(BF16)

    mixed = crossed[:, rope_lanes:]
    keys = mixed.astype(BF16).astype(F32) * key_width ** (-0.5)
    keys = jnp.where(iota2(seq, keys.shape[1], 1) < key_width, keys, 0.0)
    keys_out[...] = keys.astype(BF16)
    values = straight[:, latent:].astype(BF16)
    values_out[...] = values
    mixed_t = jnp.transpose(mixed)
    gates = mixed_t[key_width : key_width + 8]

    in_f, in_b = gates[0:1], gates[2:3]
    keep_f = log_sigmoid(gates[1:2] + level[0:1])
    keep_b = log_sigmoid(gates[3:4] + level[1:2])
    row_id, col_id = iota2(seq, seq, 0), iota2(seq, seq, 1)
    upper = jnp.where(row_id <= col_id, 1.0, 0.0).astype(BF16)
    lower = jnp.where(row_id >= col_id, 1.0, 0.0).astype(BF16)
    keeps = jnp.concatenate([keep_f, keep_b, jnp.zeros((6, seq), F32)], axis=0)
    high = keeps.astype(BF16)
    mid = (keeps - high.astype(F32)).astype(BF16)
    low = (keeps - high.astype(F32) - mid.astype(F32)).astype(BF16)
    thirds = jnp.concatenate([high, mid, low, jnp.zeros_like(low)], axis=0)
    cums = dot(thirds, jnp.concatenate([upper, lower], axis=1))
    cums = cums[0:8] + cums[8:16] + cums[16:24]
    cum_f, cum_b = cums[0:1, :seq], cums[1:2, seq:]
    all_f, all_b = cum_f[:, seq - 1 : seq], cum_b[:, 0:1]
    rows_out[...] = jnp.concatenate(
        [cum_f, in_f - cum_f, cum_b, in_b - cum_b, jnp.zeros((4, seq), F32)], axis=0
    )
    keys_t = mixed_t[:key_width].astype(BF16).astype(F32) * key_width ** (-0.5)
    base = half + quarter
    weights = []
    for cum, log_in, total in ((cum_f, in_f, all_f), (cum_b, in_b, all_b)):
        logs = total - cum + log_in
        peak = jnp.max(logs, axis=1, keepdims=True).astype(BF16).astype(F32)
        weight = jnp.exp(logs - peak)
        weights.append((weight, peak, total))
    w_f, w_b = weights[0][0], weights[1][0]
    c_both = dot(jnp.concatenate([keys_t * w_f, keys_t * w_b], axis=0).astype(BF16), values)
    sums = jnp.concatenate([w_f, w_b, jnp.zeros((6, seq), F32)], axis=0)
    n_both = dot(sums.astype(BF16), keys.astype(BF16))
    for index in range(2):
        _, peak, total = weights[index]
        c_part = c_both[index * key_width : (index + 1) * key_width]
        n_row = n_both[index : index + 1]
        zero = jnp.zeros_like(n_row)
        block = jnp.concatenate([c_part, aux_rows(n_row, zero + peak, zero + total)], axis=0)
        at = base + index * (key_width + AUX)
        message[at : at + key_width + AUX, :] = block.astype(BF16)


def thirds_of(x):
    high = x.astype(BF16)
    mid = (x - high.astype(F32)).astype(BF16)
    low = (x - high.astype(F32) - mid.astype(F32)).astype(BF16)
    return [high, mid, low]


def local_kernel(
    ids,
    normed_ref,
    keys_ref,
    values_ref,
    rows_ref,
    table_ref,
    query_down,
    query_gain,
    nope_up,
    rope_up_t,
    key_up,
    rec_query_t,
    init_state,
    init_norm,
    keep_out,
    share_out,
    whole,
    *,
    pieces,
):
    normed = normed_ref[...]
    seq = normed.shape[0]
    query_rows = jnp.concatenate([rec_query_t[...], jnp.zeros_like(rec_query_t)], axis=0)
    rec_q = dot_nt(normed, query_rows).astype(BF16)
    q_lat = rms(dot(normed, query_down[...]), query_gain[...]).astype(BF16)
    nope = dot(q_lat, nope_up[...]).astype(BF16)
    rope = rotated(dot_nt(q_lat, turned_rows(rope_up_t[...])), table_ref[...])
    lat = dot_nt(nope, key_up[...]).astype(BF16)
    width = rope_up_t.shape[0]
    lanes = iota2(seq, rope.shape[1], 1)
    low_rope = jnp.where(lanes < width, rope, 0.0).astype(BF16)
    high_rope = jnp.where(lanes >= width, rope, 0.0).astype(BF16)
    values = values_ref[...]
    wide = jnp.concatenate([values, jnp.ones_like(values)], axis=1)
    products = dot_nt(rec_q, keys_ref[...])
    row_id, col_id = iota2(seq, seq, 0), iota2(seq, seq, 1)
    rows = rows_ref[...]
    numers, denoms, marks = [], [], []
    for index in range(2):
        cum = jnp.transpose(jnp.broadcast_to(rows[2 * index : 2 * index + 1], (seq, seq)))
        seen = row_id >= col_id if index == 0 else row_id <= col_id
        logs = jnp.where(seen, cum + rows[2 * index + 1 : 2 * index + 2], NEG)
        peak = jnp.max(logs, axis=1, keepdims=True)
        gated = products * jnp.exp(logs - peak)
        sums = dot_split(gated, wide)
        numers.append(sums[:, : values.shape[1]].astype(BF16))
        denoms.append(sums[:, values.shape[1] :].astype(BF16))
        marks += thirds_of(jnp.broadcast_to(peak, (seq, seq))) + thirds_of(cum)
    columns = [lat, low_rope, high_rope] + numers + denoms + [rec_q] + marks
    step_cols = lat.shape[1]
    for index, column in enumerate(columns):
        whole[:, index * step_cols : (index + 1) * step_cols] = column
    mine = ids[0]
    pair, core = mine // 2, mine % 2
    step = seq // (2 * pieces)
    for side, out in ((core, keep_out), (1 - core, share_out)):
        for k in range(pieces):
            owner = lax.rem(pair + k, pieces) * 2 + side
            out[k * step : (k + 1) * step, 0 : whole.shape[1]] = whole[
                pl.ds(pl.multiple_of(owner * step, step), step), :
            ]
    lanes = init_state.shape[2]
    norms = init_norm[...]
    norms = jnp.concatenate([norms, jnp.zeros((2, lanes - norms.shape[1]), F32)], axis=1)
    rest = jnp.zeros((init_state.shape[1] - 2, lanes), F32)
    first = jnp.concatenate([norms, rest], axis=0).astype(BF16)
    starts = [init_state[0].astype(BF16), init_state[1].astype(BF16), first]
    for out in (keep_out, share_out):
        for index, block in enumerate(starts):
            at = whole.shape[1] + index * lanes
            out[0 : block.shape[0], at : at + lanes] = block


def fold_kernel(value_up, head_gain, out_attn, out_rec, out, ahead):
    rows = value_up.shape[0]
    top = dot(value_up[...], out_attn[...]).astype(BF16)
    out[0:rows, :] = top
    gain = head_gain[...]
    width = gain.shape[1]
    column = jnp.transpose(jnp.broadcast_to(gain, (width, width)))[:, 0:1]
    bottom = (column * out_rec[...].astype(F32)).astype(BF16)
    out[rows:, :] = bottom
    ahead[0:rows, :] = top[:, : ahead.shape[1]]
    ahead[rows:, :] = bottom[:, : ahead.shape[1]]


def level_states(ids, slot, radix, fetch):
    digit = ids[slot]
    forward, backward = [], []
    for k in range(1, radix):
        source = peer_digit(digit, radix, k, False)
        forward.append(placed(fetch(k, 0), source, source < digit))
        backward.append(placed(fetch(k, 1), -source, source > digit))
    return forward, backward


def merge_kernel(ids, *refs, slot, radix, state_rows, start, last, next_radix):
    carried = 0 if start else 1
    own = refs[carried]
    received = (own,) + refs[carried + 1 : carried + radix]
    outs = refs[carried + radix :]
    state_out, messages = outs[0], outs[1:]
    kv_rows = own.shape[0] - 2 * state_rows

    def fetch(k, direction):
        at = kv_rows + direction * state_rows
        return read_state(received[k][at : at + state_rows, :])

    digit = ids[slot]
    totals = []
    for direction in range(2):
        sign = 1 - 2 * direction
        at = slice(direction * state_rows, (direction + 1) * state_rows)
        if start:
            zero = jnp.zeros((1, own.shape[1]), F32)
            none = jnp.zeros((state_rows - AUX, own.shape[1]), F32)
            inner = placed((none, zero, zero + NEG, zero), sign * digit)
        else:
            inner = placed(read_state(refs[0][at, :]), sign * digit)
        before, whole = [inner], [placed(fetch(0, direction), sign * digit)]
        for k in range(1, radix):
            source = peer_digit(digit, radix, k, False)
            state = fetch(k, direction)
            before.append(placed(state, sign * source, sign * source < sign * digit))
            whole.append(placed(state, sign * source))
        at = slice(direction * state_rows, (direction + 1) * state_rows)
        state_out[at, :] = joined(before).astype(state_out.dtype)
        totals.append(joined(whole).astype(BF16))
    total_f, total_b = totals
    part = kv_rows // 3
    for number, message in enumerate(messages):
        for section in range(3):
            for k in range(radix):
                to = (section * radix + k) * part
                message[to : to + part, :] = received[k][section * part : (section + 1) * part, :]
        at = radix * kv_rows
        if last:
            target = peer_digit(ids[slot + 1], next_radix, number + 1, True)
            ahead = target > ids[slot + 1]
            message[at : at + state_rows, :] = jnp.where(ahead, total_f, total_b)
        else:
            message[at : at + state_rows, :] = total_f
            message[at + state_rows : at + 2 * state_rows, :] = total_b


def load_kernel(*refs):
    count = (len(refs) - 1) // 2
    sems = refs[-1]
    copies = [
        pltpu.make_async_copy(refs[i], refs[count + i], sems.at[i]) for i in range(count)
    ]
    for copy in copies:
        copy.start()
    for copy in copies:
        copy.wait()


def pack_kernel(*refs, count, state_rows):
    received, out = refs[-1 - count : -1], refs[-1]
    part = (received[0].shape[0] - state_rows) // 3
    for k, message in enumerate(received):
        for section in range(3):
            to = (section * count + k) * part
            out[to : to + part, :] = message[section * part : (section + 1) * part, :]
        if k > 0:
            to = 3 * count * part + (k - 1) * state_rows
            out[to : to + state_rows, :] = message[3 * part : 3 * part + state_rows, :]


def attend(sections, keys, part, score_scale):
    rope = keys[2 * part : 3 * part, :]
    scores, lats = [], []
    for section in range(2):
        lat = keys[section * part : (section + 1) * part, :]
        lats.append(lat)
        scores.append(dot_nt(sections[section], jnp.concatenate([lat, rope], axis=1)) * score_scale)
    top = functools.reduce(jnp.maximum, [jnp.max(s, axis=1, keepdims=True) for s in scores])
    mass = accum = None
    for part_scores, lat in zip(scores, lats):
        expo = jnp.exp(part_scores - top)
        gain = dot(expo.astype(BF16), lat)
        total = jnp.sum(expo, axis=1, keepdims=True)
        accum = gain if accum is None else accum + gain
        mass = total if mass is None else mass + total
    return top, mass, accum


def sections_of(queries, width):
    return [
        queries[:, 0 : 2 * width],
        jnp.concatenate([queries[:, 0:width], queries[:, 2 * width :]], axis=1),
    ]


def finished(ids, block, first_ref, packed, sides, slot, radix, state_rows, floor_value):
    base = packed.shape[0] - (radix - 1) * state_rows
    width = packed.shape[1]

    def column(index):
        return block[:, index * width : (index + 1) * width].astype(F32)

    def triple(index):
        return column(index) + column(index + 1) + column(index + 2)

    def fetch(k, direction):
        at = base + (k - 1) * state_rows
        return read_state(packed[at : at + state_rows, :])

    levels = level_states(ids, slot, radix, fetch)
    rec_q = block[:, 7 * width : 8 * width]
    starts = []
    for index in range(2):
        inner = read_state(sides[index * state_rows : (index + 1) * state_rows, :])
        zero = jnp.zeros_like(inner[1])
        first = (
            first_ref[:, (20 + index) * width : (21 + index) * width].astype(F32),
            first_ref[0:8, 22 * width :].astype(F32)[index : index + 1],
            zero,
            zero,
        )
        states = [placed(first, -radix)] + levels[index]
        states.append(placed(inner, ids[slot] if index == 0 else -ids[slot]))
        logs, start_top, _ = chain(states)
        starts.append(weighted(states, logs, start_top) + (start_top,))
    c_start = jnp.concatenate([starts[0][0], starts[1][0]], axis=1)
    pad = jnp.zeros((rec_q.shape[1] - c_start.shape[0], c_start.shape[1]), F32)
    c_start = jnp.concatenate([c_start, pad], axis=0)
    high = c_start.astype(BF16)
    low = (c_start - high.astype(F32)).astype(BF16)
    products = dot(rec_q, high) + dot(rec_q, low)
    summed = None
    for index in range(2):
        _, n_start, start_top = starts[index]
        from_start = products[:, index * width : (index + 1) * width]
        norm_start = jnp.sum(rec_q.astype(F32) * n_start, axis=1, keepdims=True)
        numer, denom = column(3 + index), column(5 + index)
        peak, carry = triple(8 + 6 * index), triple(11 + 6 * index) + start_top
        row_max = jnp.maximum(peak, carry)
        here, there = jnp.exp(peak - row_max), jnp.exp(carry - row_max)
        numer = here * numer + there * from_start
        denom = here * denom + there * norm_start
        result = numer / jnp.maximum(jnp.abs(denom), floor_value * jnp.exp(-row_max))
        summed = result if summed is None else summed + result
    return rms(summed, 1.0).astype(BF16)


def half_kernel(
    ids,
    packed,
    sides,
    kept,
    shared,
    recurrent_out,
    top_out,
    mass_out,
    accum_out,
    *,
    slot,
    radix,
    state_rows,
    floor_value,
    score_scale,
):
    width = packed.shape[1]
    part = (packed.shape[0] - (radix - 1) * state_rows) // 3
    recurrent_out[...] = finished(
        ids, kept[...], kept, packed, sides, slot, radix, state_rows, floor_value
    )
    queries = jnp.concatenate([kept[:, 0 : 3 * width], shared[:, 0 : 3 * width]], axis=0)
    top, mass, accum = attend(sections_of(queries, width), packed, part, score_scale)
    top_out[...] = jnp.broadcast_to(top, top_out.shape)
    mass_out[...] = jnp.broadcast_to(mass, mass_out.shape)
    accum_out[...] = accum


def mix_kernel(
    ids,
    swapped,
    sides,
    kept,
    shared,
    recurrent,
    top_half,
    mass_half,
    accum_half,
    weights,
    other_weights,
    out,
    *,
    slot,
    radix,
    state_rows,
    floor_value,
    score_scale,
    piece,
    step,
):
    width = swapped.shape[1]
    part = (swapped.shape[0] - (radix - 1) * state_rows) // 3
    at = slice(piece * step, (piece + 1) * step)
    also = slice(kept.shape[0] + piece * step, kept.shape[0] + (piece + 1) * step)
    queries = jnp.concatenate([kept[at, 0 : 3 * width], shared[at, 0 : 3 * width]], axis=0)
    top, mass, accum = attend(sections_of(queries, width), swapped, part, score_scale)

    def both(ref):
        return jnp.concatenate([ref[at, :], ref[also, :]], axis=0)

    other_top = both(top_half)
    peak = jnp.maximum(top, other_top)
    here, there = jnp.exp(top - peak), jnp.exp(other_top - peak)
    accum = here * accum + there * both(accum_half)
    mass = here * mass + there * both(mass_half)
    attended = (accum / mass).astype(BF16)
    other = finished(
        ids, shared[at, :], shared, swapped, sides, slot, radix, state_rows, floor_value
    )
    mine = jnp.concatenate([attended[:step], recurrent[at, :]], axis=1)
    theirs = jnp.concatenate([attended[step:], other], axis=1)
    if piece == 0:
        out[...] = dot(mine, weights[...]) + dot(theirs, other_weights[...])
    else:
        tail = out.shape[1] - 4 * width
        skip = weights.shape[1] - tail
        out[:, 0 : 2 * width] = mine
        out[:, 2 * width : 4 * width] = theirs
        part = dot(mine, weights[:, skip:]) + dot(theirs, other_weights[:, skip:])
        out[:, 4 * width :] = part.astype(BF16)


def last_kernel(total, *refs):
    out = refs[-1]
    split = refs[1].shape[1]
    rows = refs[1].shape[0]
    left, right = total[:, :split], total[:, split:]
    for at in range(0, len(refs) - 1, 3):
        piece, weights, other_weights = refs[at : at + 3]
        left = left + dot(piece[:, 0:rows], weights[...])
        left = left + dot(piece[:, rows : 2 * rows], other_weights[...])
        right = right + piece[:, 2 * rows :].astype(F32)
    out[:, :split] = left.astype(BF16)
    out[:, split:] = right.astype(BF16)


def call(kernel, outs, inputs, scratch=(), ids=True, limit=16 << 20, cost=None):
    vmem = pl.BlockSpec(memory_space=pltpu.VMEM)
    in_specs = [vmem] * len(inputs)
    if ids:
        in_specs[0] = pl.BlockSpec(memory_space=pltpu.SMEM)
    return pl.pallas_call(
        kernel,
        out_shape=[jax.ShapeDtypeStruct(shape, dtype) for shape, dtype in outs],
        in_specs=in_specs,
        out_specs=[vmem] * len(outs),
        scratch_shapes=scratch,
        cost_estimate=cost,
        compiler_params=pltpu.CompilerParams(vmem_limit_bytes=limit),
    )(*inputs)


def shards(
    rows_in,
    in_gain,
    query_down,
    query_gain,
    kv_down,
    kv_gain,
    rope_down,
    query_nope_up,
    query_rope_up,
    key_up,
    value_up,
    rec_query,
    rec_key,
    rec_value,
    gate_weight,
    forget_level,
    head_gain,
    init_state,
    init_norm,
    out_attn,
    out_rec,
):
    peers, lanes = lax.axis_size("sp"), lax.axis_size("tp")
    block, mine = lax.axis_index("sp"), lax.axis_index("tp")
    seq = forget_level.shape[0]
    width = rows_in.shape[1]
    nope, rope = key_up.shape[1], rope_down.shape[1]
    key_width, value_width = init_state.shape[2], init_state.shape[3]
    pieces = lanes // 2
    radices = radices_of(peers)
    strides = [int(np.prod(radices[:i])) for i in range(len(radices))]
    divide = np.array([1, 1] + strides, np.int32)
    modulo = np.array([lanes, peers] + radices, np.int32)
    first = np.arange(len(divide)) == 0
    ids = (jnp.where(first, mine, block).astype(jnp.int32) // divide) % modulo

    partner = [(i, i ^ 1) for i in range(lanes)]
    ring = [[(i, (i + 2 * k) % lanes) for i in range(lanes)] for k in range(pieces)]

    gathered = [rows_in]
    for k in range(1, pieces):
        gathered.append(lax.ppermute(rows_in, "tp", ring[k]))
    row_pieces = []
    for piece in gathered:
        row_pieces += [piece, lax.ppermute(piece, "tp", partner)]

    freq = 10000.0 ** (-np.arange(rope // 2, dtype=np.float64) / (rope // 2))
    freq = np.tile(freq, 4)[None, :]
    base = np.arange(peers, dtype=np.float64)[:, None] * seq * freq
    within = np.arange(seq, dtype=np.float64)[:, None] * freq
    tables = [np.cos(base), np.sin(base), np.cos(within), np.sin(within)]
    tables = [jnp.asarray(table.astype(np.float32)) for table in tables]

    held = [
        in_gain[None, :],
        kv_down,
        kv_gain[None, :],
        rope_down.T,
        rec_key.T,
        rec_value,
        gate_weight[:, :, 0].T,
        forget_level[:, :, 0].T,
        *tables,
        query_down,
        query_gain[None, :],
        query_nope_up,
        query_rope_up.T,
        key_up,
        rec_query.T,
        value_up,
        head_gain[None, :],
        init_state[:, 0],
        init_norm[:, 0],
        out_attn,
        out_rec,
    ]
    held = list(
        pl.pallas_call(
            load_kernel,
            out_shape=[pltpu.VMEM(array.shape, array.dtype) for array in held],
            in_specs=[pl.BlockSpec(memory_space=pltpu.HBM)] * len(held),
            out_specs=[pl.BlockSpec(memory_space=pltpu.VMEM)] * len(held),
            scratch_shapes=[pltpu.SemaphoreType.DMA((len(held),))],
            name="load",
            cost_estimate=pl.CostEstimate(flops=10**8, bytes_accessed=1 << 22, transcendentals=0),
            compiler_params=pltpu.CompilerParams(vmem_limit_bytes=16 << 20),
        )(*[pltpu.with_memory_space_constraint(array, pltpu.HBM) for array in held])
    )
    head_args, local_args = held[:12], held[12:18]
    value_up, head_gain, init_state, init_norm, out_attn, out_rec = held[18:]

    (ready,) = call(
        norms_kernel,
        [((seq - seq // lanes, width), BF16)],
        row_pieces[:-1] + [held[0]],
        ids=False,
        cost=pl.CostEstimate(flops=10**7, bytes_accessed=1 << 20, transcendentals=0),
    )
    state_rows = key_width + AUX
    kv_rows = seq // 2 + seq // 4
    message, normed, keys, values, gate_rows, table = call(
        functools.partial(head_kernel, pieces=pieces, key_width=key_width),
        [
            ((kv_rows + 2 * state_rows, value_width), BF16),
            ((seq, width), BF16),
            ((seq, 2 * key_width), BF16),
            ((seq, value_width), BF16),
            ((8, seq), F32),
            ((seq, 2 * rope), F32),
        ],
        [ids, ready, row_pieces[-1]] + head_args,
    )
    columns = 20 * value_width
    assert key_width == seq // 2
    kept, share = call(
        functools.partial(local_kernel, pieces=pieces),
        [((seq // 2, columns + 3 * value_width), BF16)] * 2,
        [
            ids,
            normed,
            keys,
            values,
            gate_rows,
            table,
            *local_args,
            init_state,
            init_norm,
        ],
        scratch=[pltpu.VMEM((seq, columns), BF16)],
        cost=pl.CostEstimate(flops=10**8, bytes_accessed=1 << 20, transcendentals=0),
    )
    tail = 3 * width // 8
    weights, ahead = call(
        fold_kernel,
        [((2 * value_width, width), BF16), ((2 * value_width, width - tail), BF16)],
        [value_up, head_gain, out_attn, out_rec],
        ids=False,
        cost=pl.CostEstimate(flops=10**8, bytes_accessed=1 << 20, transcendentals=0),
    )
    other_weights = lax.ppermute(weights, "tp", partner)
    crossed = []
    for k in range(1, pieces):
        there = lax.ppermute(ahead, "tp", ring[k])
        crossed.append((there, lax.ppermute(there, "tp", partner)))
    shared = lax.ppermute(share, "tp", partner)

    carried = []
    wide = (16 << 20) if peers <= 16 else (40 << 20)
    for level, radix in enumerate(radices[:-1]):
        received = [
            lax.ppermute(message, "sp", digit_pairs(peers, strides[level], radix, k))
            for k in range(1, radix)
        ]
        last = level == len(radices) - 2
        kv_rows *= radix
        count = radices[-1] - 1 if last else 1
        out_rows = kv_rows + (1 if last else 2) * state_rows
        sides, *messages = call(
            functools.partial(
                merge_kernel,
                slot=2 + level,
                radix=radix,
                state_rows=state_rows,
                start=level == 0,
                last=last,
                next_radix=radices[level + 1],
            ),
            [((2 * state_rows, value_width), BF16 if last else F32)]
            + [((out_rows, value_width), BF16)] * max(count, 1),
            [ids, *carried, message] + received,
            limit=wide,
        )
        message = messages[0]
        carried = [sides]
    level, radix = len(radices) - 1, radices[-1]
    received = []
    for k in range(1, radix):
        pairs = digit_pairs(peers, strides[level], radix, k)
        received.append(lax.ppermute(messages[k - 1], "sp", pairs))
    other_sides = lax.ppermute(sides, "tp", partner)
    (packed,) = call(
        functools.partial(pack_kernel, count=radix, state_rows=state_rows),
        [((radix * kv_rows + (radix - 1) * state_rows, value_width), BF16)],
        [other_weights, shared, other_sides, message] + received,
        ids=False,
        limit=wide,
    )
    swapped = lax.ppermute(packed, "tp", partner)
    level_facts = dict(
        slot=2 + level,
        radix=radix,
        state_rows=state_rows,
        floor_value=float(seq * peers) ** 0.5,
        score_scale=(nope + rope) ** (-0.5),
    )
    half = call(
        functools.partial(half_kernel, **level_facts),
        [((seq // 2, value_width), BF16)] + [((seq, value_width), F32)] * 3,
        [ids, packed, sides, kept, shared],
        limit=wide,
        cost=pl.CostEstimate(flops=10**8, bytes_accessed=1 << 20, transcendentals=0),
    )
    step = seq // lanes

    def mixed(piece, shape, dtype):
        return call(
            functools.partial(
                mix_kernel,
                piece=piece,
                step=step,
                **level_facts,
            ),
            [(shape, dtype)],
            [
                ids,
                swapped,
                other_sides,
                kept,
                shared,
                *half,
                weights,
                other_weights,
            ],
            limit=wide if peers <= 16 else 56 << 20,
            cost=pl.CostEstimate(flops=10**8, bytes_accessed=1 << 20, transcendentals=0),
        )[0]

    arrived = []
    for k in range(1, pieces):
        piece = mixed(k, (step, 4 * value_width + tail), BF16)
        arrived += [lax.ppermute(piece, "tp", ring[k]), *crossed[k - 1]]
    total = mixed(0, (step, width), F32)
    (result,) = call(last_kernel, [((step, width), BF16)], [total] + arrived, ids=False)
    return result


def solution(mesh):
    in_specs = (
        P(("sp", "tp"), None),
        P(),
        P(),
        P(),
        P(),
        P(),
        P(),
        P(None, "tp"),
        P(None, "tp"),
        P(None, "tp"),
        P(None, "tp"),
        P(None, "tp"),
        P(None, "tp"),
        P(None, "tp"),
        P(None, None, "tp"),
        P("sp", None, "tp"),
        P("tp"),
        P(None, "tp", None, None),
        P(None, "tp", None),
        P("tp", None),
        P("tp", None),
    )
    out_specs = P(("sp", "tp"), None)

    return jax.shard_map(shards, mesh=mesh, in_specs=in_specs, out_specs=out_specs, check_vma=False)
```

```python
import functools

import jax
import jax.numpy as jnp
import numpy as np
from jax import lax
from jax.experimental import pallas as pl
from jax.experimental.pallas import tpu as pltpu
from jax.sharding import PartitionSpec as P

EPS = 1e-06
NEG = -(2.0**100)
AUX = 8
F32 = jnp.float32
BF16 = jnp.bfloat16
NT = (((1,), (1,)), ((), ()))


def radices_of(peers):
    first = 2 if peers % 2 == 0 else 1
    rest = peers // first
    radices = [first]
    while rest > 1:
        step = 4 if rest % 4 == 0 else next(p for p in range(2, rest + 1) if rest % p == 0)
        radices.append(step)
        rest //= step
    if len(radices) == 1:
        radices.append(1)
    return radices


def peer_digit(digit, radix, k, sending):
    if radix & (radix - 1) == 0:
        return digit ^ k
    return (digit + k if sending else digit - k + radix) % radix


def digit_pairs(peers, stride, radix, k):
    pairs = []
    for i in range(peers):
        digit = (i // stride) % radix
        pairs.append((i, i + (peer_digit(digit, radix, k, True) - digit) * stride))
    return pairs


def dot(a, b):
    return jnp.dot(a, b, preferred_element_type=F32)


def dot_nt(a, b):
    return lax.dot_general(a, b, NT, preferred_element_type=F32)


def dot_split(a, b):
    high = a.astype(BF16)
    low = (a - high.astype(F32)).astype(BF16)
    return dot(high, b) + dot(low, b)


def rms(values, gain):
    return values * lax.rsqrt(jnp.mean(values * values, axis=-1, keepdims=True) + EPS) * gain


def iota2(rows, cols, dim):
    return lax.broadcasted_iota(jnp.int32, (rows, cols), dim)


def turned_rows(weight_t):
    half = weight_t.shape[0] // 2
    return jnp.concatenate([weight_t, -weight_t[half:], weight_t[:half]], axis=0)


def angle_table(ids_ref, cos_base, sin_base, cos_row, sin_row):
    block = ids_ref[1]
    cb, sb = cos_base[pl.ds(block, 1), :], sin_base[pl.ds(block, 1), :]
    cr, sr = cos_row[...], sin_row[...]
    cos, sin = cb * cr - sb * sr, sb * cr + cb * sr
    half = cr.shape[1] // 2
    return jnp.where(iota2(cr.shape[0], cr.shape[1], 1) < half, cos, sin)


def rotated(product, table):
    mixed = product * table
    return mixed + pltpu.roll(mixed, product.shape[1] // 2, 1)


def aux_rows(n_row, peak_row, keep_row):
    high = keep_row.astype(BF16).astype(F32)
    mid = (keep_row - high).astype(BF16).astype(F32)
    low = keep_row - high - mid
    pad = jnp.zeros((AUX - 5, n_row.shape[1]), F32)
    return jnp.concatenate([n_row, peak_row, high, mid, low, pad], axis=0)


def read_state(block):
    c_rows = block.shape[0] - AUX
    block = block.astype(F32)
    aux = block[c_rows:]
    return block[:c_rows], aux[0:1], aux[1:2], aux[2:3] + aux[3:4] + aux[4:5]


def placed(state, place, use=None):
    c_part, n_part, peak, keep = state
    if use is not None:
        peak, keep = jnp.where(use, peak, NEG), jnp.where(use, keep, 0.0)
    return c_part, n_part, peak, keep, place


def chain(states):
    logs = []
    total = functools.reduce(jnp.add, [state[3] for state in states])
    for index, (_, _, peak, _, place) in enumerate(states):
        log = peak
        for other, (_, _, _, keep, at) in enumerate(states):
            if other != index:
                log = log + jnp.where(at > place, keep, 0.0)
        logs.append(log)
    return logs, functools.reduce(jnp.maximum, logs), total


def weighted(states, logs, top):
    c_sum = n_sum = None
    for state, log in zip(states, logs):
        weight = jnp.exp(log - top)
        c_part, n_part = weight * state[0], weight * state[1]
        c_sum = c_part if c_sum is None else c_sum + c_part
        n_sum = n_part if n_sum is None else n_sum + n_part
    return c_sum, n_sum


def joined(states):
    logs, top, keep = chain(states)
    top = top.astype(BF16).astype(F32)
    c_sum, n_sum = weighted(states, logs, top)
    return jnp.concatenate([c_sum, aux_rows(n_sum, top, keep)], axis=0)


def log_sigmoid(x):
    return jnp.minimum(x, 0.0) - jnp.log(1.0 + jnp.exp(-jnp.abs(x)))


def norms_kernel(*refs):
    pieces, in_gain, out = refs[:-2], refs[-2], refs[-1]
    step = pieces[0].shape[0]
    for index, piece in enumerate(pieces):
        at = slice(index * step, (index + 1) * step)
        out[at, :] = rms(piece[...].astype(F32), in_gain[...]).astype(BF16)


def head_kernel(
    ids,
    ready,
    late,
    *refs,
    pieces,
    key_width,
):
    (
        in_gain,
        kv_down,
        kv_gain,
        rope_t,
        key_t,
        rec_value,
        gate_t,
        level,
        cos_base,
        sin_base,
        cos_row,
        sin_row,
        message,
        normed_out,
        keys_out,
        values_out,
        rows_out,
        table_out,
    ) = refs
    mine = ids[0]
    pair, core = mine // 2, mine % 2
    step = late.shape[0]
    seq = normed_out.shape[0]
    last = rms(late[...].astype(F32), in_gain[...]).astype(BF16)
    for index in range(2 * pieces):
        source = lax.rem(pair - index // 2 + pieces, pieces) * 2
        source += core if index % 2 == 0 else 1 - core
        if index < 2 * pieces - 1:
            block = ready[index * step : (index + 1) * step, :]
        else:
            block = last
        normed_out[pl.ds(pl.multiple_of(source * step, step), step), :] = block
    normed = normed_out[...]
    table = angle_table(ids, cos_base, sin_base, cos_row, sin_row)
    table_out[...] = table
    latent = kv_down.shape[1]
    straight = dot(normed, jnp.concatenate([kv_down[...], rec_value[...]], axis=1))
    turned = turned_rows(rope_t[...])
    gate_rows = gate_t.shape[0]
    fill = jnp.zeros((turned.shape[0] - key_width - gate_rows, turned.shape[1]), BF16)
    crossed = dot_nt(
        normed, jnp.concatenate([turned, key_t[...], gate_t[...], fill], axis=0)
    )
    rope_lanes = turned.shape[0]
    lat = rms(straight[:, :latent], kv_gain[...]).astype(BF16)
    rope = rotated(crossed[:, :rope_lanes], table)
    half = seq // 2
    quarter = half // 2
    lat = jnp.where(core == 0, lat[:half], lat[half:])
    rope = jnp.where(core == 0, rope[:half], rope[half:])
    lanes = iota2(quarter, rope.shape[1], 1)
    packed = jnp.where(lanes < rope_t.shape[0], rope[:quarter], rope[quarter:])
    message[0:half, :] = lat
    message[half : half + quarter, :] = packed.astype(BF16)

    mixed = crossed[:, rope_lanes:]
    keys = mixed.astype(BF16).astype(F32) * key_width ** (-0.5)
    keys = jnp.where(iota2(seq, keys.shape[1], 1) < key_width, keys, 0.0)
    keys_out[...] = keys.astype(BF16)
    values = straight[:, latent:].astype(BF16)
    values_out[...] = values
    mixed_t = jnp.transpose(mixed)
    gates = mixed_t[key_width : key_width + 8]

    in_f, in_b = gates[0:1], gates[2:3]
    keep_f = log_sigmoid(gates[1:2] + level[0:1])
    keep_b = log_sigmoid(gates[3:4] + level[1:2])
    row_id, col_id = iota2(seq, seq, 0), iota2(seq, seq, 1)
    upper = jnp.where(row_id <= col_id, 1.0, 0.0).astype(BF16)
    lower = jnp.where(row_id >= col_id, 1.0, 0.0).astype(BF16)
    keeps = jnp.concatenate([keep_f, keep_b, jnp.zeros((6, seq), F32)], axis=0)
    high = keeps.astype(BF16)
    mid = (keeps - high.astype(F32)).astype(BF16)
    low = (keeps - high.astype(F32) - mid.astype(F32)).astype(BF16)
    thirds = jnp.concatenate([high, mid, low, jnp.zeros_like(low)], axis=0)
    cums = dot(thirds, jnp.concatenate([upper, lower], axis=1))
    cums = cums[0:8] + cums[8:16] + cums[16:24]
    cum_f, cum_b = cums[0:1, :seq], cums[1:2, seq:]
    all_f, all_b = cum_f[:, seq - 1 : seq], cum_b[:, 0:1]
    rows_out[...] = jnp.concatenate(
        [cum_f, in_f - cum_f, cum_b, in_b - cum_b, jnp.zeros((4, seq), F32)], axis=0
    )
    keys_t = mixed_t[:key_width].astype(BF16).astype(F32) * key_width ** (-0.5)
    base = half + quarter
    weights = []
    for cum, log_in, total in ((cum_f, in_f, all_f), (cum_b, in_b, all_b)):
        logs = total - cum + log_in
        peak = jnp.max(logs, axis=1, keepdims=True).astype(BF16).astype(F32)
        weight = jnp.exp(logs - peak)
        weights.append((weight, peak, total))
    w_f, w_b = weights[0][0], weights[1][0]
    c_both = dot(jnp.concatenate([keys_t * w_f, keys_t * w_b], axis=0).astype(BF16), values)
    sums = jnp.concatenate([w_f, w_b, jnp.zeros((6, seq), F32)], axis=0)
    n_both = dot(sums.astype(BF16), keys.astype(BF16))
    for index in range(2):
        _, peak, total = weights[index]
        c_part = c_both[index * key_width : (index + 1) * key_width]
        n_row = n_both[index : index + 1]
        zero = jnp.zeros_like(n_row)
        block = jnp.concatenate([c_part, aux_rows(n_row, zero + peak, zero + total)], axis=0)
        at = base + index * (key_width + AUX)
        message[at : at + key_width + AUX, :] = block.astype(BF16)


def thirds_of(x):
    high = x.astype(BF16)
    mid = (x - high.astype(F32)).astype(BF16)
    low = (x - high.astype(F32) - mid.astype(F32)).astype(BF16)
    return [high, mid, low]


def local_kernel(
    ids,
    normed_ref,
    keys_ref,
    values_ref,
    rows_ref,
    table_ref,
    query_down,
    query_gain,
    nope_up,
    rope_up_t,
    key_up,
    rec_query_t,
    init_state,
    init_norm,
    keep_out,
    share_out,
    whole,
    *,
    pieces,
):
    normed = normed_ref[...]
    seq = normed.shape[0]
    query_rows = jnp.concatenate([rec_query_t[...], jnp.zeros_like(rec_query_t)], axis=0)
    rec_q = dot_nt(normed, query_rows).astype(BF16)
    q_lat = rms(dot(normed, query_down[...]), query_gain[...]).astype(BF16)
    nope = dot(q_lat, nope_up[...]).astype(BF16)
    rope = rotated(dot_nt(q_lat, turned_rows(rope_up_t[...])), table_ref[...])
    lat = dot_nt(nope, key_up[...]).astype(BF16)
    width = rope_up_t.shape[0]
    lanes = iota2(seq, rope.shape[1], 1)
    low_rope = jnp.where(lanes < width, rope, 0.0).astype(BF16)
    high_rope = jnp.where(lanes >= width, rope, 0.0).astype(BF16)
    values = values_ref[...]
    wide = jnp.concatenate([values, jnp.ones_like(values)], axis=1)
    products = dot_nt(rec_q, keys_ref[...])
    row_id, col_id = iota2(seq, seq, 0), iota2(seq, seq, 1)
    rows = rows_ref[...]
    numers, denoms, marks = [], [], []
    for index in range(2):
        cum = jnp.transpose(jnp.broadcast_to(rows[2 * index : 2 * index + 1], (seq, seq)))
        seen = row_id >= col_id if index == 0 else row_id <= col_id
        logs = jnp.where(seen, cum + rows[2 * index + 1 : 2 * index + 2], NEG)
        peak = jnp.max(logs, axis=1, keepdims=True)
        gated = products * jnp.exp(logs - peak)
        sums = dot_split(gated, wide)
        numers.append(sums[:, : values.shape[1]].astype(BF16))
        denoms.append(sums[:, values.shape[1] :].astype(BF16))
        marks += thirds_of(jnp.broadcast_to(peak, (seq, seq))) + thirds_of(cum)
    columns = [lat, low_rope, high_rope] + numers + denoms + [rec_q] + marks
    step_cols = lat.shape[1]
    for index, column in enumerate(columns):
        whole[:, index * step_cols : (index + 1) * step_cols] = column
    mine = ids[0]
    pair, core = mine // 2, mine % 2
    step = seq // (2 * pieces)
    for side, out in ((core, keep_out), (1 - core, share_out)):
        for k in range(pieces):
            owner = lax.rem(pair + k, pieces) * 2 + side
            out[k * step : (k + 1) * step, 0 : whole.shape[1]] = whole[
                pl.ds(pl.multiple_of(owner * step, step), step), :
            ]
    lanes = init_state.shape[2]
    norms = init_norm[...]
    norms = jnp.concatenate([norms, jnp.zeros((2, lanes - norms.shape[1]), F32)], axis=1)
    rest = jnp.zeros((init_state.shape[1] - 2, lanes), F32)
    first = jnp.concatenate([norms, rest], axis=0).astype(BF16)
    starts = [init_state[0].astype(BF16), init_state[1].astype(BF16), first]
    for out in (keep_out, share_out):
        for index, block in enumerate(starts):
            at = whole.shape[1] + index * lanes
            out[0 : block.shape[0], at : at + lanes] = block


def fold_kernel(value_up, head_gain, out_attn, out_rec, out, ahead):
    rows = value_up.shape[0]
    top = dot(value_up[...], out_attn[...]).astype(BF16)
    out[0:rows, :] = top
    gain = head_gain[...]
    width = gain.shape[1]
    column = jnp.transpose(jnp.broadcast_to(gain, (width, width)))[:, 0:1]
    bottom = (column * out_rec[...].astype(F32)).astype(BF16)
    out[rows:, :] = bottom
    ahead[0:rows, :] = top[:, : ahead.shape[1]]
    ahead[rows:, :] = bottom[:, : ahead.shape[1]]


def level_states(ids, slot, radix, fetch):
    digit = ids[slot]
    forward, backward = [], []
    for k in range(1, radix):
        source = peer_digit(digit, radix, k, False)
        forward.append(placed(fetch(k, 0), source, source < digit))
        backward.append(placed(fetch(k, 1), -source, source > digit))
    return forward, backward


def merge_kernel(ids, *refs, slot, radix, state_rows, start, last, next_radix):
    carried = 0 if start else 1
    own = refs[carried]
    received = (own,) + refs[carried + 1 : carried + radix]
    outs = refs[carried + radix :]
    state_out, messages = outs[0], outs[1:]
    kv_rows = own.shape[0] - 2 * state_rows

    def fetch(k, direction):
        at = kv_rows + direction * state_rows
        return read_state(received[k][at : at + state_rows, :])

    digit = ids[slot]
    totals = []
    for direction in range(2):
        sign = 1 - 2 * direction
        at = slice(direction * state_rows, (direction + 1) * state_rows)
        if start:
            zero = jnp.zeros((1, own.shape[1]), F32)
            none = jnp.zeros((state_rows - AUX, own.shape[1]), F32)
            inner = placed((none, zero, zero + NEG, zero), sign * digit)
        else:
            inner = placed(read_state(refs[0][at, :]), sign * digit)
        before, whole = [inner], [placed(fetch(0, direction), sign * digit)]
        for k in range(1, radix):
            source = peer_digit(digit, radix, k, False)
            state = fetch(k, direction)
            before.append(placed(state, sign * source, sign * source < sign * digit))
            whole.append(placed(state, sign * source))
        at = slice(direction * state_rows, (direction + 1) * state_rows)
        if start and radix == 2:
            c_part, n_part, peak, keep, _ = before[1]
            inside = jnp.concatenate([c_part, aux_rows(n_part, peak, keep)], axis=0)
        else:
            inside = joined(before)
        state_out[at, :] = inside.astype(state_out.dtype)
        totals.append(joined(whole).astype(BF16))
    total_f, total_b = totals
    part = kv_rows // 3
    for number, message in enumerate(messages):
        for section in range(3):
            for k in range(radix):
                to = (section * radix + k) * part
                message[to : to + part, :] = received[k][section * part : (section + 1) * part, :]
        at = radix * kv_rows
        if last:
            target = peer_digit(ids[slot + 1], next_radix, number + 1, True)
            ahead = target > ids[slot + 1]
            message[at : at + state_rows, :] = jnp.where(ahead, total_f, total_b)
        else:
            message[at : at + state_rows, :] = total_f
            message[at + state_rows : at + 2 * state_rows, :] = total_b


def load_kernel(*refs):
    count = (len(refs) - 1) // 2
    sems = refs[-1]
    copies = [
        pltpu.make_async_copy(refs[i], refs[count + i], sems.at[i]) for i in range(count)
    ]
    for copy in copies:
        copy.start()
    for copy in copies:
        copy.wait()


def late_of(radix):
    return min(2, radix - 1)


def early_of(radix):
    return [k for k in range(1, radix) if k != late_of(radix)]


def pack_kernel(*refs, count, state_rows):
    received, out = refs[-1 - count : -1], refs[-1]
    part = (received[0].shape[0] - state_rows) // 3
    for k, message in enumerate(received):
        for section in range(3):
            to = (section * count + k) * part
            out[to : to + part, :] = message[section * part : (section + 1) * part, :]
        if k > 0:
            to = 3 * count * part + (k - 1) * state_rows
            out[to : to + state_rows, :] = message[3 * part : 3 * part + state_rows, :]


def attend(sections, sources, score_scale):
    scores, lats = [], []
    for keys, part in sources:
        rope = keys[2 * part : 3 * part, :]
        for section in range(2):
            lat = keys[section * part : (section + 1) * part, :]
            lats.append(lat)
            scores.append(
                dot_nt(sections[section], jnp.concatenate([lat, rope], axis=1)) * score_scale
            )
    top = functools.reduce(jnp.maximum, [jnp.max(s, axis=1, keepdims=True) for s in scores])
    mass = accum = None
    for part_scores, lat in zip(scores, lats):
        expo = jnp.exp(part_scores - top)
        gain = dot(expo.astype(BF16), lat)
        total = jnp.sum(expo, axis=1, keepdims=True)
        accum = gain if accum is None else accum + gain
        mass = total if mass is None else mass + total
    return top, mass, accum


def sources_of(packed, late, radix, state_rows):
    part = (packed.shape[0] - (radix - 2) * state_rows) // 3
    return [(packed, part), (late, (late.shape[0] - state_rows) // 3)]


def sections_of(queries, width):
    return [
        queries[:, 0 : 2 * width],
        jnp.concatenate([queries[:, 0:width], queries[:, 2 * width :]], axis=1),
    ]


def finished(ids, block, first_ref, packed, late, sides, slot, radix, state_rows, floor_value):
    base = packed.shape[0] - (radix - 2) * state_rows
    width = packed.shape[1]

    def column(index):
        return block[:, index * width : (index + 1) * width].astype(F32)

    def triple(index):
        return column(index) + column(index + 1) + column(index + 2)

    def fetch(k, direction):
        if k == late_of(radix):
            return read_state(late[late.shape[0] - state_rows :, :])
        at = base + early_of(radix).index(k) * state_rows
        return read_state(packed[at : at + state_rows, :])

    levels = level_states(ids, slot, radix, fetch)
    rec_q = block[:, 7 * width : 8 * width]
    starts = []
    for index in range(2):
        inner = read_state(sides[index * state_rows : (index + 1) * state_rows, :])
        zero = jnp.zeros_like(inner[1])
        first = (
            first_ref[:, (20 + index) * width : (21 + index) * width].astype(F32),
            first_ref[0:8, 22 * width :].astype(F32)[index : index + 1],
            zero,
            zero,
        )
        states = [placed(first, -radix)] + levels[index]
        states.append(placed(inner, ids[slot] if index == 0 else -ids[slot]))
        logs, start_top, _ = chain(states)
        starts.append(weighted(states, logs, start_top) + (start_top,))
    c_start = jnp.concatenate([starts[0][0], starts[1][0]], axis=1)
    pad = jnp.zeros((rec_q.shape[1] - c_start.shape[0], c_start.shape[1]), F32)
    c_start = jnp.concatenate([c_start, pad], axis=0)
    high = c_start.astype(BF16)
    low = (c_start - high.astype(F32)).astype(BF16)
    products = dot(rec_q, high) + dot(rec_q, low)
    summed = None
    for index in range(2):
        _, n_start, start_top = starts[index]
        from_start = products[:, index * width : (index + 1) * width]
        norm_start = jnp.sum(rec_q.astype(F32) * n_start, axis=1, keepdims=True)
        numer, denom = column(3 + index), column(5 + index)
        peak, carry = triple(8 + 6 * index), triple(11 + 6 * index) + start_top
        row_max = jnp.maximum(peak, carry)
        here, there = jnp.exp(peak - row_max), jnp.exp(carry - row_max)
        numer = here * numer + there * from_start
        denom = here * denom + there * norm_start
        result = numer / jnp.maximum(jnp.abs(denom), floor_value * jnp.exp(-row_max))
        summed = result if summed is None else summed + result
    return rms(summed, 1.0).astype(BF16)


def half_kernel(
    ids,
    packed,
    late,
    sides,
    kept,
    shared,
    recurrent_out,
    top_out,
    mass_out,
    accum_out,
    *,
    slot,
    radix,
    state_rows,
    floor_value,
    score_scale,
):
    width = packed.shape[1]
    recurrent_out[...] = finished(
        ids, kept[...], kept, packed, late, sides, slot, radix, state_rows, floor_value
    )
    queries = jnp.concatenate([kept[:, 0 : 3 * width], shared[:, 0 : 3 * width]], axis=0)
    sources = sources_of(packed, late, radix, state_rows)
    top, mass, accum = attend(sections_of(queries, width), sources, score_scale)
    top_out[...] = jnp.broadcast_to(top, top_out.shape)
    mass_out[...] = jnp.broadcast_to(mass, mass_out.shape)
    accum_out[...] = accum


def mix_kernel(
    ids,
    swapped,
    late,
    sides,
    kept,
    shared,
    recurrent,
    top_half,
    mass_half,
    accum_half,
    weights,
    other_weights,
    out,
    *,
    slot,
    radix,
    state_rows,
    floor_value,
    score_scale,
    piece,
    step,
):
    width = swapped.shape[1]
    at = slice(piece * step, (piece + 1) * step)
    also = slice(kept.shape[0] + piece * step, kept.shape[0] + (piece + 1) * step)
    queries = jnp.concatenate([kept[at, 0 : 3 * width], shared[at, 0 : 3 * width]], axis=0)
    sources = sources_of(swapped, late, radix, state_rows)
    top, mass, accum = attend(sections_of(queries, width), sources, score_scale)

    def both(ref):
        return jnp.concatenate([ref[at, :], ref[also, :]], axis=0)

    other_top = both(top_half)
    peak = jnp.maximum(top, other_top)
    here, there = jnp.exp(top - peak), jnp.exp(other_top - peak)
    accum = here * accum + there * both(accum_half)
    mass = here * mass + there * both(mass_half)
    attended = (accum / mass).astype(BF16)
    other = finished(
        ids, shared[at, :], shared, swapped, late, sides, slot, radix, state_rows, floor_value
    )
    mine = jnp.concatenate([attended[:step], recurrent[at, :]], axis=1)
    theirs = jnp.concatenate([attended[step:], other], axis=1)
    if piece == 0:
        out[...] = dot(mine, weights[...]) + dot(theirs, other_weights[...])
    else:
        tail = out.shape[1] - 4 * width
        skip = weights.shape[1] - tail
        out[:, 0 : 2 * width] = mine
        out[:, 2 * width : 4 * width] = theirs
        part = dot(mine, weights[:, skip:]) + dot(theirs, other_weights[:, skip:])
        out[:, 4 * width :] = part.astype(BF16)


def last_kernel(total, *refs):
    out = refs[-1]
    split = refs[1].shape[1]
    rows = refs[1].shape[0]
    left, right = total[:, :split], total[:, split:]
    for at in range(0, len(refs) - 1, 3):
        piece, weights, other_weights = refs[at : at + 3]
        left = left + dot(piece[:, 0:rows], weights[...])
        left = left + dot(piece[:, rows : 2 * rows], other_weights[...])
        right = right + piece[:, 2 * rows :].astype(F32)
    out[:, :split] = left.astype(BF16)
    out[:, split:] = right.astype(BF16)


def call(kernel, outs, inputs, scratch=(), ids=True, limit=16 << 20, cost=None):
    vmem = pl.BlockSpec(memory_space=pltpu.VMEM)
    in_specs = [vmem] * len(inputs)
    if ids:
        in_specs[0] = pl.BlockSpec(memory_space=pltpu.SMEM)
    return pl.pallas_call(
        kernel,
        out_shape=[jax.ShapeDtypeStruct(shape, dtype) for shape, dtype in outs],
        in_specs=in_specs,
        out_specs=[vmem] * len(outs),
        scratch_shapes=scratch,
        cost_estimate=cost,
        compiler_params=pltpu.CompilerParams(vmem_limit_bytes=limit),
    )(*inputs)


def shards(
    rows_in,
    in_gain,
    query_down,
    query_gain,
    kv_down,
    kv_gain,
    rope_down,
    query_nope_up,
    query_rope_up,
    key_up,
    value_up,
    rec_query,
    rec_key,
    rec_value,
    gate_weight,
    forget_level,
    head_gain,
    init_state,
    init_norm,
    out_attn,
    out_rec,
):
    peers, lanes = lax.axis_size("sp"), lax.axis_size("tp")
    block, mine = lax.axis_index("sp"), lax.axis_index("tp")
    seq = forget_level.shape[0]
    width = rows_in.shape[1]
    nope, rope = key_up.shape[1], rope_down.shape[1]
    key_width, value_width = init_state.shape[2], init_state.shape[3]
    pieces = lanes // 2
    radices = radices_of(peers)
    strides = [int(np.prod(radices[:i])) for i in range(len(radices))]
    divide = np.array([1, 1] + strides, np.int32)
    modulo = np.array([lanes, peers] + radices, np.int32)
    first = np.arange(len(divide)) == 0
    ids = (jnp.where(first, mine, block).astype(jnp.int32) // divide) % modulo

    partner = [(i, i ^ 1) for i in range(lanes)]
    ring = [[(i, (i + 2 * k) % lanes) for i in range(lanes)] for k in range(pieces)]

    gathered = [rows_in]
    for k in range(1, pieces):
        gathered.append(lax.ppermute(rows_in, "tp", ring[k]))
    row_pieces = []
    for piece in gathered:
        row_pieces += [piece, lax.ppermute(piece, "tp", partner)]

    freq = 10000.0 ** (-np.arange(rope // 2, dtype=np.float64) / (rope // 2))
    freq = np.tile(freq, 4)[None, :]
    base = np.arange(peers, dtype=np.float64)[:, None] * seq * freq
    within = np.arange(seq, dtype=np.float64)[:, None] * freq
    tables = [np.cos(base), np.sin(base), np.cos(within), np.sin(within)]
    tables = [jnp.asarray(table.astype(np.float32)) for table in tables]

    held = [
        in_gain[None, :],
        kv_down,
        kv_gain[None, :],
        rope_down.T,
        rec_key.T,
        rec_value,
        gate_weight[:, :, 0].T,
        forget_level[:, :, 0].T,
        *tables,
        query_down,
        query_gain[None, :],
        query_nope_up,
        query_rope_up.T,
        key_up,
        rec_query.T,
        value_up,
        head_gain[None, :],
        init_state[:, 0],
        init_norm[:, 0],
        out_attn,
        out_rec,
    ]
    held = list(
        pl.pallas_call(
            load_kernel,
            out_shape=[pltpu.VMEM(array.shape, array.dtype) for array in held],
            in_specs=[pl.BlockSpec(memory_space=pltpu.HBM)] * len(held),
            out_specs=[pl.BlockSpec(memory_space=pltpu.VMEM)] * len(held),
            scratch_shapes=[pltpu.SemaphoreType.DMA((len(held),))],
            name="load",
            cost_estimate=pl.CostEstimate(flops=10**8, bytes_accessed=1 << 22, transcendentals=0),
            compiler_params=pltpu.CompilerParams(vmem_limit_bytes=16 << 20),
        )(*[pltpu.with_memory_space_constraint(array, pltpu.HBM) for array in held])
    )
    head_args, local_args = held[:12], held[12:18]
    value_up, head_gain, init_state, init_norm, out_attn, out_rec = held[18:]

    (ready,) = call(
        norms_kernel,
        [((seq - seq // lanes, width), BF16)],
        row_pieces[:-1] + [held[0]],
        ids=False,
        cost=pl.CostEstimate(flops=10**7, bytes_accessed=1 << 20, transcendentals=0),
    )
    state_rows = key_width + AUX
    kv_rows = seq // 2 + seq // 4
    message, normed, keys, values, gate_rows, table = call(
        functools.partial(head_kernel, pieces=pieces, key_width=key_width),
        [
            ((kv_rows + 2 * state_rows, value_width), BF16),
            ((seq, width), BF16),
            ((seq, 2 * key_width), BF16),
            ((seq, value_width), BF16),
            ((8, seq), F32),
            ((seq, 2 * rope), F32),
        ],
        [ids, ready, row_pieces[-1]] + head_args,
    )
    columns = 20 * value_width
    assert key_width == seq // 2
    kept, share = call(
        functools.partial(local_kernel, pieces=pieces),
        [((seq // 2, columns + 3 * value_width), BF16)] * 2,
        [
            ids,
            normed,
            keys,
            values,
            gate_rows,
            table,
            *local_args,
            init_state,
            init_norm,
        ],
        scratch=[pltpu.VMEM((seq, columns), BF16)],
        cost=pl.CostEstimate(flops=10**8, bytes_accessed=1 << 20, transcendentals=0),
    )
    tail = 3 * width // 8
    weights, ahead = call(
        fold_kernel,
        [((2 * value_width, width), BF16), ((2 * value_width, width - tail), BF16)],
        [value_up, head_gain, out_attn, out_rec],
        ids=False,
        cost=pl.CostEstimate(flops=10**8, bytes_accessed=1 << 20, transcendentals=0),
    )
    other_weights = lax.ppermute(weights, "tp", partner)
    crossed = []
    for k in range(1, pieces):
        there = lax.ppermute(ahead, "tp", ring[k])
        crossed.append((there, lax.ppermute(there, "tp", partner)))
    shared = lax.ppermute(share, "tp", partner)

    carried = []
    wide = (16 << 20) if peers <= 16 else (40 << 20)
    for level, radix in enumerate(radices[:-1]):
        received = [
            lax.ppermute(message, "sp", digit_pairs(peers, strides[level], radix, k))
            for k in range(1, radix)
        ]
        last = level == len(radices) - 2
        kv_rows *= radix
        count = radices[-1] - 1 if last else 1
        out_rows = kv_rows + (1 if last else 2) * state_rows
        sides, *messages = call(
            functools.partial(
                merge_kernel,
                slot=2 + level,
                radix=radix,
                state_rows=state_rows,
                start=level == 0,
                last=last,
                next_radix=radices[level + 1],
            ),
            [((2 * state_rows, value_width), BF16 if last else F32)]
            + [((out_rows, value_width), BF16)] * max(count, 1),
            [ids, *carried, message] + received,
            limit=wide,
        )
        message = messages[0]
        carried = [sides]
    level, radix = len(radices) - 1, radices[-1]
    received = []
    for k in range(1, radix):
        pairs = digit_pairs(peers, strides[level], radix, k)
        received.append(lax.ppermute(messages[k - 1], "sp", pairs))
    other_sides = lax.ppermute(sides, "tp", partner)
    late = received.pop(late_of(radix) - 1)
    (packed,) = call(
        functools.partial(pack_kernel, count=radix - 1, state_rows=state_rows),
        [(((radix - 1) * kv_rows + (radix - 2) * state_rows, value_width), BF16)],
        [shared, other_sides, message] + received,
        ids=False,
        limit=wide,
    )
    swapped = lax.ppermute(packed, "tp", partner)
    other_late = lax.ppermute(late, "tp", partner)
    level_facts = dict(
        slot=2 + level,
        radix=radix,
        state_rows=state_rows,
        floor_value=float(seq * peers) ** 0.5,
        score_scale=(nope + rope) ** (-0.5),
    )
    half = call(
        functools.partial(half_kernel, **level_facts),
        [((seq // 2, value_width), BF16)] + [((seq, value_width), F32)] * 3,
        [ids, packed, late, sides, kept, shared],
        limit=wide,
        cost=pl.CostEstimate(flops=10**8, bytes_accessed=1 << 20, transcendentals=0),
    )
    step = seq // lanes

    def mixed(piece, shape, dtype):
        return call(
            functools.partial(
                mix_kernel,
                piece=piece,
                step=step,
                **level_facts,
            ),
            [(shape, dtype)],
            [
                ids,
                swapped,
                other_late,
                other_sides,
                kept,
                shared,
                *half,
                weights,
                other_weights,
            ],
            limit=wide if peers <= 16 else 56 << 20,
            cost=pl.CostEstimate(flops=10**8, bytes_accessed=1 << 20, transcendentals=0),
        )[0]

    arrived = []
    for k in range(1, pieces):
        piece = mixed(k, (step, 4 * value_width + tail), BF16)
        arrived += [lax.ppermute(piece, "tp", ring[k]), *crossed[k - 1]]
    total = mixed(0, (step, width), F32)
    (result,) = call(last_kernel, [((step, width), BF16)], [total] + arrived, ids=False)
    return result


def solution(mesh):
    in_specs = (
        P(("sp", "tp"), None),
        P(),
        P(),
        P(),
        P(),
        P(),
        P(),
        P(None, "tp"),
        P(None, "tp"),
        P(None, "tp"),
        P(None, "tp"),
        P(None, "tp"),
        P(None, "tp"),
        P(None, "tp"),
        P(None, None, "tp"),
        P("sp", None, "tp"),
        P("tp"),
        P(None, "tp", None, None),
        P(None, "tp", None),
        P("tp", None),
        P("tp", None),
    )
    out_specs = P(("sp", "tp"), None)

    return jax.shard_map(shards, mesh=mesh, in_specs=in_specs, out_specs=out_specs, check_vma=False)
```
